512 devices in a mesh: rep: 2 (over z_hi), fs: 32 (over z_lo, y), tp: 8 (over x, core).
Axes of the slice: x: 4, y: 4, z: 16 (z_hi: 2, z_lo: 8; z = z_hi * 8 + z_lo), core: 2. Of those that a mesh axis runs over, the one named last changes fastest.
Arguments:
- tokens: bfloat16 [64, 1024, 1024], P(('rep', 'fs'), 'tp'), may hold values from -6 to 6
- mixer_in_gain: float32 [1024], replicated, may hold values from 0.5 to 1.5
- query_weight: bfloat16 [1024, 1024], P('fs', 'tp'), may hold values from -0.1875 to 0.1875
- key_weight: bfloat16 [1024, 1024], P('fs', 'tp'), may hold values from -0.1875 to 0.1875
- value_weight: bfloat16 [1024, 2048], P('fs', 'tp'), may hold values from -0.1875 to 0.1875
- gate_weight: bfloat16 [1024, 2048], P('fs', 'tp'), may hold values from -0.1875 to 0.1875
- decay_logits: float32 [2, 8], P(None, 'tp'), may hold values from 3.4 to 6.2
- mixer_output: bfloat16 [2048, 1024], P('tp', 'fs'), may hold values from -0.125 to 0.125
- mixer_out_gain: float32 [1024], replicated, may hold values from 0.5 to 1.5
- channel_in_gain: float32 [1024], replicated, may hold values from 0.5 to 1.5
- gelu_weight: bfloat16 [1024, 2816], P('fs', 'tp'), may hold values from -0.1875 to 0.1875
- linear_weight: bfloat16 [1024, 2816], P('fs', 'tp'), may hold values from -0.1875 to 0.1875
- gelu_kernel: float32 [3, 2816], P(None, 'tp'), may hold values from -3.5 to 3.5
- linear_kernel: float32 [3, 2816], P(None, 'tp'), may hold values from -3.5 to 3.5
- gelu_bias: float32 [2816], P('tp'), may hold values from -1.2 to 1.2
- linear_bias: float32 [2816], P('tp'), may hold values from -1.2 to 1.2
- down_weight: bfloat16 [2816, 1024], P('tp', 'fs'), may hold values from -0.109375 to 0.109375
- channel_out_gain: float32 [1024], replicated, may hold values from 0.5 to 1.5
Outputs:
- layer_output: bfloat16 [64, 1024, 1024], P(('rep', 'fs'), 'tp')
The draws below stay inside these ranges and needn't reach their ends.
All inputs are finite; a program needn't handle non-finite values.
Results may differ from the reference program's by a relative error of at most 0.02.
Values may be sent and summed in bfloat16 or wider, within the bound.
No kernel may reach another device: no remote copies, remote signals or barrier semaphores. Data moves between devices by JAX's collectives and lax.ppermute only.
A program may use at most 64 MiB of HBM per device.

```python
import jax
import jax.numpy as jnp
from jax import lax

D = 1024
HEADS = 8
DK = 128
DV = 256
FF = 2816
TAPS = 3
SPAN = 128
SEQ = 1024
SEQS = 64


def block_levels(own_key, shape, pieces, low, largest):
    level = 1.0
    for position, blocks in pieces:
        heights = jax.random.uniform(jax.random.fold_in(jax.random.fold_in(own_key, 6), position), (blocks,), jnp.float32, low / len(pieces), largest / len(pieces))
        level = level * jnp.repeat(jnp.exp(heights), shape[position] // blocks).reshape((-1,) + (1,) * (len(shape) - 1 - position))
    return level


def noise(own_key, dims, deviation, reach, pieces=(), kind=jnp.bfloat16):
    result = deviation * jax.random.normal(own_key, dims, jnp.float32)
    if pieces:
        result = result * block_levels(own_key, dims, pieces, -0.22, 0.18)
    return jnp.clip(result, -reach, reach).astype(kind)


def setup_inputs(seed: int = 0) -> dict:
    splits = jax.random.split(jax.random.key(seed), 19)
    return {
        "tokens": noise(splits[0], (SEQS, SEQ, D), 1.0, 6.0, ((0, 64), (1, 8))),
        "mixer_in_gain": jnp.clip(1.0 + 0.1 * jax.random.normal(splits[1], (D,), jnp.float32), 0.5, 1.5),
        "query_weight": noise(splits[2], (D, HEADS * DK), D ** -0.5, 0.1875, ((0, 32), (1, 8))),
        "key_weight": noise(splits[3], (D, HEADS * DK), D ** -0.5, 0.1875, ((0, 32), (1, 8))),
        "value_weight": noise(splits[4], (D, HEADS * DV), D ** -0.5, 0.1875, ((0, 32), (1, 8))),
        "gate_weight": noise(splits[5], (D, HEADS * DV), D ** -0.5, 0.1875, ((0, 32), (1, 8))),
        "decay_logits": jnp.clip(3.4 + 2.7999997 * jax.random.uniform(splits[6], (2, HEADS), jnp.float32) ** block_levels(splits[6], (2, HEADS), ((1, 8),), -0.2, 0.2), 3.4, 6.2),
        "mixer_output": noise(splits[7], (HEADS * DV, D), (HEADS * DV) ** -0.5, 0.125, ((0, 8), (1, 32))),
        "mixer_out_gain": jnp.clip(1.0 + 0.1 * jax.random.normal(splits[8], (D,), jnp.float32), 0.5, 1.5),
        "channel_in_gain": jnp.clip(1.0 + 0.1 * jax.random.normal(splits[9], (D,), jnp.float32), 0.5, 1.5),
        "gelu_weight": noise(splits[10], (D, FF), D ** -0.5, 0.1875, ((0, 32), (1, 8))),
        "linear_weight": noise(splits[11], (D, FF), D ** -0.5, 0.1875, ((0, 32), (1, 8))),
        "gelu_kernel": noise(splits[12], (TAPS, FF), TAPS ** -0.5, 3.5, ((1, 8),), jnp.float32),
        "linear_kernel": noise(splits[13], (TAPS, FF), TAPS ** -0.5, 3.5, ((1, 8),), jnp.float32),
        "gelu_bias": noise(splits[14], (FF,), 0.3, 1.2, ((0, 8),), jnp.float32),
        "linear_bias": noise(splits[15], (FF,), 0.3, 1.2, ((0, 8),), jnp.float32),
        "down_weight": noise(splits[16], (FF, D), FF ** -0.5, 0.109375, ((0, 8), (1, 32))),
        "channel_out_gain": jnp.clip(1.0 + 0.1 * jax.random.normal(splits[17], (D,), jnp.float32), 0.5, 1.5),
    }


epsilon = 1e-06
rope_base = 10000.0

def rms_scaled(row_values, norm_gain):
    values = row_values.astype(jnp.float32)
    return values * lax.rsqrt(lax.optimization_barrier(jnp.mean(values * values, axis=-1, keepdims=True)) + epsilon) * norm_gain

def rotate(values, positions):
    half_width = values.shape[-1] // 2
    frequency = 1.0 / rope_base ** (jnp.arange(half_width, dtype=jnp.float32) / half_width)
    angles = positions.astype(jnp.float32)[:, None] * frequency[None, :]
    cosine = jnp.cos(angles)[:, None, :]
    sine_part = jnp.sin(angles)[:, None, :]
    first_half = values[..., :half_width]
    second = values[..., half_width:]
    return jnp.concatenate([first_half * cosine - second * sine_part, first_half * sine_part + second * cosine], axis=-1)

def one_direction(queries, key_rows, value_rows, log_decay, strict):
    highest = lax.Precision.HIGHEST
    length = queries.shape[0]
    head_count = queries.shape[1]
    block_count = length // SPAN
    inside_index = jnp.arange(SPAN, dtype=jnp.float32)
    offset = inside_index[:, None] - inside_index[None, :]
    allowed = offset >= (1.0 if strict else 0.0)
    within = jnp.where(allowed[None], jnp.exp(jnp.where(allowed, offset, 0.0)[None] * log_decay[:, None, None]), 0.0)
    query_blocks = queries.reshape(block_count, SPAN, head_count, -1).astype(jnp.float32)
    key_blocks = key_rows.reshape(block_count, SPAN, head_count, -1).astype(jnp.float32)
    value_blocks = value_rows.reshape(block_count, SPAN, head_count, -1).astype(jnp.float32)
    scores = jnp.einsum('nchd,nmhd->nhcm', query_blocks, key_blocks, precision=highest) * within[None]
    inside = jnp.einsum('nhcm,nmhe->nche', scores, value_blocks, precision=highest)
    tail_decay = jnp.exp((SPAN - 1.0 - inside_index)[:, None] * log_decay[None, :])
    lead_decay = jnp.exp((inside_index + 1.0)[:, None] * log_decay[None, :])
    step_decay = jnp.exp(SPAN * log_decay)
    updates = jnp.einsum('nmhd,nmhe->nhde', key_blocks, value_blocks * tail_decay[None, :, :, None], precision=highest)

    def advance(carried, update):
        return (step_decay[:, None, None] * carried + update, carried)
    _, before = lax.scan(advance, jnp.zeros(updates.shape[1:], jnp.float32), updates)
    across = jnp.einsum('nchd,nhde->nche', query_blocks * lead_decay[None, :, :, None], before, precision=highest)
    return (inside + across).reshape(length, head_count, -1)

def retention(queries, key_rows, value_rows, logits):
    log_forward = jax.nn.log_sigmoid(logits[0])
    log_backward = jax.nn.log_sigmoid(logits[1])
    forward = one_direction(queries, key_rows, value_rows, log_forward, False)
    behind = one_direction(queries[::-1], key_rows[::-1], value_rows[::-1], log_backward, True)[::-1]
    return forward + behind

def head_norm(values):
    centred = values - lax.optimization_barrier(jnp.mean(values, axis=-1, keepdims=True))
    return centred * lax.rsqrt(lax.optimization_barrier(jnp.mean(centred * centred, axis=-1, keepdims=True)) + epsilon)

def conv_positions(values, kernel, biases):
    padded = jnp.pad(values.astype(jnp.float32), ((1, 1), (0, 0)))
    return kernel[0] * padded[:-2] + kernel[1] * padded[1:-1] + kernel[2] * padded[2:] + biases

def reference(tokens, mixer_in_gain, query_weight, key_weight, value_weight, gate_weight, decay_logits, mixer_output, mixer_out_gain, channel_in_gain, gelu_weight, linear_weight, gelu_kernel, linear_kernel, gelu_bias, linear_bias, down_weight, channel_out_gain):

    def one_sequence(token_rows):
        positions = jnp.arange(SEQ, dtype=jnp.int32)
        normed = rms_scaled(token_rows, mixer_in_gain).astype(jnp.bfloat16)
        query_raw = jnp.dot(normed, query_weight, preferred_element_type=jnp.float32).reshape(SEQ, HEADS, DK)
        queries = rotate(query_raw, positions).astype(jnp.bfloat16)
        key_raw = jnp.dot(normed, key_weight, preferred_element_type=jnp.float32).reshape(SEQ, HEADS, DK)
        key_rows = (rotate(key_raw, positions) * DK ** (-0.5)).astype(jnp.bfloat16)
        value_rows = jnp.dot(normed, value_weight, preferred_element_type=jnp.float32).astype(jnp.bfloat16).reshape(SEQ, HEADS, DV)
        gate_rows = jnp.dot(normed, gate_weight, preferred_element_type=jnp.float32).astype(jnp.bfloat16)
        retained = retention(queries, key_rows, value_rows, decay_logits)
        gated = (head_norm(retained).reshape(SEQ, HEADS * DV) * jax.nn.silu(gate_rows.astype(jnp.float32))).astype(jnp.bfloat16)
        mix_sum = jnp.dot(gated, mixer_output, preferred_element_type=jnp.float32)
        after_mix = (token_rows.astype(jnp.float32) + rms_scaled(mix_sum, mixer_out_gain)).astype(jnp.bfloat16)
        channel_in = rms_scaled(after_mix, channel_in_gain).astype(jnp.bfloat16)
        gelu_in = jnp.dot(channel_in, gelu_weight, preferred_element_type=jnp.float32).astype(jnp.bfloat16)
        linear_in = jnp.dot(channel_in, linear_weight, preferred_element_type=jnp.float32).astype(jnp.bfloat16)
        hidden = (jax.nn.gelu(conv_positions(gelu_in, gelu_kernel, gelu_bias)) * conv_positions(linear_in, linear_kernel, linear_bias)).astype(jnp.bfloat16)
        channel_sum = jnp.dot(hidden, down_weight, preferred_element_type=jnp.float32)
        return (after_mix.astype(jnp.float32) + rms_scaled(channel_sum, channel_out_gain)).astype(jnp.bfloat16)
    return lax.map(one_sequence, tokens)
```

```python
import jax
import jax.numpy as jnp
from jax import lax
from jax.sharding import Mesh
from jax.sharding import PartitionSpec as P

DK = 128
DV = 256
TP = ("x", "c")
FS = ("z", "y")
SWAP = ((0, 1), (1, 0))
PAD = 384
epsilon = 1e-06
rope_base = 10000.0


def gather_axis(piece, axis):
    count = lax.axis_size(axis)
    return lax.all_to_all(
        jnp.broadcast_to(piece[None], (count, *piece.shape)), axis, 0, 0, tiled=True
    )


def swap(value):
    return lax.ppermute(value, "c", SWAP)


def after(value, other):
    return lax.optimization_barrier((value, other))[0]


def rows_in_order(pieces):
    return pieces.transpose(1, 0, 2, 3).reshape(-1, pieces.shape[-1])


def rms_scaled(row_values, norm_gain):
    values = row_values.astype(jnp.float32)
    return (
        values * lax.rsqrt(jnp.mean(values * values, axis=-1, keepdims=True) + epsilon) * norm_gain
    )


def rotate(values, positions):
    half_width = values.shape[-1] // 2
    frequency = 1.0 / rope_base ** (jnp.arange(half_width, dtype=jnp.float32) / half_width)
    angles = positions.astype(jnp.float32)[:, None] * frequency[None, :]
    cosine = jnp.cos(angles)
    sine_part = jnp.sin(angles)
    first_half = values[..., :half_width]
    second = values[..., half_width:]
    return jnp.concatenate(
        [first_half * cosine - second * sine_part, first_half * sine_part + second * cosine],
        axis=-1,
    )


def head_norm(values):
    centred = values - jnp.mean(values, axis=-1, keepdims=True)
    return centred * lax.rsqrt(jnp.mean(centred * centred, axis=-1, keepdims=True) + epsilon)


def dot(a, b):
    return jnp.dot(a, b, preferred_element_type=jnp.float32)


def dot_nt(a, b):
    return lax.dot_general(a, b, (((1,), (1,)), ((), ())), preferred_element_type=jnp.float32)


def per_device(
    tokens,
    mixer_in_gain,
    query_weight,
    key_weight,
    value_weight,
    gate_weight,
    decay_logits,
    mixer_output,
    mixer_out_gain,
    channel_in_gain,
    gelu_weight,
    linear_weight,
    gelu_kernel,
    linear_kernel,
    gelu_bias,
    linear_bias,
    down_weight,
    channel_out_gain,
):
    core = lax.axis_index("c")
    token_rows = tokens[0]
    own = token_rows.shape[0]
    model = token_rows.shape[1]
    chips = lax.axis_size("x")
    bf16 = jnp.bfloat16

    first = jnp.concatenate([query_weight, key_weight, value_weight, gate_weight], axis=1)
    second = mixer_output.T
    width = gelu_weight.shape[1]

    def padded(value):
        return jnp.pad(value, ((0, 0), (0, PAD - width)))

    third = jnp.concatenate(
        [padded(gelu_weight), padded(linear_weight), padded(down_weight.T)], axis=1
    )
    taps = padded(
        jnp.concatenate([gelu_kernel, linear_kernel, gelu_bias[None], linear_bias[None]], axis=0)
    )
    first_z = gather_axis(first, "z")
    normed = rms_scaled(token_rows, mixer_in_gain).astype(bf16)
    normed_own = gather_axis(normed, "x").reshape(chips * own, model)
    second_z = gather_axis(after(second, first_z), "z")
    first_y = gather_axis(first_z, "y")
    third_z = gather_axis(after(third, second_z), "z")
    second_y = gather_axis(after(second_z, first_y), "y")
    normed_other = swap(normed_own)
    taps_other = swap(taps)
    third_y = gather_axis(after(third_z, second_y), "y")
    second_other = swap(second_y)
    third_other = swap(third_y)

    qkvg = rows_in_order(first_y)
    block = jnp.arange(chips, dtype=jnp.int32)[:, None] * (2 * own)
    inside = jnp.arange(own, dtype=jnp.int32)[None, :]
    own_positions = (block + inside + core * own).reshape(-1)
    other_positions = (block + inside + (1 - core) * own).reshape(-1)
    positions = jnp.concatenate([own_positions, other_positions])
    rows = jnp.concatenate([normed_own, normed_other], axis=0)
    projected = dot(rows, qkvg)
    queries = rotate(projected[:, :DK], positions).astype(bf16)
    keys = (rotate(projected[:, DK : 2 * DK], positions) * DK ** (-0.5)).astype(bf16)
    values = projected[:, 2 * DK : 2 * DK + DV].astype(bf16)
    gates = projected[:, 2 * DK + DV :]
    log_forward = jax.nn.log_sigmoid(decay_logits[0, 0])
    log_backward = jax.nn.log_sigmoid(decay_logits[1, 0])
    offset = (positions[:, None] - positions[None, :]).astype(jnp.float32)
    decay = jnp.exp(jnp.where(offset >= 0, offset * log_forward, -offset * log_backward))
    scores = (dot_nt(queries, keys) * decay).astype(bf16)
    retained = dot(scores, values)
    gated = (head_norm(retained) * jax.nn.silu(gates)).astype(bf16)
    half = chips * own
    gated_partner = swap(gated[half:])
    out_own = rows_in_order(second_y)
    out_other = rows_in_order(second_other)
    mixed = dot_nt(gated[:half], out_own) + dot_nt(gated_partner, out_other)

    def summed(partial):
        pieces = lax.all_to_all(
            partial.astype(bf16).reshape(chips, own, model), "x", 0, 0, tiled=True
        )
        return jnp.sum(pieces.astype(jnp.float32), axis=0)

    mix_sum = summed(mixed)
    after_mix = (token_rows.astype(jnp.float32) + rms_scaled(mix_sum, mixer_out_gain)).astype(bf16)
    channel_in = rms_scaled(after_mix, channel_in_gain).astype(bf16)
    channel_rows = gather_axis(channel_in, "x")
    edges = jnp.stack([channel_rows[:, 0], channel_rows[:, own - 1]], axis=0)
    edges_other = swap(edges)
    zero = jnp.zeros((1, model), bf16)
    firsts, lasts = edges_other[0], edges_other[1]
    before = jnp.where(core == 0, jnp.concatenate([zero, lasts[:-1]], 0), lasts)
    behind = jnp.where(core == 0, firsts, jnp.concatenate([firsts[1:], zero], 0))
    edge_rows = jnp.concatenate([before, behind], axis=0)
    third_full = [rows_in_order(third_y), rows_in_order(third_other)]
    hidden_parts = []
    flat_rows = channel_rows.reshape(half, model)
    for weights, tap in zip(third_full, (taps, taps_other)):
        up = weights[:, : 2 * PAD]
        main = dot(flat_rows, up).reshape(chips, own, 2 * PAD)
        edge = dot(edge_rows, up).reshape(2, chips, 1, 2 * PAD)
        prev = jnp.concatenate([edge[0], main[:, :-1]], axis=1)
        nxt = jnp.concatenate([main[:, 1:], edge[1]], axis=1)
        kernel = jnp.concatenate([tap[0:3], tap[3:6]], axis=1)
        bias = jnp.concatenate([tap[6], tap[7]], axis=0)
        conv = kernel[0] * prev + kernel[1] * main + kernel[2] * nxt + bias
        hidden = (jax.nn.gelu(conv[..., :PAD]) * conv[..., PAD:]).astype(bf16)
        hidden_parts.append(hidden.reshape(half, PAD))
    channel = sum(
        dot_nt(hidden, weights[:, 2 * PAD :])
        for hidden, weights in zip(hidden_parts, third_full)
    )
    channel_sum = summed(channel)
    result = (after_mix.astype(jnp.float32) + rms_scaled(channel_sum, channel_out_gain)).astype(
        bf16
    )
    return result[None]


def solution(mesh):
    fs = mesh.shape["fs"]
    tp = mesh.shape["tp"]
    split = Mesh(
        mesh.devices.reshape(mesh.shape["rep"], fs // 4, 4, tp // 2, 2),
        ("rep", "z", "y", "x", "c"),
    )
    in_specs = (
        P(("rep", "z", "y"), TP, None),
        P(),
        P(FS, TP),
        P(FS, TP),
        P(FS, TP),
        P(FS, TP),
        P(None, TP),
        P(TP, FS),
        P(),
        P(),
        P(FS, TP),
        P(FS, TP),
        P(None, TP),
        P(None, TP),
        P(TP),
        P(TP),
        P(TP, FS),
        P(),
    )
    out_specs = P(("rep", "z", "y"), TP, None)
    return jax.shard_map(
        per_device, mesh=split, in_specs=in_specs, out_specs=out_specs, check_vma=False
    )
```

```python
import functools

import jax
import jax.numpy as jnp
from jax import lax
from jax.experimental import pallas as pl
from jax.experimental.pallas import tpu as pltpu
from jax.sharding import Mesh
from jax.sharding import PartitionSpec as P


DK = 128
DV = 256
TP = ("x", "c")
FS = ("z", "y")
RING = ("rep", "z")
SWAP = ((0, 1), (1, 0))
PAD = 384
FIRST, SECOND, THIRD = 2 * DK + 2 * DV, DV, 3 * PAD
Z_SHIFTS = (4, 3, 2, 1, 0, -1, -2, -3)
Z_ISSUE = (4, -3, 3, -2, 2, -1, 1)
Y_SHIFTS = (0, 1, 2, -1)
Y_ISSUE = (2, 1, -1)
epsilon = 1e-06
rope_base = 10000.0
bf16 = jnp.bfloat16
f32 = jnp.float32

VMEM = pl.BlockSpec(memory_space=pltpu.VMEM)
SMEM = pl.BlockSpec(memory_space=pltpu.SMEM)


def call(body, out_shapes, *args, flops=0, moved=0, smem=0, **options):
    specs = [SMEM] * smem + [VMEM] * (len(args) - smem)
    single = not isinstance(out_shapes, (list, tuple))
    return pl.pallas_call(
        body,
        out_shape=out_shapes,
        in_specs=specs,
        out_specs=VMEM if single else [VMEM] * len(out_shapes),
        cost_estimate=pl.CostEstimate(
            flops=max(flops, 1 << 20), bytes_accessed=max(moved, 1 << 20), transcendentals=0
        ),
        **options,
    )(*args)


def shape(dims, kind=bf16):
    return jax.ShapeDtypeStruct(dims, kind)


def permuted(value, axes, shift, size):
    return lax.ppermute(value, axes, [(i, (i + shift) % size) for i in range(size)])


def swap(value):
    return lax.ppermute(value, "c", SWAP)


def exchanged(value):
    return lax.all_to_all(value, "x", 0, 0, tiled=True)


def rms_rows(values, gain):
    return values * lax.rsqrt(jnp.mean(values * values, axis=-1, keepdims=True) + epsilon) * gain


def pack_body(width, q, k, v, g, mo, ge, li, dn, out):
    out[:, :DK] = q[...]
    out[:, DK : 2 * DK] = k[...]
    out[:, 2 * DK : 2 * DK + DV] = v[...]
    out[:, 2 * DK + DV : FIRST] = g[...]
    out[:, FIRST : FIRST + SECOND] = mo[...]
    gap = jnp.zeros((out.shape[0], PAD - width), bf16)
    for place, piece in enumerate((ge, li, dn)):
        at = FIRST + SECOND + place * PAD
        out[:, at : at + PAD] = jnp.concatenate([piece[...], gap], axis=1)


def first_norm_body(tokens, gain, out):
    rows = rms_rows(tokens[...].astype(f32), gain[...]).astype(bf16)
    for k in range(out.shape[0]):
        out[k] = rows


def ring_order_body(index, *refs):
    pieces, (one, two, three) = refs[:8], refs[8:]
    for shift, piece in zip(Z_SHIFTS, pieces):
        at = lax.rem(index[0] - shift + 8, 8)
        one[at] = piece[:, :FIRST]
        two[at] = piece[:, FIRST : FIRST + SECOND]
        three[at] = piece[:, FIRST + SECOND :]


def line_order_body(index, *refs):
    pieces, out = refs[:4], refs[4]
    for shift, piece in zip(Y_SHIFTS, pieces):
        at = lax.rem(index[0] - shift + 4, 4)
        for z in range(8):
            out[z, at] = piece[z]


def middle_body(pieces, tokens, out_gain, in_gain, after_mix, channel_in):
    mixed = pieces[0].astype(f32)
    for k in range(1, pieces.shape[0]):
        mixed = mixed + pieces[k].astype(f32)
    mix = (tokens[...].astype(f32) + rms_rows(mixed, out_gain[...])).astype(bf16)
    after_mix[...] = mix
    rows = rms_rows(mix.astype(f32), in_gain[...]).astype(bf16)
    for k in range(channel_in.shape[0]):
        channel_in[k] = rows


def final_body(pieces, after_mix, gain, out):
    total = pieces[0].astype(f32)
    for k in range(1, pieces.shape[0]):
        total = total + pieces[k].astype(f32)
    out[...] = (after_mix[...].astype(f32) + rms_rows(total, gain[...])).astype(bf16)


def rotate(values, positions):
    half_width = values.shape[-1] // 2
    frequency = 1.0 / rope_base ** (jnp.arange(half_width, dtype=f32) / half_width)
    angles = positions.astype(f32)[:, None] * frequency[None, :]
    cosine = jnp.cos(angles)
    sine_part = jnp.sin(angles)
    first_half = values[..., :half_width]
    second = values[..., half_width:]
    return jnp.concatenate(
        [first_half * cosine - second * sine_part, first_half * sine_part + second * cosine],
        axis=-1,
    )


def head_norm(values):
    centred = values - jnp.mean(values, axis=-1, keepdims=True)
    return centred * lax.rsqrt(jnp.mean(centred * centred, axis=-1, keepdims=True) + epsilon)


def dot(a, b):
    return jnp.dot(a, b, preferred_element_type=f32)


def dot_nt(a, b):
    return lax.dot_general(a, b, (((1,), (1,)), ((), ())), preferred_element_type=f32)


def line_gather(piece):
    got = {0: piece}
    for shift in Y_ISSUE:
        got[shift] = permuted(piece, "y", shift, 4)
    return [got[s] for s in Y_SHIFTS]


def in_line_order(pieces, y_index):
    columns = pieces[0].shape[-1]
    ordered = call(
        line_order_body, shape((8, 4, 32, columns)), y_index, *pieces, smem=1
    )
    return ordered.reshape(1024, columns)


def layer(
    tokens,
    mixer_in_gain,
    query_weight,
    key_weight,
    value_weight,
    gate_weight,
    decay_logits,
    mixer_output,
    mixer_out_gain,
    channel_in_gain,
    gelu_weight,
    linear_weight,
    gelu_kernel,
    linear_kernel,
    gelu_bias,
    linear_bias,
    down_weight,
    channel_out_gain,
):
    core = lax.axis_index("c")
    y_index = lax.axis_index("y").astype(jnp.int32)[None]
    z_index = lax.axis_index("z").astype(jnp.int32)[None]
    token_rows = tokens[0]
    own, model = token_rows.shape
    chips = lax.axis_size("x")
    width = gelu_weight.shape[1]

    def gain_row(gain):
        return gain.reshape(1, -1)

    packed = call(
        functools.partial(pack_body, width),
        shape((32, FIRST + SECOND + THIRD)),
        query_weight,
        key_weight,
        value_weight,
        gate_weight,
        mixer_output.T,
        gelu_weight,
        linear_weight,
        down_weight.T,
    )
    got = {0: packed}
    for shift in Z_ISSUE:
        got[shift] = permuted(packed, RING, shift, 16)
    spread = call(
        first_norm_body, shape((chips, own, model)), token_rows, gain_row(mixer_in_gain)
    )
    normed_own = exchanged(spread).reshape(chips * own, model)
    normed_other = swap(normed_own)

    def padded(value):
        return jnp.pad(value, ((0, 0), (0, PAD - width)))

    taps = padded(
        jnp.concatenate([gelu_kernel, linear_kernel, gelu_bias[None], linear_bias[None]], axis=0)
    )
    taps_other = swap(taps)

    first_z, second_z, third_z = call(
        ring_order_body,
        [shape((8, 32, FIRST)), shape((8, 32, SECOND)), shape((8, 32, THIRD))],
        z_index,
        *[got[s] for s in Z_SHIFTS],
        smem=1,
    )
    first_pieces = line_gather(first_z)
    second_pieces = line_gather(second_z)
    third_pieces = line_gather(third_z)
    qkvg = in_line_order(first_pieces, y_index)

    block = jnp.arange(chips, dtype=jnp.int32)[:, None] * (2 * own)
    inside = jnp.arange(own, dtype=jnp.int32)[None, :]
    own_positions = (block + inside + core * own).reshape(-1)
    other_positions = (block + inside + (1 - core) * own).reshape(-1)
    positions = jnp.concatenate([own_positions, other_positions])
    rows = jnp.concatenate([normed_own, normed_other], axis=0)
    projected = dot(rows, qkvg)
    queries = rotate(projected[:, :DK], positions).astype(bf16)
    keys = (rotate(projected[:, DK : 2 * DK], positions) * DK ** (-0.5)).astype(bf16)
    values = projected[:, 2 * DK : 2 * DK + DV].astype(bf16)
    gates = projected[:, 2 * DK + DV :]
    log_forward = jax.nn.log_sigmoid(decay_logits[0, 0])
    log_backward = jax.nn.log_sigmoid(decay_logits[1, 0])
    offset = (positions[:, None] - positions[None, :]).astype(f32)
    decay = jnp.exp(jnp.where(offset >= 0, offset * log_forward, -offset * log_backward))
    scores = (dot_nt(queries, keys) * decay).astype(bf16)
    retained = dot(scores, values)
    gated = (head_norm(retained) * jax.nn.silu(gates)).astype(bf16)
    half = chips * own
    gated_partner = swap(gated[half:])
    out_own = in_line_order(second_pieces, y_index)
    out_other = swap(out_own)
    mixed = dot_nt(gated[:half], out_own) + dot_nt(gated_partner, out_other)
    mix_pieces = exchanged(mixed.astype(bf16).reshape(chips, own, model))
    after_mix, channel_spread = call(
        middle_body,
        [shape((own, model)), shape((chips, own, model))],
        mix_pieces,
        token_rows,
        gain_row(mixer_out_gain),
        gain_row(channel_in_gain),
    )
    channel_rows = exchanged(channel_spread)
    third_own = in_line_order(third_pieces, y_index)
    third_other = swap(third_own)

    edges = jnp.stack([channel_rows[:, 0], channel_rows[:, own - 1]], axis=0)
    edges_other = swap(edges)
    zero = jnp.zeros((1, model), bf16)
    firsts, lasts = edges_other[0], edges_other[1]
    before = jnp.where(core == 0, jnp.concatenate([zero, lasts[:-1]], 0), lasts)
    behind = jnp.where(core == 0, firsts, jnp.concatenate([firsts[1:], zero], 0))
    edge_rows = jnp.concatenate([before, behind], axis=0)
    hidden_parts = []
    flat_rows = channel_rows.reshape(half, model)
    for weights, tap in ((third_own, taps), (third_other, taps_other)):
        up = weights[:, : 2 * PAD]
        main = dot(flat_rows, up).reshape(chips, own, 2 * PAD)
        edge = dot(edge_rows, up).reshape(2, chips, 1, 2 * PAD)
        prev = jnp.concatenate([edge[0], main[:, :-1]], axis=1)
        nxt = jnp.concatenate([main[:, 1:], edge[1]], axis=1)
        kernel = jnp.concatenate([tap[0:3], tap[3:6]], axis=1)
        bias = jnp.concatenate([tap[6], tap[7]], axis=0)
        conv = kernel[0] * prev + kernel[1] * main + kernel[2] * nxt + bias
        hidden = (jax.nn.gelu(conv[..., :PAD]) * conv[..., PAD:]).astype(bf16)
        hidden_parts.append(hidden.reshape(half, PAD))
    channel = sum(
        dot_nt(hidden, weights[:, 2 * PAD :])
        for hidden, weights in zip(hidden_parts, (third_own, third_other))
    )
    channel_pieces = exchanged(channel.astype(bf16).reshape(chips, own, model))
    result = call(
        final_body, shape((own, model)), channel_pieces, after_mix, gain_row(channel_out_gain)
    )
    return result[None]


def solution(mesh):
    fs = mesh.shape["fs"]
    tp = mesh.shape["tp"]
    split = Mesh(
        mesh.devices.reshape(mesh.shape["rep"], fs // 4, 4, tp // 2, 2),
        ("rep", "z", "y", "x", "c"),
    )
    in_specs = (
        P(("rep", "z", "y"), TP, None),
        P(),
        P(FS, TP),
        P(FS, TP),
        P(FS, TP),
        P(FS, TP),
        P(None, TP),
        P(TP, FS),
        P(),
        P(),
        P(FS, TP),
        P(FS, TP),
        P(None, TP),
        P(None, TP),
        P(TP),
        P(TP),
        P(TP, FS),
        P(),
    )
    out_specs = P(("rep", "z", "y"), TP, None)
    return jax.shard_map(layer, mesh=split, in_specs=in_specs, out_specs=out_specs, check_vma=False)
```

```python
import functools

import jax
import jax.numpy as jnp
from jax import lax
from jax.experimental import pallas as pl
from jax.experimental.pallas import tpu as pltpu
from jax.sharding import Mesh
from jax.sharding import PartitionSpec as P


DK = 128
DV = 256
TP = ("x", "c")
FS = ("z", "y")
RING = ("rep", "z")
SWAP = ((0, 1), (1, 0))
PAD = 384
FIRST, SECOND, THIRD = 2 * DK + 2 * DV, DV, 3 * PAD
Z_SHIFTS = (4, 3, 2, 1, 0, -1, -2, -3)
Z_ISSUE = (4, -3, 3, -2, 2, -1, 1)
Y_SHIFTS = (0, 1, 2, -1)
Y_ISSUE = (2, 1, -1)
epsilon = 1e-06
rope_base = 10000.0
bf16 = jnp.bfloat16
f32 = jnp.float32

VMEM = pl.BlockSpec(memory_space=pltpu.VMEM)
SMEM = pl.BlockSpec(memory_space=pltpu.SMEM)


def call(body, out_shapes, *args, flops=0, smem=0, scratch=()):
    specs = [SMEM] * smem + [VMEM] * (len(args) - smem)
    single = not isinstance(out_shapes, (list, tuple))
    return pl.pallas_call(
        body,
        out_shape=out_shapes,
        in_specs=specs,
        out_specs=VMEM if single else [VMEM] * len(out_shapes),
        scratch_shapes=list(scratch),
        cost_estimate=pl.CostEstimate(
            flops=max(flops, 1 << 24), bytes_accessed=1 << 21, transcendentals=0
        ),
    )(*args)


def shape(dims, kind=bf16):
    return jax.ShapeDtypeStruct(dims, kind)


def permuted(value, axes, shift, size):
    return lax.ppermute(value, axes, [(i, (i + shift) % size) for i in range(size)])


def swap(value):
    return lax.ppermute(value, "c", SWAP)


def exchanged(value):
    return lax.all_to_all(value, "x", 0, 0, tiled=True)


def rms_rows(values, gain):
    return values * lax.rsqrt(jnp.mean(values * values, axis=-1, keepdims=True) + epsilon) * gain


def to_pieces(values):
    return jnp.concatenate(
        [values[:, z * 128 + y * 32 : z * 128 + y * 32 + 32] for y in range(4) for z in range(8)],
        axis=1,
    )


def from_pieces(values):
    return jnp.concatenate(
        [values[:, y * 256 + z * 32 : y * 256 + z * 32 + 32] for z in range(8) for y in range(4)],
        axis=1,
    )


def pack_body(width, q, k, v, g, mo, ge, li, dn, out):
    out[:, :DK] = q[...]
    out[:, DK : 2 * DK] = k[...]
    out[:, 2 * DK : 2 * DK + DV] = v[...]
    out[:, 2 * DK + DV : FIRST] = g[...]
    out[:, FIRST : FIRST + SECOND] = mo[...]
    gap = jnp.zeros((out.shape[0], PAD - width), bf16)
    for place, piece in enumerate((ge, li, dn)):
        at = FIRST + SECOND + place * PAD
        out[:, at : at + PAD] = jnp.concatenate([piece[...], gap], axis=1)


def taps_body(width, ge_kernel, li_kernel, ge_bias, li_bias, out):
    out[...] = jnp.zeros(out.shape, f32)
    out[0:3, :width] = ge_kernel[...]
    out[3:6, :width] = li_kernel[...]
    out[6:7, :width] = ge_bias[...]
    out[7:8, :width] = li_bias[...]


def first_norm_body(tokens, gain, out):
    rows = to_pieces(rms_rows(tokens[...].astype(f32), gain[...])).astype(bf16)
    for k in range(out.shape[0]):
        out[k] = rows


def ring_order_body(index, *refs):
    pieces, (one, two, three) = refs[:8], refs[8:]
    for shift, piece in zip(Z_SHIFTS, pieces):
        at = lax.rem(index[0] - shift + 8, 8)
        one[at] = piece[:, :FIRST]
        two[at] = piece[:, FIRST : FIRST + SECOND]
        three[at] = piece[:, FIRST + SECOND :]


def line_order_body(index, *refs):
    pieces, out = refs[:4], refs[4]
    for shift, piece in zip(Y_SHIFTS, pieces):
        out[lax.rem(index[0] - shift + 4, 4)] = piece[...]


def summed(pieces):
    total = pieces[0].astype(f32)
    for k in range(1, pieces.shape[0]):
        total = total + pieces[k].astype(f32)
    inverse = lax.rsqrt(jnp.mean(total * total, axis=-1, keepdims=True) + epsilon)
    return from_pieces(total * inverse)


def middle_body(pieces, tokens, out_gain, in_gain, after_mix, channel_in):
    mix = (tokens[...].astype(f32) + summed(pieces) * out_gain[...]).astype(bf16)
    after_mix[...] = mix
    rows = to_pieces(rms_rows(mix.astype(f32), in_gain[...])).astype(bf16)
    for k in range(channel_in.shape[0]):
        channel_in[k] = rows


def final_body(pieces, after_mix, gain, out):
    out[...] = (after_mix[...].astype(f32) + summed(pieces) * gain[...]).astype(bf16)


def log_sigmoid_tile(logit):
    value = jnp.full((8, 128), logit, f32)
    tile = jnp.minimum(value, 0.0) - jnp.log1p(jnp.exp(-jnp.abs(value)))
    return tile[0:1, 0:1]


def attend_body(
    index, logits, own, other, p0, p1, p2, p3, cosine, sine, out_own, out_other, w, qs, ks, vs, gs
):
    y, core = index[0], index[1]
    for shift, piece in zip(Y_SHIFTS, (p0, p1, p2, p3)):
        at = lax.rem(y - shift + 4, 4) * 256
        w[pl.ds(pl.multiple_of(at, 256), 256), :] = piece[...]
    step = 256
    for r in range(0, 1024, step):
        rows = own[r : r + step, :] if r < 512 else other[r - 512 : r - 512 + step, :]
        projected = dot(rows, w[...])
        cos, sin = cosine[r : r + step, :], sine[r : r + step, :]
        q = projected[:, :DK]
        k = projected[:, DK : 2 * DK]
        qs[r : r + step, :] = (q * cos + pltpu.roll(q, DK // 2, 1) * sin).astype(bf16)
        ks[r : r + step, :] = (
            (k * cos + pltpu.roll(k, DK // 2, 1) * sin) * DK ** (-0.5)
        ).astype(bf16)
        vs[r : r + step, :] = projected[:, 2 * DK : 2 * DK + DV].astype(bf16)
        gs[r : r + step, :] = projected[:, 2 * DK + DV :]
    forward = log_sigmoid_tile(logits[0])
    backward = log_sigmoid_tile(logits[1])
    lag = (
        lax.broadcasted_iota(jnp.int32, (128, 128), 0)
        - lax.broadcasted_iota(jnp.int32, (128, 128), 1)
    ).astype(f32)
    ahead, behind = lag * forward, lag * -backward
    side = ((2 * core - 1) * 128).astype(f32)
    for r in range(8):
        decays = []
        for c in range(8):
            gap = float((r % 4 - c % 4) * 256)
            if r < 4 <= c:
                gap = gap + side
            if c < 4 <= r:
                gap = gap - side
            decays.append(jnp.exp(jnp.minimum(ahead + gap * forward, behind - gap * backward)))
        rows = slice(r * 128, r * 128 + 128)
        scores = dot_nt(qs[rows, :], ks[...])
        weighted = (scores * jnp.concatenate(decays, axis=1)).astype(bf16)
        kept = head_norm(dot(weighted, vs[...]))
        gate = gs[rows, :]
        gated = (kept * (gate / (1.0 + jnp.exp(-gate)))).astype(bf16)
        if r < 4:
            out_own[rows, :] = gated
        else:
            out_other[r * 128 - 512 : r * 128 - 384, :] = gated


def output_body(index, mine, theirs, p0, p1, p2, p3, out):
    for shift, piece in zip(Y_SHIFTS, (p0, p1, p2, p3)):
        at = lax.rem(index[0] - shift + 4, 4) * 256
        part = dot_nt(mine[...], piece[:, :DV]) + dot_nt(theirs[...], piece[:, DV:])
        out[:, pl.ds(pl.multiple_of(at, 256), 256)] = part.astype(bf16)


def feed_body(index, rows, edges, mine, theirs, my_taps, their_taps, out, hidden):
    core = index[0]
    line = lax.broadcasted_iota(jnp.int32, (128, 1), 0)
    for part, (weights, taps) in enumerate(((mine, my_taps), (theirs, their_taps))):
        kernel = [
            jnp.concatenate([taps[t : t + 1, :], taps[t + 3 : t + 4, :]], axis=1) for t in range(3)
        ]
        bias = jnp.concatenate([taps[6:7, :], taps[7:8, :]], axis=1)
        edge = dot(edges[...], weights[:, : 2 * PAD])
        none = jnp.zeros((1, 2 * PAD), f32)
        for x in range(4):
            main = dot(rows[x * 128 : x * 128 + 128, :], weights[:, : 2 * PAD])
            last = edge[4 + x : 5 + x, :]
            sooner = edge[3 + x : 4 + x, :] if x else none
            first = edge[x : x + 1, :]
            later = edge[x + 1 : x + 2, :] if x < 3 else none
            before = jnp.where(core == 0, sooner, last)
            after = jnp.where(core == 0, first, later)
            prev = jnp.where(line == 0, before, pltpu.roll(main, 1, 0))
            nxt = jnp.where(line == 127, after, pltpu.roll(main, 127, 0))
            conv = kernel[0] * prev + kernel[1] * main + kernel[2] * nxt + bias
            value = conv[:, :PAD]
            bent = value * (
                0.5 + 0.5 * jnp.tanh(0.7978845608028654 * (value + 0.044715 * value**3))
            )
            hidden[x * 128 : x * 128 + 128, part * PAD : part * PAD + PAD] = (
                bent * conv[:, PAD:]
            ).astype(bf16)
    for d in range(0, 1024, 256):
        total = dot_nt(hidden[:, :PAD], mine[d : d + 256, 2 * PAD :]) + dot_nt(
            hidden[:, PAD:], theirs[d : d + 256, 2 * PAD :]
        )
        out[:, d : d + 256] = total.astype(bf16)


def head_norm(values):
    centred = values - jnp.mean(values, axis=-1, keepdims=True)
    return centred * lax.rsqrt(jnp.mean(centred * centred, axis=-1, keepdims=True) + epsilon)


def dot(a, b):
    return jnp.dot(a, b, preferred_element_type=f32)


def dot_nt(a, b):
    return lax.dot_general(a, b, (((1,), (1,)), ((), ())), preferred_element_type=f32)


def line_gather(piece):
    got = {0: piece}
    for shift in Y_ISSUE:
        got[shift] = permuted(piece, "y", shift, 4)
    return [got[s].reshape(256, piece.shape[-1]) for s in Y_SHIFTS]


def rope_tables(core, chips, own):
    block = jnp.arange(chips, dtype=jnp.int32)[:, None] * (2 * own)
    inside = jnp.arange(own, dtype=jnp.int32)[None, :]
    positions = jnp.concatenate(
        [(block + inside + side * own).reshape(-1) for side in (core, 1 - core)]
    )
    half = DK // 2
    frequency = 1.0 / rope_base ** (jnp.arange(half, dtype=f32) / half)
    angles = positions.astype(f32)[:, None] * frequency[None, :]
    cosine, sine = jnp.cos(angles), jnp.sin(angles)
    return jnp.concatenate([cosine, cosine], axis=1), jnp.concatenate([-sine, sine], axis=1)


def layer(
    tokens,
    mixer_in_gain,
    query_weight,
    key_weight,
    value_weight,
    gate_weight,
    decay_logits,
    mixer_output,
    mixer_out_gain,
    channel_in_gain,
    gelu_weight,
    linear_weight,
    gelu_kernel,
    linear_kernel,
    gelu_bias,
    linear_bias,
    down_weight,
    channel_out_gain,
):
    core = lax.axis_index("c").astype(jnp.int32)
    y_index = lax.axis_index("y").astype(jnp.int32)
    z_index = lax.axis_index("z").astype(jnp.int32)
    token_rows = tokens[0]
    own, model = token_rows.shape
    chips = lax.axis_size("x")
    half = chips * own
    width = gelu_weight.shape[1]

    def row(vector):
        return vector.reshape(1, -1)

    packed = call(
        functools.partial(pack_body, width),
        shape((32, FIRST + SECOND + THIRD)),
        query_weight,
        key_weight,
        value_weight,
        gate_weight,
        mixer_output.T,
        gelu_weight,
        linear_weight,
        down_weight.T,
    )
    got = {0: packed}
    for shift in Z_ISSUE:
        got[shift] = permuted(packed, RING, shift, 16)
    spread = call(first_norm_body, shape((chips, own, model)), token_rows, row(mixer_in_gain))
    normed_own = exchanged(spread).reshape(half, model)
    normed_other = swap(normed_own)
    first_z, second_z, third_z = call(
        ring_order_body,
        [shape((8, 32, FIRST)), shape((8, 32, SECOND)), shape((8, 32, THIRD))],
        z_index[None],
        *[got[s] for s in Z_SHIFTS],
        smem=1,
    )
    first_pieces = line_gather(first_z)
    second_both = jnp.concatenate([second_z, swap(second_z)], axis=2)
    second_pieces = line_gather(second_both)
    third_pieces = line_gather(third_z)
    cosine, sine = rope_tables(core, chips, own)
    gated_own, gated_other = call(
        attend_body,
        [shape((half, DV)), shape((half, DV))],
        jnp.stack([y_index, core]),
        decay_logits[:, 0],
        normed_own,
        normed_other,
        *first_pieces,
        cosine,
        sine,
        flops=1 << 32,
        smem=2,
        scratch=[
            pltpu.VMEM((model, FIRST), bf16),
            pltpu.VMEM((2 * half, DK), bf16),
            pltpu.VMEM((2 * half, DK), bf16),
            pltpu.VMEM((2 * half, DV), bf16),
            pltpu.VMEM((2 * half, DV), f32),
        ],
    )
    gated_partner = swap(gated_other)
    mixed = call(
        output_body,
        shape((half, model)),
        y_index[None],
        gated_own,
        gated_partner,
        *second_pieces,
        flops=1 << 30,
        smem=1,
    )
    mix_pieces = exchanged(mixed.reshape(chips, own, model))
    taps = call(
        functools.partial(taps_body, width),
        shape((8, PAD), f32),
        gelu_kernel,
        linear_kernel,
        row(gelu_bias),
        row(linear_bias),
    )
    taps_other = swap(taps)
    after_mix, channel_spread = call(
        middle_body,
        [shape((own, model)), shape((chips, own, model))],
        mix_pieces,
        token_rows,
        row(mixer_out_gain),
        row(channel_in_gain),
    )
    channel_rows = exchanged(channel_spread)
    third_own = call(
        line_order_body, shape((4, 256, THIRD)), y_index[None], *third_pieces, smem=1
    ).reshape(model, THIRD)
    third_other = swap(third_own)
    edges = jnp.concatenate([channel_rows[:, 0], channel_rows[:, own - 1]], axis=0)
    edges_other = swap(edges)
    channel = call(
        feed_body,
        shape((half, model)),
        core[None],
        channel_rows.reshape(half, model),
        edges_other,
        third_own,
        third_other,
        taps,
        taps_other,
        flops=1 << 32,
        smem=1,
        scratch=[pltpu.VMEM((half, 2 * PAD), bf16)],
    )
    channel_pieces = exchanged(channel.reshape(chips, own, model))
    result = call(final_body, shape((own, model)), channel_pieces, after_mix, row(channel_out_gain))
    return result[None]


def solution(mesh):
    fs = mesh.shape["fs"]
    tp = mesh.shape["tp"]
    split = Mesh(
        mesh.devices.reshape(mesh.shape["rep"], fs // 4, 4, tp // 2, 2),
        ("rep", "z", "y", "x", "c"),
    )
    in_specs = (
        P(("rep", "z", "y"), TP, None),
        P(),
        P(FS, TP),
        P(FS, TP),
        P(FS, TP),
        P(FS, TP),
        P(None, TP),
        P(TP, FS),
        P(),
        P(),
        P(FS, TP),
        P(FS, TP),
        P(None, TP),
        P(None, TP),
        P(TP),
        P(TP),
        P(TP, FS),
        P(),
    )
    out_specs = P(("rep", "z", "y"), TP, None)
    return jax.shard_map(layer, mesh=split, in_specs=in_specs, out_specs=out_specs, check_vma=False)
```

```python
import functools

import jax
import jax.numpy as jnp
import numpy as np
from jax import lax
from jax.experimental import pallas as pl
from jax.experimental.pallas import tpu as pltpu
from jax.sharding import Mesh
from jax.sharding import PartitionSpec as P


DK = 128
DV = 256
TP = ("x", "c")
FS = ("z", "y")
RING = ("rep", "z")
SWAP = ((0, 1), (1, 0))
PAD = 384
FIRST, SECOND, THIRD = 2 * DK + 2 * DV, DV, 3 * PAD
Z_SHIFTS = (4, 3, 2, 1, 0, -1, -2, -3)
Z_ISSUE = (4, -3, 3, -2, 2, -1, 1)
Y_SHIFTS = (0, 1, 2, -1)
Y_ISSUE = (2, 1, -1)
epsilon = 1e-06
rope_base = 10000.0
bf16 = jnp.bfloat16
f32 = jnp.float32

VMEM = pl.BlockSpec(memory_space=pltpu.VMEM)
SMEM = pl.BlockSpec(memory_space=pltpu.SMEM)


def call(body, out_shapes, *args, flops=0, smem=0, scratch=()):
    specs = [SMEM] * smem + [VMEM] * (len(args) - smem)
    single = not isinstance(out_shapes, (list, tuple))
    return pl.pallas_call(
        body,
        out_shape=out_shapes,
        in_specs=specs,
        out_specs=VMEM if single else [VMEM] * len(out_shapes),
        scratch_shapes=list(scratch),
        cost_estimate=pl.CostEstimate(
            flops=max(flops, 1 << 24), bytes_accessed=1 << 21, transcendentals=0
        ),
    )(*args)


def shape(dims, kind=bf16):
    return jax.ShapeDtypeStruct(dims, kind)


def permuted(value, axes, shift, size):
    return lax.ppermute(value, axes, [(i, (i + shift) % size) for i in range(size)])


def swap(value):
    return lax.ppermute(value, "c", SWAP)


def exchanged(value):
    return lax.all_to_all(value, "x", 0, 0, tiled=True)


def rms_rows(values, gain):
    return values * lax.rsqrt(jnp.mean(values * values, axis=-1, keepdims=True) + epsilon) * gain


def pack_body(width, q, k, v, g, mo, ge, li, dn, out):
    out[:, :DK] = q[...]
    out[:, DK : 2 * DK] = k[...]
    out[:, 2 * DK : 2 * DK + DV] = v[...]
    out[:, 2 * DK + DV : FIRST] = g[...]
    out[:, FIRST : FIRST + SECOND] = mo[...]
    gap = jnp.zeros((out.shape[0], PAD - width), bf16)
    for place, piece in enumerate((ge, li, dn)):
        at = FIRST + SECOND + place * PAD
        out[:, at : at + PAD] = jnp.concatenate([piece[...], gap], axis=1)


def taps_body(width, ge_kernel, li_kernel, ge_bias, li_bias, out):
    out[...] = jnp.zeros(out.shape, f32)
    out[0:3, :width] = ge_kernel[...]
    out[3:6, :width] = li_kernel[...]
    out[6:7, :width] = ge_bias[...]
    out[7:8, :width] = li_bias[...]


def first_norm_body(tokens, gain, out):
    rows = rms_rows(tokens[...].astype(f32), gain[...]).astype(bf16)
    for k in range(out.shape[0]):
        out[k] = rows


def ring_order_body(index, *refs):
    pieces, (one, two, three) = refs[:8], refs[8:]
    for shift, piece in zip(Z_SHIFTS, pieces):
        at = lax.rem(index[0] - shift + 8, 8)
        one[at] = piece[:, :FIRST]
        two[at] = piece[:, FIRST : FIRST + SECOND]
        three[at] = piece[:, FIRST + SECOND :]


def line_order_body(index, *refs):
    pieces, out = refs[:4], refs[4]
    for shift, piece in zip(Y_SHIFTS, pieces):
        at = lax.rem(index[0] - shift + 4, 4)
        for z in range(8):
            out[z, at] = piece[z * 32 : z * 32 + 32, :]


def summed(pieces):
    total = pieces[0].astype(f32)
    for k in range(1, pieces.shape[0]):
        total = total + pieces[k].astype(f32)
    return total * lax.rsqrt(jnp.mean(total * total, axis=-1, keepdims=True) + epsilon)


def middle_body(pieces, tokens, out_gain, in_gain, after_mix, channel_in):
    mix = (tokens[...].astype(f32) + summed(pieces) * out_gain[...]).astype(bf16)
    after_mix[...] = mix
    rows = rms_rows(mix.astype(f32), in_gain[...]).astype(bf16)
    for k in range(channel_in.shape[0]):
        channel_in[k] = rows


def final_body(pieces, after_mix, gain, out):
    out[...] = (after_mix[...].astype(f32) + summed(pieces) * gain[...]).astype(bf16)


def log_sigmoid_tile(logit):
    value = jnp.full((8, 128), logit, f32)
    tile = jnp.minimum(value, 0.0) - jnp.log1p(jnp.exp(-jnp.abs(value)))
    return tile[0:1, 0:1]


def attend_body(
    index, logits, own, other, p0, p1, p2, p3, frequency, out_own, out_other, w, qs, ks, vs, gs
):
    y, core = index[0], index[1]
    for shift, piece in zip(Y_SHIFTS, (p0, p1, p2, p3)):
        at = lax.rem(y - shift + 4, 4) * 32
        for z in range(8):
            place = pl.ds(pl.multiple_of(z * 128 + at, 32), 32)
            w[place, :] = piece[z * 32 : z * 32 + 32, :]
    inside = lax.broadcasted_iota(jnp.int32, (128, DK), 0).astype(f32) * frequency[...]
    cos_in, sin_in = jnp.cos(inside), jnp.sin(inside)
    block = lax.broadcasted_iota(jnp.int32, (8, DK), 0)
    base = (block % 4) * 256 + jnp.where(block < 4, core, 1 - core) * 128
    start = base.astype(f32) * frequency[...]
    cos_at, sin_at = jnp.cos(start), jnp.sin(start)
    sign = jnp.where(lax.broadcasted_iota(jnp.int32, (128, DK), 1) < DK // 2, -1.0, 1.0)
    cos_turn, sin_turn = cos_in * sign, sin_in * sign

    def tables(r):
        c, s = cos_at[r : r + 1, :], sin_at[r : r + 1, :]
        return c * cos_in - s * sin_in, s * cos_turn + c * sin_turn

    step = 256
    for r in range(0, 1024, step):
        rows = own[r : r + step, :] if r < 512 else other[r - 512 : r - 512 + step, :]
        projected = dot(rows, w[...])
        pair = [tables(b) for b in range(r // 128, (r + step) // 128)]
        cos = jnp.concatenate([p[0] for p in pair], axis=0)
        sin = jnp.concatenate([p[1] for p in pair], axis=0)
        q = projected[:, :DK]
        k = projected[:, DK : 2 * DK]
        qs[r : r + step, :] = (q * cos + pltpu.roll(q, DK // 2, 1) * sin).astype(bf16)
        ks[r : r + step, :] = (
            (k * cos + pltpu.roll(k, DK // 2, 1) * sin) * DK ** (-0.5)
        ).astype(bf16)
        vs[r : r + step, :] = projected[:, 2 * DK : 2 * DK + DV].astype(bf16)
        gs[r : r + step, :] = projected[:, 2 * DK + DV :]
    forward = log_sigmoid_tile(logits[0])
    backward = log_sigmoid_tile(logits[1])
    lag = (
        lax.broadcasted_iota(jnp.int32, (128, 128), 0)
        - lax.broadcasted_iota(jnp.int32, (128, 128), 1)
    ).astype(f32)
    ahead, behind = lag * forward, lag * -backward
    side = ((2 * core - 1) * 128).astype(f32)
    for r in range(8):
        decays = []
        for c in range(8):
            gap = float((r % 4 - c % 4) * 256)
            if r < 4 <= c:
                gap = gap + side
            if c < 4 <= r:
                gap = gap - side
            decays.append(jnp.exp(jnp.minimum(ahead + gap * forward, behind - gap * backward)))
        rows = slice(r * 128, r * 128 + 128)
        scores = dot_nt(qs[rows, :], ks[...])
        weighted = (scores * jnp.concatenate(decays, axis=1)).astype(bf16)
        kept = head_norm(dot(weighted, vs[...]))
        gate = gs[rows, :]
        gated = (kept * (gate / (1.0 + jnp.exp(-gate)))).astype(bf16)
        if r < 4:
            out_own[rows, :] = gated
        else:
            out_other[r * 128 - 512 : r * 128 - 384, :] = gated


def spread_body(mine, theirs, out):
    for y in range(out.shape[0]):
        out[y, :, :, :DV] = mine[...]
        out[y, :, :, DV:] = theirs[...]


def output_body(mine, theirs, pieces, out, w):
    for y in range(4):
        for z in range(8):
            at = z * 128 + y * 32
            w[at : at + 32, :] = pieces[y, z]
    step = 256
    for d in range(0, 1024, step):
        part = dot_nt(mine[...], w[d : d + step, :DV]) + dot_nt(theirs[...], w[d : d + step, DV:])
        out[:, d : d + step] = part.astype(bf16)


def feed_body(index, rows, edges, mine, theirs, my_taps, their_taps, out, hidden):
    core = index[0]
    line = lax.broadcasted_iota(jnp.int32, (128, 1), 0)
    for part, (weights, taps) in enumerate(((mine, my_taps), (theirs, their_taps))):
        kernel = [
            jnp.concatenate([taps[t : t + 1, :], taps[t + 3 : t + 4, :]], axis=1) for t in range(3)
        ]
        bias = jnp.concatenate([taps[6:7, :], taps[7:8, :]], axis=1)
        edge = dot(edges[...], weights[:, : 2 * PAD])
        none = jnp.zeros((1, 2 * PAD), f32)
        for x in range(4):
            main = dot(rows[x * 128 : x * 128 + 128, :], weights[:, : 2 * PAD])
            last = edge[4 + x : 5 + x, :]
            sooner = edge[3 + x : 4 + x, :] if x else none
            first = edge[x : x + 1, :]
            later = edge[x + 1 : x + 2, :] if x < 3 else none
            before = jnp.where(core == 0, sooner, last)
            after = jnp.where(core == 0, first, later)
            prev = jnp.where(line == 0, before, pltpu.roll(main, 1, 0))
            nxt = jnp.where(line == 127, after, pltpu.roll(main, 127, 0))
            conv = kernel[0] * prev + kernel[1] * main + kernel[2] * nxt + bias
            value = conv[:, :PAD]
            bent = value * (
                0.5 + 0.5 * jnp.tanh(0.7978845608028654 * (value + 0.044715 * value**3))
            )
            hidden[x * 128 : x * 128 + 128, part * PAD : part * PAD + PAD] = (
                bent * conv[:, PAD:]
            ).astype(bf16)
    for d in range(0, 1024, 256):
        total = dot_nt(hidden[:, :PAD], mine[d : d + 256, 2 * PAD :]) + dot_nt(
            hidden[:, PAD:], theirs[d : d + 256, 2 * PAD :]
        )
        out[:, d : d + 256] = total.astype(bf16)


def head_norm(values):
    centred = values - jnp.mean(values, axis=-1, keepdims=True)
    return centred * lax.rsqrt(jnp.mean(centred * centred, axis=-1, keepdims=True) + epsilon)


def dot(a, b):
    return jnp.dot(a, b, preferred_element_type=f32)


def dot_nt(a, b):
    return lax.dot_general(a, b, (((1,), (1,)), ((), ())), preferred_element_type=f32)


def line_gather(piece):
    got = {0: piece}
    for shift in Y_ISSUE:
        got[shift] = permuted(piece, "y", shift, 4)
    return [got[s].reshape(256, piece.shape[-1]) for s in Y_SHIFTS]


def rope_frequency():
    half = DK // 2
    frequency = 1.0 / rope_base ** (np.arange(half, dtype=np.float32) / half)
    return jnp.asarray(np.tile(frequency.astype(np.float32), 2)[None])


def layer(
    tokens,
    mixer_in_gain,
    query_weight,
    key_weight,
    value_weight,
    gate_weight,
    decay_logits,
    mixer_output,
    mixer_out_gain,
    channel_in_gain,
    gelu_weight,
    linear_weight,
    gelu_kernel,
    linear_kernel,
    gelu_bias,
    linear_bias,
    down_weight,
    channel_out_gain,
):
    core = lax.axis_index("c").astype(jnp.int32)
    y_index = lax.axis_index("y").astype(jnp.int32)
    z_index = lax.axis_index("z").astype(jnp.int32)
    token_rows = tokens[0]
    own, model = token_rows.shape
    chips = lax.axis_size("x")
    half = chips * own
    width = gelu_weight.shape[1]

    def row(vector):
        return vector.reshape(1, -1)

    packed = call(
        functools.partial(pack_body, width),
        shape((32, FIRST + SECOND + THIRD)),
        query_weight,
        key_weight,
        value_weight,
        gate_weight,
        mixer_output.T,
        gelu_weight,
        linear_weight,
        down_weight.T,
    )
    got = {0: packed}
    for shift in Z_ISSUE:
        got[shift] = permuted(packed, RING, shift, 16)
    spread = call(first_norm_body, shape((chips, own, model)), token_rows, row(mixer_in_gain))
    normed_own = exchanged(spread).reshape(half, model)
    normed_other = swap(normed_own)
    first_z, second_z, third_z = call(
        ring_order_body,
        [shape((8, 32, FIRST)), shape((8, 32, SECOND)), shape((8, 32, THIRD))],
        z_index[None],
        *[got[s] for s in Z_SHIFTS],
        smem=1,
    )
    first_pieces = line_gather(first_z)
    second_spread = call(spread_body, shape((4, 8, 32, 2 * SECOND)), second_z, swap(second_z))
    second_pieces = lax.all_to_all(second_spread, "y", 0, 0, tiled=True)
    third_pieces = line_gather(third_z)
    gated_own, gated_other = call(
        attend_body,
        [shape((half, DV)), shape((half, DV))],
        jnp.stack([y_index, core]),
        decay_logits[:, 0],
        normed_own,
        normed_other,
        *first_pieces,
        rope_frequency(),
        flops=1 << 32,
        smem=2,
        scratch=[
            pltpu.VMEM((model, FIRST), bf16),
            pltpu.VMEM((2 * half, DK), bf16),
            pltpu.VMEM((2 * half, DK), bf16),
            pltpu.VMEM((2 * half, DV), bf16),
            pltpu.VMEM((2 * half, DV), f32),
        ],
    )
    gated_partner = swap(gated_other)
    mixed = call(
        output_body,
        shape((half, model)),
        gated_own,
        gated_partner,
        second_pieces,
        flops=1 << 30,
        scratch=[pltpu.VMEM((model, 2 * SECOND), bf16)],
    )
    mix_pieces = exchanged(mixed.reshape(chips, own, model))
    taps = call(
        functools.partial(taps_body, width),
        shape((8, PAD), f32),
        gelu_kernel,
        linear_kernel,
        row(gelu_bias),
        row(linear_bias),
    )
    taps_other = swap(taps)
    after_mix, channel_spread = call(
        middle_body,
        [shape((own, model)), shape((chips, own, model))],
        mix_pieces,
        token_rows,
        row(mixer_out_gain),
        row(channel_in_gain),
    )
    channel_rows = exchanged(channel_spread)
    third_own = call(
        line_order_body, shape((8, 4, 32, THIRD)), y_index[None], *third_pieces, smem=1
    ).reshape(model, THIRD)
    third_other = swap(third_own)
    edges = jnp.concatenate([channel_rows[:, 0], channel_rows[:, own - 1]], axis=0)
    edges_other = swap(edges)
    channel = call(
        feed_body,
        shape((half, model)),
        core[None],
        channel_rows.reshape(half, model),
        edges_other,
        third_own,
        third_other,
        taps,
        taps_other,
        flops=1 << 32,
        smem=1,
        scratch=[pltpu.VMEM((half, 2 * PAD), bf16)],
    )
    channel_pieces = exchanged(channel.reshape(chips, own, model))
    result = call(final_body, shape((own, model)), channel_pieces, after_mix, row(channel_out_gain))
    return result[None]


def solution(mesh):
    fs = mesh.shape["fs"]
    tp = mesh.shape["tp"]
    split = Mesh(
        mesh.devices.reshape(mesh.shape["rep"], fs // 4, 4, tp // 2, 2),
        ("rep", "z", "y", "x", "c"),
    )
    in_specs = (
        P(("rep", "z", "y"), TP, None),
        P(),
        P(FS, TP),
        P(FS, TP),
        P(FS, TP),
        P(FS, TP),
        P(None, TP),
        P(TP, FS),
        P(),
        P(),
        P(FS, TP),
        P(FS, TP),
        P(None, TP),
        P(None, TP),
        P(TP),
        P(TP),
        P(TP, FS),
        P(),
    )
    out_specs = P(("rep", "z", "y"), TP, None)
    return jax.shard_map(layer, mesh=split, in_specs=in_specs, out_specs=out_specs, check_vma=False)
```

```python
import functools

import jax
import jax.numpy as jnp
import numpy as np
from jax import lax
from jax.experimental import pallas as pl
from jax.experimental.pallas import tpu as pltpu
from jax.sharding import Mesh
from jax.sharding import PartitionSpec as P


DK = 128
DV = 256
TP = ("x", "c")
FS = ("z", "y")
RING = ("rep", "z")
SWAP = ((0, 1), (1, 0))
PAD = 384
FIRST, SECOND, THIRD = 2 * DK + 2 * DV, DV, 3 * PAD
Z_SHIFTS = (4, 3, 2, 1, 0, -1, -2, -3)
Z_ISSUE = (4, -3, 3, -2, 2, -1, 1)
Y_SHIFTS = (0, 1, 2, -1)
Y_ISSUE = (2, 1, -1)
epsilon = 1e-06
rope_base = 10000.0
bf16 = jnp.bfloat16
f32 = jnp.float32

VMEM = pl.BlockSpec(memory_space=pltpu.VMEM)
SMEM = pl.BlockSpec(memory_space=pltpu.SMEM)


def call(body, out_shapes, *args, flops=0, smem=0, scratch=()):
    specs = [SMEM] * smem + [VMEM] * (len(args) - smem)
    single = not isinstance(out_shapes, (list, tuple))
    return pl.pallas_call(
        body,
        out_shape=out_shapes,
        in_specs=specs,
        out_specs=VMEM if single else [VMEM] * len(out_shapes),
        scratch_shapes=list(scratch),
        cost_estimate=pl.CostEstimate(
            flops=max(flops, 1 << 24), bytes_accessed=1 << 21, transcendentals=0
        ),
    )(*args)


def shape(dims, kind=bf16):
    return jax.ShapeDtypeStruct(dims, kind)


def permuted(value, axes, shift, size):
    return lax.ppermute(value, axes, [(i, (i + shift) % size) for i in range(size)])


def swap(value):
    return lax.ppermute(value, "c", SWAP)


def exchanged(value):
    return lax.all_to_all(value, "x", 0, 0, tiled=True)


def rms_rows(values, gain):
    return values * lax.rsqrt(jnp.mean(values * values, axis=-1, keepdims=True) + epsilon) * gain


def pack_body(width, q, k, v, g, mo, ge, li, dn, out):
    out[:, :DK] = q[...]
    out[:, DK : 2 * DK] = k[...]
    out[:, 2 * DK : 2 * DK + DV] = v[...]
    out[:, 2 * DK + DV : FIRST] = g[...]
    out[:, FIRST : FIRST + SECOND] = mo[...]
    gap = jnp.zeros((out.shape[0], PAD - width), bf16)
    for place, piece in enumerate((ge, li, dn)):
        at = FIRST + SECOND + place * PAD
        out[:, at : at + PAD] = jnp.concatenate([piece[...], gap], axis=1)


def taps_body(width, ge_kernel, li_kernel, ge_bias, li_bias, out):
    out[...] = jnp.zeros(out.shape, f32)
    out[0:3, :width] = ge_kernel[...]
    out[3:6, :width] = li_kernel[...]
    out[6:7, :width] = ge_bias[...]
    out[7:8, :width] = li_bias[...]


def first_norm_body(tokens, gain, out):
    rows = rms_rows(tokens[...].astype(f32), gain[...]).astype(bf16)
    for k in range(out.shape[0]):
        out[k] = rows


def ring_order_body(index, *refs):
    pieces, (one, two, three) = refs[:8], refs[8:]
    for shift, piece in zip(Z_SHIFTS, pieces):
        at = lax.rem(index[0] - shift + 8, 8)
        one[at] = piece[:, :FIRST]
        for y in range(two.shape[0]):
            two[y, at] = piece[:, FIRST : FIRST + SECOND]
        three[at] = piece[:, FIRST + SECOND :]


def line_order_body(index, *refs):
    pieces, out = refs[:4], refs[4]
    for shift, piece in zip(Y_SHIFTS, pieces):
        at = lax.rem(index[0] - shift + 4, 4)
        for z in range(8):
            out[z, at] = piece[z * 32 : z * 32 + 32, :]


def summed(pieces):
    total = pieces[0].astype(f32)
    for piece in pieces[1:]:
        total = total + piece.astype(f32)
    return total * lax.rsqrt(jnp.mean(total * total, axis=-1, keepdims=True) + epsilon)


def middle_body(pieces, tokens, out_gain, in_gain, after_mix, channel_in):
    mix = (tokens[...].astype(f32) + summed([pieces[k] for k in range(4)]) * out_gain[...]).astype(bf16)
    after_mix[...] = mix
    rows = rms_rows(mix.astype(f32), in_gain[...]).astype(bf16)
    for k in range(channel_in.shape[0]):
        channel_in[k] = rows


def final_body(here, right, left, far, after_mix, gain, out):
    out[...] = (after_mix[...].astype(f32) + summed([here[...], right[...], left[...], far[...]]) * gain[...]).astype(bf16)


def log_sigmoid_tile(logit):
    value = jnp.full((8, 128), logit, f32)
    tile = jnp.minimum(value, 0.0) - jnp.log1p(jnp.exp(-jnp.abs(value)))
    return tile[0:1, 0:1]


def attend_body(
    y_ref, core_ref, logits, own, other, p0, p1, p2, p3, frequency, out_own, out_other, w, qs, ks, vs, gs
):
    y, core = y_ref[0], core_ref[0]
    for shift, piece in zip(Y_SHIFTS, (p0, p1, p2, p3)):
        at = lax.rem(y - shift + 4, 4) * 32
        for z in range(8):
            place = pl.ds(pl.multiple_of(z * 128 + at, 32), 32)
            w[place, :] = piece[z * 32 : z * 32 + 32, :]
    inside = lax.broadcasted_iota(jnp.int32, (128, DK), 0).astype(f32) * frequency[...]
    cos_in, sin_in = jnp.cos(inside), jnp.sin(inside)
    block = lax.broadcasted_iota(jnp.int32, (8, DK), 0)
    base = (block % 4) * 256 + jnp.where(block < 4, core, 1 - core) * 128
    start = base.astype(f32) * frequency[...]
    cos_at, sin_at = jnp.cos(start), jnp.sin(start)
    sign = jnp.where(lax.broadcasted_iota(jnp.int32, (128, DK), 1) < DK // 2, -1.0, 1.0)
    cos_turn, sin_turn = cos_in * sign, sin_in * sign

    def tables(r):
        c, s = cos_at[r : r + 1, :], sin_at[r : r + 1, :]
        return c * cos_in - s * sin_in, s * cos_turn + c * sin_turn

    step = 256
    for r in range(0, 1024, step):
        rows = own[r : r + step, :] if r < 512 else other[r - 512 : r - 512 + step, :]
        projected = dot(rows, w[...])
        pair = [tables(b) for b in range(r // 128, (r + step) // 128)]
        cos = jnp.concatenate([p[0] for p in pair], axis=0)
        sin = jnp.concatenate([p[1] for p in pair], axis=0)
        q = projected[:, :DK]
        k = projected[:, DK : 2 * DK]
        qs[r : r + step, :] = (q * cos + pltpu.roll(q, DK // 2, 1) * sin).astype(bf16)
        ks[r : r + step, :] = (
            (k * cos + pltpu.roll(k, DK // 2, 1) * sin) * DK ** (-0.5)
        ).astype(bf16)
        vs[r : r + step, :] = projected[:, 2 * DK : 2 * DK + DV].astype(bf16)
        gs[r : r + step, :] = projected[:, 2 * DK + DV :]
    forward = log_sigmoid_tile(logits[0])
    backward = log_sigmoid_tile(logits[1])
    lag = (
        lax.broadcasted_iota(jnp.int32, (128, 128), 0)
        - lax.broadcasted_iota(jnp.int32, (128, 128), 1)
    ).astype(f32)
    ahead, behind = lag * forward, lag * -backward
    side = ((2 * core - 1) * 128).astype(f32)
    for r in range(8):
        decays = []
        for c in range(8):
            gap = float((r % 4 - c % 4) * 256)
            if r < 4 <= c:
                gap = gap + side
            if c < 4 <= r:
                gap = gap - side
            decays.append(jnp.exp(jnp.minimum(ahead + gap * forward, behind - gap * backward)))
        rows = slice(r * 128, r * 128 + 128)
        scores = dot_nt(qs[rows, :], ks[...])
        weighted = (scores * jnp.concatenate(decays, axis=1)).astype(bf16)
        kept = head_norm(dot(weighted, vs[...]))
        gate = gs[rows, :]
        gated = (kept * (gate / (1.0 + jnp.exp(-gate)))).astype(bf16)
        if r < 4:
            out_own[rows, :] = gated
        else:
            out_other[r * 128 - 512 : r * 128 - 384, :] = gated


def output_body(mine, theirs, my_pieces, their_pieces, out, w):
    for y in range(4):
        for z in range(8):
            at = z * 128 + y * 32
            w[at : at + 32, :DV] = my_pieces[y, z]
            w[at : at + 32, DV:] = their_pieces[y, z]
    step = 256
    for d in range(0, 1024, step):
        part = dot_nt(mine[...], w[d : d + step, :DV]) + dot_nt(theirs[...], w[d : d + step, DV:])
        out[:, d : d + step] = part.astype(bf16)


def feed_block(main, before, after, taps):
    line = lax.broadcasted_iota(jnp.int32, (128, 1), 0)
    prev = jnp.where(line == 0, before, pltpu.roll(main, 1, 0))
    nxt = jnp.where(line == 127, after, pltpu.roll(main, 127, 0))
    kernel = [
        jnp.concatenate([taps[t : t + 1, :], taps[t + 3 : t + 4, :]], axis=1) for t in range(3)
    ]
    bias = jnp.concatenate([taps[6:7, :], taps[7:8, :]], axis=1)
    conv = kernel[0] * prev + kernel[1] * main + kernel[2] * nxt + bias
    value = conv[:, :PAD]
    bent = value * (0.5 + 0.5 * jnp.tanh(0.7978845608028654 * (value + 0.044715 * value**3)))
    return (bent * conv[:, PAD:]).astype(bf16)


def feed_down(hidden, mine, theirs, outs):
    for d in range(0, 1024, 256):
        total = dot_nt(hidden[:, :PAD], mine[d : d + 256, 2 * PAD :]) + dot_nt(
            hidden[:, PAD:], theirs[d : d + 256, 2 * PAD :]
        )
        for place, out in enumerate(outs):
            out[:, d : d + 256] = total[place * 128 : place * 128 + 128, :].astype(bf16)


def feed_far_body(
    x_ref, core_ref, rows, edges, mine, theirs, my_taps, their_taps, out, outer, lines, hidden
):
    core = core_ref[0]
    block = lax.rem(x_ref[0] + 2, 4)
    lines[:128, :] = rows[pl.ds(pl.multiple_of(block * 128, 128), 128), :]
    lines[128:136, :] = edges[...]
    lines[136:144, :] = jnp.zeros((8, 1024), bf16)
    outer[...] = jnp.zeros(outer.shape, f32)
    for part, (weights, taps) in enumerate(((mine, my_taps), (theirs, their_taps))):
        columns = slice(part * 2 * PAD, part * 2 * PAD + 2 * PAD)
        main = dot(lines[...], weights[:, : 2 * PAD])
        for x in range(4):
            outer[8 + x : 9 + x, columns] = main[128 + 2 * x : 129 + 2 * x, :]
            outer[1 + x : 2 + x, columns] = main[129 + 2 * x : 130 + 2 * x, :]
        before = outer[pl.ds(block + core, 1), columns]
        after = outer[pl.ds(8 + block + core, 1), columns]
        hidden[:, part * PAD : part * PAD + PAD] = feed_block(main[:128, :], before, after, taps)
    feed_down(hidden, mine, theirs, (out,))


def feed_near_body(
    x_ref,
    core_ref,
    rows,
    outer,
    mine,
    theirs,
    my_taps,
    their_taps,
    right,
    left,
    here,
    lines,
    hidden,
):
    core = core_ref[0]
    blocks = [lax.rem(x_ref[0] + k, 4) for k in (1, 3, 0)]
    for place, block in enumerate(blocks):
        lines[place * 128 : place * 128 + 128, :] = rows[
            pl.ds(pl.multiple_of(block * 128, 128), 128), :
        ]
    for part, (weights, taps) in enumerate(((mine, my_taps), (theirs, their_taps))):
        columns = slice(part * 2 * PAD, part * 2 * PAD + 2 * PAD)
        main = dot(lines[...], weights[:, : 2 * PAD])
        for place, block in enumerate(blocks):
            inner = slice(place * 128, place * 128 + 128)
            before = outer[pl.ds(block + core, 1), columns]
            after = outer[pl.ds(8 + block + core, 1), columns]
            hidden[inner, part * PAD : part * PAD + PAD] = feed_block(
                main[inner, :], before, after, taps
            )
    feed_down(hidden, mine, theirs, (right, left, here))


def head_norm(values):
    centred = values - jnp.mean(values, axis=-1, keepdims=True)
    return centred * lax.rsqrt(jnp.mean(centred * centred, axis=-1, keepdims=True) + epsilon)


def dot(a, b):
    return jnp.dot(a, b, preferred_element_type=f32)


def dot_nt(a, b):
    return lax.dot_general(a, b, (((1,), (1,)), ((), ())), preferred_element_type=f32)


def line_gather(piece):
    got = {0: piece}
    for shift in Y_ISSUE:
        got[shift] = permuted(piece, "y", shift, 4)
    return [got[s].reshape(256, piece.shape[-1]) for s in Y_SHIFTS]


def rope_frequency():
    half = DK // 2
    frequency = 1.0 / rope_base ** (np.arange(half, dtype=np.float32) / half)
    return jnp.asarray(np.tile(frequency.astype(np.float32), 2)[None])


def layer(
    tokens,
    mixer_in_gain,
    query_weight,
    key_weight,
    value_weight,
    gate_weight,
    decay_logits,
    mixer_output,
    mixer_out_gain,
    channel_in_gain,
    gelu_weight,
    linear_weight,
    gelu_kernel,
    linear_kernel,
    gelu_bias,
    linear_bias,
    down_weight,
    channel_out_gain,
):
    core = lax.axis_index("c").astype(jnp.int32)
    y_index = lax.axis_index("y").astype(jnp.int32)
    z_index = lax.axis_index("z").astype(jnp.int32)
    token_rows = tokens[0]
    own, model = token_rows.shape
    chips = lax.axis_size("x")
    half = chips * own
    width = gelu_weight.shape[1]

    def row(vector):
        return vector.reshape(1, -1)

    packed = call(
        functools.partial(pack_body, width),
        shape((32, FIRST + SECOND + THIRD)),
        query_weight,
        key_weight,
        value_weight,
        gate_weight,
        mixer_output.T,
        gelu_weight,
        linear_weight,
        down_weight.T,
    )
    got = {0: packed}
    for shift in Z_ISSUE:
        got[shift] = permuted(packed, RING, shift, 16)
    spread = call(first_norm_body, shape((chips, own, model)), token_rows, row(mixer_in_gain))
    normed_own = exchanged(spread).reshape(half, model)
    normed_other = swap(normed_own)
    first_z, second_z, third_z = call(
        ring_order_body,
        [shape((8, 32, FIRST)), shape((4, 8, 32, SECOND)), shape((8, 32, THIRD))],
        z_index[None],
        *[got[s] for s in Z_SHIFTS],
        smem=1,
    )
    first_pieces = line_gather(first_z)
    second_own = lax.all_to_all(second_z, "y", 0, 0, tiled=True)
    third_pieces = line_gather(third_z)
    gated_own, gated_other = call(
        attend_body,
        [shape((half, DV)), shape((half, DV))],
        y_index[None],
        core[None],
        decay_logits[:, 0],
        normed_own,
        normed_other,
        *first_pieces,
        rope_frequency(),
        flops=1 << 32,
        smem=3,
        scratch=[
            pltpu.VMEM((model, FIRST), bf16),
            pltpu.VMEM((2 * half, DK), bf16),
            pltpu.VMEM((2 * half, DK), bf16),
            pltpu.VMEM((2 * half, DV), bf16),
            pltpu.VMEM((2 * half, DV), f32),
        ],
    )
    gated_partner = swap(gated_other)
    mixed = call(
        output_body,
        shape((half, model)),
        gated_own,
        gated_partner,
        second_own,
        swap(second_own),
        flops=1 << 30,
        scratch=[pltpu.VMEM((model, 2 * SECOND), bf16)],
    )
    mix_pieces = exchanged(mixed.reshape(chips, own, model))
    taps = call(
        functools.partial(taps_body, width),
        shape((8, PAD), f32),
        gelu_kernel,
        linear_kernel,
        row(gelu_bias),
        row(linear_bias),
    )
    taps_other = swap(taps)
    after_mix, channel_spread = call(
        middle_body,
        [shape((own, model)), shape((chips, own, model))],
        mix_pieces,
        token_rows,
        row(mixer_out_gain),
        row(channel_in_gain),
    )
    channel_rows = exchanged(channel_spread)
    third_own = call(
        line_order_body, shape((8, 4, 32, THIRD)), y_index[None], *third_pieces, smem=1
    ).reshape(model, THIRD)
    third_other = swap(third_own)
    edges = lax.slice(
        channel_rows, (0, 0, 0), (chips, own, model), (1, own - 1, 1)
    ).reshape(2 * chips, model)
    edges_other = swap(edges)
    flat_rows = channel_rows.reshape(half, model)
    x_index = lax.axis_index("x").astype(jnp.int32)[None]
    far, outer = call(
        feed_far_body,
        [shape((own, model)), shape((16, 4 * PAD), f32)],
        x_index,
        core[None],
        flat_rows,
        edges_other,
        third_own,
        third_other,
        taps,
        taps_other,
        flops=1 << 31,
        smem=2,
        scratch=[pltpu.VMEM((own + 16, model), bf16), pltpu.VMEM((own, 2 * PAD), bf16)],
    )
    far_got = permuted(far, "x", 2, 4)
    right, left, here = call(
        feed_near_body,
        [shape((own, model))] * 3,
        x_index,
        core[None],
        flat_rows,
        outer,
        third_own,
        third_other,
        taps,
        taps_other,
        flops=1 << 32,
        smem=2,
        scratch=[pltpu.VMEM((3 * own, model), bf16), pltpu.VMEM((3 * own, 2 * PAD), bf16)],
    )
    right_got = permuted(right, "x", 1, 4)
    left_got = permuted(left, "x", -1, 4)
    result = call(
        final_body,
        shape((own, model)),
        here,
        right_got,
        left_got,
        far_got,
        after_mix,
        row(channel_out_gain),
    )
    return result[None]


def solution(mesh):
    fs = mesh.shape["fs"]
    tp = mesh.shape["tp"]
    split = Mesh(
        mesh.devices.reshape(mesh.shape["rep"], fs // 4, 4, tp // 2, 2),
        ("rep", "z", "y", "x", "c"),
    )
    in_specs = (
        P(("rep", "z", "y"), TP, None),
        P(),
        P(FS, TP),
        P(FS, TP),
        P(FS, TP),
        P(FS, TP),
        P(None, TP),
        P(TP, FS),
        P(),
        P(),
        P(FS, TP),
        P(FS, TP),
        P(None, TP),
        P(None, TP),
        P(TP),
        P(TP),
        P(TP, FS),
        P(),
    )
    out_specs = P(("rep", "z", "y"), TP, None)
    return jax.shard_map(layer, mesh=split, in_specs=in_specs, out_specs=out_specs, check_vma=False)
```

```python
import functools

import jax
import jax.numpy as jnp
import numpy as np
from jax import lax
from jax.experimental import pallas as pl
from jax.experimental.pallas import tpu as pltpu
from jax.sharding import Mesh
from jax.sharding import PartitionSpec as P


DK = 128
DV = 256
TP = ("x", "c")
FS = ("z", "y")
RING = ("rep", "z")
SWAP = ((0, 1), (1, 0))
PAD = 384
PROJECT, FIRST, THIRD = 2 * DK + 2 * DV, 2 * DK + 3 * DV, 3 * PAD
Z_SHIFTS = (4, 3, 2, 1, 0, -1, -2, -3)
Z_ISSUE = (4, -3, 3, -2, 2, -1, 1)
Y_SHIFTS = (0, 1, 2, -1)
Y_ISSUE = (2, 1, -1)
epsilon = 1e-06
rope_base = 10000.0
bf16 = jnp.bfloat16
f32 = jnp.float32

VMEM = pl.BlockSpec(memory_space=pltpu.VMEM)
SMEM = pl.BlockSpec(memory_space=pltpu.SMEM)


def call(body, out_shapes, *args, flops=0, smem=0, scratch=()):
    specs = [SMEM] * smem + [VMEM] * (len(args) - smem)
    single = not isinstance(out_shapes, (list, tuple))
    return pl.pallas_call(
        body,
        out_shape=out_shapes,
        in_specs=specs,
        out_specs=VMEM if single else [VMEM] * len(out_shapes),
        scratch_shapes=list(scratch),
        cost_estimate=pl.CostEstimate(
            flops=max(flops, 1 << 24), bytes_accessed=1 << 21, transcendentals=0
        ),
    )(*args)


def shape(dims, kind=bf16):
    return jax.ShapeDtypeStruct(dims, kind)


def permuted(value, axes, shift, size):
    return lax.ppermute(value, axes, [(i, (i + shift) % size) for i in range(size)])


def swap(value):
    return lax.ppermute(value, "c", SWAP)


def exchanged(value):
    return lax.all_to_all(value, "x", 0, 0, tiled=True)


def rms_rows(values, gain):
    return values * lax.rsqrt(jnp.mean(values * values, axis=-1, keepdims=True) + epsilon) * gain


def pack_body(width, q, k, v, g, mo, ge, li, dn, out):
    out[:, :DK] = q[...]
    out[:, DK : 2 * DK] = k[...]
    out[:, 2 * DK : 2 * DK + DV] = v[...]
    out[:, 2 * DK + DV : PROJECT] = g[...]
    out[:, PROJECT:FIRST] = mo[...]
    gap = jnp.zeros((out.shape[0], PAD - width), bf16)
    for place, piece in enumerate((ge, li, dn)):
        at = FIRST + place * PAD
        out[:, at : at + PAD] = jnp.concatenate([piece[...], gap], axis=1)


def taps_body(width, ge_kernel, li_kernel, ge_bias, li_bias, out):
    out[...] = jnp.zeros(out.shape, f32)
    out[0:3, :width] = ge_kernel[...]
    out[3:6, :width] = li_kernel[...]
    out[6:7, :width] = ge_bias[...]
    out[7:8, :width] = li_bias[...]


def first_norm_body(tokens, gain, out):
    rows = rms_rows(tokens[...].astype(f32), gain[...]).astype(bf16)
    for k in range(out.shape[0]):
        out[k] = rows


def ring_order_body(index, *refs):
    pieces, (one, three) = refs[:8], refs[8:]
    for shift, piece in zip(Z_SHIFTS, pieces):
        at = lax.rem(index[0] - shift + 8, 8)
        one[at] = piece[:, :FIRST]
        for y in range(three.shape[0]):
            three[y, at] = piece[:, FIRST:]


def summed(pieces):
    total = pieces[0][...].astype(f32)
    for piece in pieces[1:]:
        total = total + piece[...].astype(f32)
    return total * lax.rsqrt(jnp.mean(total * total, axis=-1, keepdims=True) + epsilon)


def middle_body(far, right, left, here, tokens, out_gain, in_gain, after_mix, channel_in):
    total = summed((here, right, left, far))
    mix = (tokens[...].astype(f32) + total * out_gain[...]).astype(bf16)
    after_mix[...] = mix
    channel_in[...] = rms_rows(mix.astype(f32), in_gain[...]).astype(bf16)


def final_body(far, right, left, here, after_mix, gain, out):
    total = summed((here, right, left, far))
    out[...] = (after_mix[...].astype(f32) + total * gain[...]).astype(bf16)


def log_sigmoid_tile(logit):
    value = jnp.full((8, 128), logit, f32)
    tile = jnp.minimum(value, 0.0) - jnp.log1p(jnp.exp(-jnp.abs(value)))
    return tile[0:1, 0:1]


def attend_body(
    y_ref, core_ref, logits, own, other, p0, p1, p2, p3, frequency, out_own, out_other, mo, w, qs, ks, vs, gs
):
    y, core = y_ref[0], core_ref[0]
    for shift, piece in zip(Y_SHIFTS, (p0, p1, p2, p3)):
        at = lax.rem(y - shift + 4, 4) * 32
        for z in range(8):
            place = pl.ds(pl.multiple_of(z * 128 + at, 32), 32)
            w[place, :] = piece[z * 32 : z * 32 + 32, :PROJECT]
            mo[place, :] = piece[z * 32 : z * 32 + 32, PROJECT:]
    inside = lax.broadcasted_iota(jnp.int32, (128, DK), 0).astype(f32) * frequency[...]
    cos_in, sin_in = jnp.cos(inside), jnp.sin(inside)
    block = lax.broadcasted_iota(jnp.int32, (8, DK), 0)
    base = (block % 4) * 256 + jnp.where(block < 4, core, 1 - core) * 128
    start = base.astype(f32) * frequency[...]
    cos_at, sin_at = jnp.cos(start), jnp.sin(start)
    sign = jnp.where(lax.broadcasted_iota(jnp.int32, (128, DK), 1) < DK // 2, -1.0, 1.0)
    cos_turn, sin_turn = cos_in * sign, sin_in * sign

    def tables(r):
        c, s = cos_at[r : r + 1, :], sin_at[r : r + 1, :]
        return c * cos_in - s * sin_in, s * cos_turn + c * sin_turn

    step = 256
    for r in range(0, 1024, step):
        rows = own[r : r + step, :] if r < 512 else other[r - 512 : r - 512 + step, :]
        projected = dot(rows, w[...])
        pair = [tables(b) for b in range(r // 128, (r + step) // 128)]
        cos = jnp.concatenate([p[0] for p in pair], axis=0)
        sin = jnp.concatenate([p[1] for p in pair], axis=0)
        q = projected[:, :DK]
        k = projected[:, DK : 2 * DK]
        qs[r : r + step, :] = (q * cos + pltpu.roll(q, DK // 2, 1) * sin).astype(bf16)
        ks[r : r + step, :] = (
            (k * cos + pltpu.roll(k, DK // 2, 1) * sin) * DK ** (-0.5)
        ).astype(bf16)
        vs[r : r + step, :] = projected[:, 2 * DK : 2 * DK + DV].astype(bf16)
        gs[r : r + step, :] = projected[:, 2 * DK + DV :]
    forward = log_sigmoid_tile(logits[0])
    backward = log_sigmoid_tile(logits[1])
    lag = (
        lax.broadcasted_iota(jnp.int32, (128, 128), 0)
        - lax.broadcasted_iota(jnp.int32, (128, 128), 1)
    ).astype(f32)
    ahead, behind = lag * forward, lag * -backward
    side = ((2 * core - 1) * 128).astype(f32)
    for r in range(8):
        decays = []
        for c in range(8):
            gap = float((r % 4 - c % 4) * 256)
            if r < 4 <= c:
                gap = gap + side
            if c < 4 <= r:
                gap = gap - side
            decays.append(jnp.exp(jnp.minimum(ahead + gap * forward, behind - gap * backward)))
        rows = slice(r * 128, r * 128 + 128)
        scores = dot_nt(qs[rows, :], ks[...])
        weighted = (scores * jnp.concatenate(decays, axis=1)).astype(bf16)
        kept = head_norm(dot(weighted, vs[...]))
        gate = gs[rows, :]
        gated = (kept * (gate / (1.0 + jnp.exp(-gate)))).astype(bf16)
        if r < 4:
            out_own[rows, :] = gated
        else:
            out_other[r * 128 - 512 : r * 128 - 384, :] = gated


def output_body(x_ref, mine, theirs, my_weights, their_weights, far, right, left, here, lines):
    for place, ahead in enumerate((2, 1, 3, 0)):
        block = lax.rem(x_ref[0] + ahead, 4)
        rows = pl.ds(pl.multiple_of(block * 128, 128), 128)
        lines[place * 128 : place * 128 + 128, :DV] = mine[rows, :]
        lines[place * 128 : place * 128 + 128, DV:] = theirs[rows, :]
    for d in range(0, 1024, 256):
        columns = slice(d, d + 256)
        total = dot_nt(lines[:, :DV], my_weights[columns, :]) + dot_nt(
            lines[:, DV:], their_weights[columns, :]
        )
        for place, out in enumerate((far, right, left, here)):
            out[:, columns] = total[place * 128 : place * 128 + 128, :].astype(bf16)


def feed_block(main, before, after, taps):
    line = lax.broadcasted_iota(jnp.int32, (128, 1), 0)
    prev = jnp.where(line == 0, before, pltpu.roll(main, 1, 0))
    nxt = jnp.where(line == 127, after, pltpu.roll(main, 127, 0))
    kernel = [
        jnp.concatenate([taps[t : t + 1, :], taps[t + 3 : t + 4, :]], axis=1) for t in range(3)
    ]
    bias = jnp.concatenate([taps[6:7, :], taps[7:8, :]], axis=1)
    conv = kernel[0] * prev + kernel[1] * main + kernel[2] * nxt + bias
    value = conv[:, :PAD]
    bent = value * (0.5 + 0.5 * jnp.tanh(0.7978845608028654 * (value + 0.044715 * value**3)))
    return (bent * conv[:, PAD:]).astype(bf16)


def feed_body(
    x_ref,
    core_ref,
    got_far,
    got_next,
    got_prev,
    own,
    edges,
    mine,
    theirs,
    my_taps,
    their_taps,
    far,
    right,
    left,
    here,
    lines,
    outer,
    hidden,
    my_weights,
    their_weights,
):
    core = core_ref[0]
    blocks = [lax.rem(x_ref[0] + k, 4) for k in (2, 1, 3, 0)]
    for place, piece in enumerate((got_far, got_next, got_prev, own)):
        lines[place * 128 : place * 128 + 128, :] = piece[...]
    lines[512:520, :] = edges[...]
    lines[520:528, :] = jnp.zeros((8, 1024), bf16)
    outer[...] = jnp.zeros(outer.shape, f32)
    for part, (raw, weights, taps) in enumerate(
        ((mine, my_weights, my_taps), (theirs, their_weights, their_taps))
    ):
        for z in range(8):
            for y in range(4):
                at = z * 128 + y * 32
                weights[at : at + 32, :] = raw[y, z]
        main = dot(lines[...], weights[:, : 2 * PAD])
        for place, block in enumerate(blocks):
            outer[pl.ds(8 + block, 1), :] = main[512 + 2 * place : 513 + 2 * place, :]
            outer[pl.ds(1 + block, 1), :] = main[513 + 2 * place : 514 + 2 * place, :]
        for place, block in enumerate(blocks):
            inner = slice(place * 128, place * 128 + 128)
            before = outer[pl.ds(block + core, 1), :]
            after = outer[pl.ds(8 + block + core, 1), :]
            hidden[inner, part * PAD : part * PAD + PAD] = feed_block(
                main[inner, :], before, after, taps
            )
    for d in range(0, 1024, 256):
        columns = slice(d, d + 256)
        total = dot_nt(hidden[:, :PAD], my_weights[columns, 2 * PAD :]) + dot_nt(
            hidden[:, PAD:], their_weights[columns, 2 * PAD :]
        )
        for place, out in enumerate((far, right, left, here)):
            out[:, columns] = total[place * 128 : place * 128 + 128, :].astype(bf16)


def head_norm(values):
    centred = values - jnp.mean(values, axis=-1, keepdims=True)
    return centred * lax.rsqrt(jnp.mean(centred * centred, axis=-1, keepdims=True) + epsilon)


def dot(a, b):
    return jnp.dot(a, b, preferred_element_type=f32)


def dot_nt(a, b):
    return lax.dot_general(a, b, (((1,), (1,)), ((), ())), preferred_element_type=f32)


def line_gather(piece):
    got = {0: piece}
    for shift in Y_ISSUE:
        got[shift] = permuted(piece, "y", shift, 4)
    return [got[s].reshape(256, piece.shape[-1]) for s in Y_SHIFTS]


def sent(far, right, left):
    return (permuted(far, "x", 2, 4), permuted(right, "x", 1, 4), permuted(left, "x", -1, 4))


def rope_frequency():
    half = DK // 2
    frequency = 1.0 / rope_base ** (np.arange(half, dtype=np.float32) / half)
    return jnp.asarray(np.tile(frequency.astype(np.float32), 2)[None])


def layer(
    tokens,
    mixer_in_gain,
    query_weight,
    key_weight,
    value_weight,
    gate_weight,
    decay_logits,
    mixer_output,
    mixer_out_gain,
    channel_in_gain,
    gelu_weight,
    linear_weight,
    gelu_kernel,
    linear_kernel,
    gelu_bias,
    linear_bias,
    down_weight,
    channel_out_gain,
):
    core = lax.axis_index("c").astype(jnp.int32)
    y_index = lax.axis_index("y").astype(jnp.int32)
    z_index = lax.axis_index("z").astype(jnp.int32)
    token_rows = tokens[0]
    own, model = token_rows.shape
    chips = lax.axis_size("x")
    half = chips * own
    width = gelu_weight.shape[1]

    def row(vector):
        return vector.reshape(1, -1)

    packed = call(
        functools.partial(pack_body, width),
        shape((32, FIRST + THIRD)),
        query_weight,
        key_weight,
        value_weight,
        gate_weight,
        mixer_output.T,
        gelu_weight,
        linear_weight,
        down_weight.T,
    )
    got = {0: packed}
    for shift in Z_ISSUE:
        got[shift] = permuted(packed, RING, shift, 16)
    spread = call(first_norm_body, shape((chips, own, model)), token_rows, row(mixer_in_gain))
    normed_own = exchanged(spread).reshape(half, model)
    normed_other = swap(normed_own)
    first_z, third_z = call(
        ring_order_body,
        [shape((8, 32, FIRST)), shape((4, 8, 32, THIRD))],
        z_index[None],
        *[got[s] for s in Z_SHIFTS],
        smem=1,
    )
    first_pieces = line_gather(first_z)
    third_own = lax.all_to_all(third_z, "y", 0, 0, tiled=True)
    taps = call(
        functools.partial(taps_body, width),
        shape((8, PAD), f32),
        gelu_kernel,
        linear_kernel,
        row(gelu_bias),
        row(linear_bias),
    )
    taps_other = swap(taps)
    gated_own, gated_other, out_own = call(
        attend_body,
        [shape((half, DV)), shape((half, DV)), shape((model, DV))],
        y_index[None],
        core[None],
        decay_logits[:, 0],
        normed_own,
        normed_other,
        *first_pieces,
        rope_frequency(),
        flops=1 << 32,
        smem=3,
        scratch=[
            pltpu.VMEM((model, PROJECT), bf16),
            pltpu.VMEM((2 * half, DK), bf16),
            pltpu.VMEM((2 * half, DK), bf16),
            pltpu.VMEM((2 * half, DV), bf16),
            pltpu.VMEM((2 * half, DV), f32),
        ],
    )
    gated_partner = swap(gated_other)
    x_index = lax.axis_index("x").astype(jnp.int32)[None]
    far, right, left, here = call(
        output_body,
        [shape((own, model))] * 4,
        x_index,
        gated_own,
        gated_partner,
        out_own,
        swap(out_own),
        flops=1 << 30,
        smem=1,
        scratch=[pltpu.VMEM((half, 2 * DV), bf16)],
    )
    after_mix, channel_in = call(
        middle_body,
        [shape((own, model)), shape((own, model))],
        *sent(far, right, left),
        here,
        token_rows,
        row(mixer_out_gain),
        row(channel_in_gain),
    )
    third_other = swap(third_own)
    got_far, got_prev, got_next = sent(channel_in, channel_in, channel_in)
    blocks = (got_far, got_next, got_prev, channel_in)
    edges = jnp.concatenate([b[k : k + 1] for b in blocks for k in (0, own - 1)], axis=0)
    far, right, left, here = call(
        feed_body,
        [shape((own, model))] * 4,
        x_index,
        core[None],
        *blocks,
        swap(edges),
        third_own,
        third_other,
        taps,
        taps_other,
        flops=1 << 32,
        smem=2,
        scratch=[
            pltpu.VMEM((half + 16, model), bf16),
            pltpu.VMEM((16, 2 * PAD), f32),
            pltpu.VMEM((half, 2 * PAD), bf16),
            pltpu.VMEM((model, THIRD), bf16),
            pltpu.VMEM((model, THIRD), bf16),
        ],
    )
    result = call(
        final_body,
        shape((own, model)),
        *sent(far, right, left),
        here,
        after_mix,
        row(channel_out_gain),
    )
    return result[None]


def solution(mesh):
    fs = mesh.shape["fs"]
    tp = mesh.shape["tp"]
    split = Mesh(
        mesh.devices.reshape(mesh.shape["rep"], fs // 4, 4, tp // 2, 2),
        ("rep", "z", "y", "x", "c"),
    )
    in_specs = (
        P(("rep", "z", "y"), TP, None),
        P(),
        P(FS, TP),
        P(FS, TP),
        P(FS, TP),
        P(FS, TP),
        P(None, TP),
        P(TP, FS),
        P(),
        P(),
        P(FS, TP),
        P(FS, TP),
        P(None, TP),
        P(None, TP),
        P(TP),
        P(TP),
        P(TP, FS),
        P(),
    )
    out_specs = P(("rep", "z", "y"), TP, None)
    return jax.shard_map(layer, mesh=split, in_specs=in_specs, out_specs=out_specs, check_vma=False)
```

```python
import functools

import jax
import jax.numpy as jnp
import numpy as np
from jax import lax
from jax.experimental import pallas as pl
from jax.experimental.pallas import tpu as pltpu
from jax.sharding import Mesh
from jax.sharding import PartitionSpec as P


DK = 128
DV = 256
TP = ("x", "c")
FS = ("z", "y")
RING = ("rep", "z")
SWAP = ((0, 1), (1, 0))
PAD = 384
PROJECT, FIRST, THIRD = 2 * DK + 2 * DV, 2 * DK + 3 * DV, 3 * PAD
Z_SHIFTS = (4, 3, 2, 1, 0, -1, -2, -3)
Z_ISSUE = (4, -3, 3, -2, 2, -1, 1)
Y_SHIFTS = (0, 1, 2, -1)
Y_ISSUE = (2, 1, -1)
epsilon = 1e-06
rope_base = 10000.0
bf16 = jnp.bfloat16
f32 = jnp.float32

VMEM = pl.BlockSpec(memory_space=pltpu.VMEM)
SMEM = pl.BlockSpec(memory_space=pltpu.SMEM)


def call(body, out_shapes, *args, flops=0, smem=0, scratch=(), limit=6):
    specs = [SMEM] * smem + [VMEM] * (len(args) - smem)
    single = not isinstance(out_shapes, (list, tuple))
    return pl.pallas_call(
        body,
        out_shape=out_shapes,
        in_specs=specs,
        out_specs=VMEM if single else [VMEM] * len(out_shapes),
        scratch_shapes=list(scratch),
        compiler_params=pltpu.CompilerParams(vmem_limit_bytes=limit << 20),
        cost_estimate=pl.CostEstimate(
            flops=max(flops, 1 << 24), bytes_accessed=1 << 21, transcendentals=0
        ),
    )(*args)


def shape(dims, kind=bf16):
    return jax.ShapeDtypeStruct(dims, kind)


def permuted(value, axes, shift, size):
    return lax.ppermute(value, axes, [(i, (i + shift) % size) for i in range(size)])


def swap(value):
    return lax.ppermute(value, "c", SWAP)


def exchanged(value):
    return lax.all_to_all(value, "x", 0, 0, tiled=True)


def rms_rows(values, gain):
    return values * lax.rsqrt(jnp.mean(values * values, axis=-1, keepdims=True) + epsilon) * gain


def pack_body(width, q, k, v, g, mo, ge, li, dn, out):
    out[:, :DK] = q[...]
    out[:, DK : 2 * DK] = k[...]
    out[:, 2 * DK : 2 * DK + DV] = v[...]
    out[:, 2 * DK + DV : PROJECT] = g[...]
    out[:, PROJECT:FIRST] = mo[...]
    gap = jnp.zeros((out.shape[0], PAD - width), bf16)
    for place, piece in enumerate((ge, li, dn)):
        at = FIRST + place * PAD
        out[:, at : at + PAD] = jnp.concatenate([piece[...], gap], axis=1)


def taps_body(width, ge_kernel, li_kernel, ge_bias, li_bias, out):
    out[...] = jnp.zeros(out.shape, f32)
    out[0:3, :width] = ge_kernel[...]
    out[3:6, :width] = li_kernel[...]
    out[6:7, :width] = ge_bias[...]
    out[7:8, :width] = li_bias[...]


def first_norm_body(tokens, gain, out):
    rows = rms_rows(tokens[...].astype(f32), gain[...]).astype(bf16)
    for k in range(out.shape[0]):
        out[k] = rows


def ring_order_body(index, *refs):
    pieces, (one, three) = refs[:8], refs[8:]
    for shift, piece in zip(Z_SHIFTS, pieces):
        at = lax.rem(index[0] - shift + 8, 8)
        one[at] = piece[:, :FIRST]
        for y in range(three.shape[0]):
            three[y, at] = piece[:, FIRST:]


def summed(pieces):
    total = pieces[0][...].astype(f32)
    for piece in pieces[1:]:
        total = total + piece[...].astype(f32)
    return total * lax.rsqrt(jnp.mean(total * total, axis=-1, keepdims=True) + epsilon)


def middle_body(far, right, left, here, tokens, out_gain, in_gain, after_mix, channel_in):
    total = summed((here, right, left, far))
    mix = (tokens[...].astype(f32) + total * out_gain[...]).astype(bf16)
    after_mix[...] = mix
    channel_in[...] = rms_rows(mix.astype(f32), in_gain[...]).astype(bf16)


def final_body(far, right, left, here, after_mix, gain, out):
    total = summed((here, right, left, far))
    out[...] = (after_mix[...].astype(f32) + total * gain[...]).astype(bf16)


def log_sigmoid_tile(logit):
    value = jnp.full((8, 128), logit, f32)
    tile = jnp.minimum(value, 0.0) - jnp.log1p(jnp.exp(-jnp.abs(value)))
    return tile[0:1, 0:1]


def attend_body(
    y_ref, core_ref, logits, own, other, p0, p1, p2, p3, frequency, out_own, out_other, mo, w, qs, ks, vs, gs
):
    y, core = y_ref[0], core_ref[0]
    for shift, piece in zip(Y_SHIFTS, (p0, p1, p2, p3)):
        at = lax.rem(y - shift + 4, 4) * 32
        for z in range(8):
            place = pl.ds(pl.multiple_of(z * 128 + at, 32), 32)
            w[place, :] = piece[z * 32 : z * 32 + 32, :PROJECT]
            mo[place, :] = piece[z * 32 : z * 32 + 32, PROJECT:]
    inside = lax.broadcasted_iota(jnp.int32, (128, DK), 0).astype(f32) * frequency[...]
    cos_in, sin_in = jnp.cos(inside), jnp.sin(inside)
    block = lax.broadcasted_iota(jnp.int32, (8, DK), 0)
    base = (block % 4) * 256 + jnp.where(block < 4, core, 1 - core) * 128
    start = base.astype(f32) * frequency[...]
    cos_at, sin_at = jnp.cos(start), jnp.sin(start)
    sign = jnp.where(lax.broadcasted_iota(jnp.int32, (128, DK), 1) < DK // 2, -1.0, 1.0)
    cos_turn, sin_turn = cos_in * sign, sin_in * sign

    def tables(r):
        c, s = cos_at[r : r + 1, :], sin_at[r : r + 1, :]
        return c * cos_in - s * sin_in, s * cos_turn + c * sin_turn

    step = 256
    for r in range(0, 1024, step):
        rows = own[r : r + step, :] if r < 512 else other[r - 512 : r - 512 + step, :]
        projected = dot(rows, w[...])
        pair = [tables(b) for b in range(r // 128, (r + step) // 128)]
        cos = jnp.concatenate([p[0] for p in pair], axis=0)
        sin = jnp.concatenate([p[1] for p in pair], axis=0)
        q = projected[:, :DK]
        k = projected[:, DK : 2 * DK]
        qs[r : r + step, :] = (q * cos + pltpu.roll(q, DK // 2, 1) * sin).astype(bf16)
        ks[r : r + step, :] = (
            (k * cos + pltpu.roll(k, DK // 2, 1) * sin) * DK ** (-0.5)
        ).astype(bf16)
        vs[r : r + step, :] = projected[:, 2 * DK : 2 * DK + DV].astype(bf16)
        gs[r : r + step, :] = projected[:, 2 * DK + DV :]
    forward = log_sigmoid_tile(logits[0])
    backward = log_sigmoid_tile(logits[1])
    lag = (
        lax.broadcasted_iota(jnp.int32, (128, 128), 0)
        - lax.broadcasted_iota(jnp.int32, (128, 128), 1)
    ).astype(f32)
    ahead, behind = lag * forward, lag * -backward
    side = ((2 * core - 1) * 128).astype(f32)
    for r in range(8):
        decays = []
        for c in range(8):
            gap = float((r % 4 - c % 4) * 256)
            if r < 4 <= c:
                gap = gap + side
            if c < 4 <= r:
                gap = gap - side
            decays.append(jnp.exp(jnp.minimum(ahead + gap * forward, behind - gap * backward)))
        rows = slice(r * 128, r * 128 + 128)
        scores = dot_nt(qs[rows, :], ks[...])
        weighted = (scores * jnp.concatenate(decays, axis=1)).astype(bf16)
        kept = head_norm(dot(weighted, vs[...]))
        gate = gs[rows, :]
        gated = (kept * (gate / (1.0 + jnp.exp(-gate)))).astype(bf16)
        if r < 4:
            out_own[rows, :] = gated
        else:
            out_other[r * 128 - 512 : r * 128 - 384, :] = gated


def output_body(x_ref, mine, theirs, my_weights, their_weights, far, right, left, here, lines):
    for place, ahead in enumerate((2, 1, 3, 0)):
        block = lax.rem(x_ref[0] + ahead, 4)
        rows = pl.ds(pl.multiple_of(block * 128, 128), 128)
        lines[place * 128 : place * 128 + 128, :DV] = mine[rows, :]
        lines[place * 128 : place * 128 + 128, DV:] = theirs[rows, :]
    for d in range(0, 1024, 256):
        columns = slice(d, d + 256)
        total = dot_nt(lines[:, :DV], my_weights[columns, :]) + dot_nt(
            lines[:, DV:], their_weights[columns, :]
        )
        for place, out in enumerate((far, right, left, here)):
            out[:, columns] = total[place * 128 : place * 128 + 128, :].astype(bf16)


def feed_block(main, before, after, taps):
    line = lax.broadcasted_iota(jnp.int32, (128, 1), 0)
    prev = jnp.where(line == 0, before, pltpu.roll(main, 1, 0))
    nxt = jnp.where(line == 127, after, pltpu.roll(main, 127, 0))
    kernel = [
        jnp.concatenate([taps[t : t + 1, :], taps[t + 3 : t + 4, :]], axis=1) for t in range(3)
    ]
    bias = jnp.concatenate([taps[6:7, :], taps[7:8, :]], axis=1)
    conv = kernel[0] * prev + kernel[1] * main + kernel[2] * nxt + bias
    value = conv[:, :PAD]
    bent = value * (0.5 + 0.5 * jnp.tanh(0.7978845608028654 * (value + 0.044715 * value**3)))
    return (bent * conv[:, PAD:]).astype(bf16)


def feed_body(
    x_ref,
    core_ref,
    got_far,
    got_next,
    got_prev,
    own,
    edges,
    mine,
    theirs,
    my_taps,
    their_taps,
    far,
    right,
    left,
    here,
    lines,
    outer,
    hidden,
    my_weights,
    their_weights,
):
    core = core_ref[0]
    blocks = [lax.rem(x_ref[0] + k, 4) for k in (2, 1, 3, 0)]
    for place, piece in enumerate((got_far, got_next, got_prev, own)):
        lines[place * 128 : place * 128 + 128, :] = piece[...]
    lines[512:520, :] = edges[...]
    lines[520:528, :] = jnp.zeros((8, 1024), bf16)
    outer[...] = jnp.zeros(outer.shape, f32)
    for part, (raw, weights, taps) in enumerate(
        ((mine, my_weights, my_taps), (theirs, their_weights, their_taps))
    ):
        for z in range(8):
            for y in range(4):
                at = z * 128 + y * 32
                weights[at : at + 32, :] = raw[y, z]
        main = dot(lines[...], weights[:, : 2 * PAD])
        for place, block in enumerate(blocks):
            outer[pl.ds(8 + block, 1), :] = main[512 + 2 * place : 513 + 2 * place, :]
            outer[pl.ds(1 + block, 1), :] = main[513 + 2 * place : 514 + 2 * place, :]
        for place, block in enumerate(blocks):
            inner = slice(place * 128, place * 128 + 128)
            before = outer[pl.ds(block + core, 1), :]
            after = outer[pl.ds(8 + block + core, 1), :]
            hidden[inner, part * PAD : part * PAD + PAD] = feed_block(
                main[inner, :], before, after, taps
            )
    for d in range(0, 1024, 256):
        columns = slice(d, d + 256)
        total = dot_nt(hidden[:, :PAD], my_weights[columns, 2 * PAD :]) + dot_nt(
            hidden[:, PAD:], their_weights[columns, 2 * PAD :]
        )
        for place, out in enumerate((far, right, left, here)):
            out[:, columns] = total[place * 128 : place * 128 + 128, :].astype(bf16)


def head_norm(values):
    centred = values - jnp.mean(values, axis=-1, keepdims=True)
    return centred * lax.rsqrt(jnp.mean(centred * centred, axis=-1, keepdims=True) + epsilon)


def dot(a, b):
    return jnp.dot(a, b, preferred_element_type=f32)


def dot_nt(a, b):
    return lax.dot_general(a, b, (((1,), (1,)), ((), ())), preferred_element_type=f32)


def line_gather(piece):
    got = {0: piece}
    for shift in Y_ISSUE:
        got[shift] = permuted(piece, "y", shift, 4)
    return [got[s].reshape(256, piece.shape[-1]) for s in Y_SHIFTS]


def sent(far, right, left):
    return (permuted(far, "x", 2, 4), permuted(right, "x", 1, 4), permuted(left, "x", -1, 4))


def rope_frequency():
    half = DK // 2
    frequency = 1.0 / rope_base ** (np.arange(half, dtype=np.float32) / half)
    return jnp.asarray(np.tile(frequency.astype(np.float32), 2)[None])


def layer(
    tokens,
    mixer_in_gain,
    query_weight,
    key_weight,
    value_weight,
    gate_weight,
    decay_logits,
    mixer_output,
    mixer_out_gain,
    channel_in_gain,
    gelu_weight,
    linear_weight,
    gelu_kernel,
    linear_kernel,
    gelu_bias,
    linear_bias,
    down_weight,
    channel_out_gain,
):
    core = lax.axis_index("c").astype(jnp.int32)
    y_index = lax.axis_index("y").astype(jnp.int32)
    z_index = lax.axis_index("z").astype(jnp.int32)
    token_rows = tokens[0]
    own, model = token_rows.shape
    chips = lax.axis_size("x")
    half = chips * own
    width = gelu_weight.shape[1]

    def row(vector):
        return vector.reshape(1, -1)

    packed = call(
        functools.partial(pack_body, width),
        shape((32, FIRST + THIRD)),
        query_weight,
        key_weight,
        value_weight,
        gate_weight,
        mixer_output.T,
        gelu_weight,
        linear_weight,
        down_weight.T,
    )
    got = {0: packed}
    for shift in Z_ISSUE:
        got[shift] = permuted(packed, RING, shift, 16)
    spread = call(first_norm_body, shape((chips, own, model)), token_rows, row(mixer_in_gain))
    normed_own = exchanged(spread).reshape(half, model)
    normed_other = swap(normed_own)
    first_z, third_z = call(
        ring_order_body,
        [shape((8, 32, FIRST)), shape((4, 8, 32, THIRD))],
        z_index[None],
        *[got[s] for s in Z_SHIFTS],
        smem=1,
    )
    first_pieces = line_gather(first_z)
    third_own = lax.all_to_all(third_z, "y", 0, 0, tiled=True)
    taps = call(
        functools.partial(taps_body, width),
        shape((8, PAD), f32),
        gelu_kernel,
        linear_kernel,
        row(gelu_bias),
        row(linear_bias),
    )
    taps_other = swap(taps)
    gated_own, gated_other, out_own = call(
        attend_body,
        [shape((half, DV)), shape((half, DV)), shape((model, DV))],
        y_index[None],
        core[None],
        decay_logits[:, 0],
        normed_own,
        normed_other,
        *first_pieces,
        rope_frequency(),
        flops=1 << 32,
        smem=3,
        limit=14,
        scratch=[
            pltpu.VMEM((model, PROJECT), bf16),
            pltpu.VMEM((2 * half, DK), bf16),
            pltpu.VMEM((2 * half, DK), bf16),
            pltpu.VMEM((2 * half, DV), bf16),
            pltpu.VMEM((2 * half, DV), f32),
        ],
    )
    gated_partner = swap(gated_other)
    x_index = lax.axis_index("x").astype(jnp.int32)[None]
    far, right, left, here = call(
        output_body,
        [shape((own, model))] * 4,
        x_index,
        gated_own,
        gated_partner,
        out_own,
        swap(out_own),
        flops=1 << 30,
        smem=1,
        scratch=[pltpu.VMEM((half, 2 * DV), bf16)],
    )
    after_mix, channel_in = call(
        middle_body,
        [shape((own, model)), shape((own, model))],
        *sent(far, right, left),
        here,
        token_rows,
        row(mixer_out_gain),
        row(channel_in_gain),
    )
    third_other = swap(third_own)
    got_far, got_prev, got_next = sent(channel_in, channel_in, channel_in)
    blocks = (got_far, got_next, got_prev, channel_in)
    edges = jnp.concatenate([b[k : k + 1] for b in blocks for k in (0, own - 1)], axis=0)
    far, right, left, here = call(
        feed_body,
        [shape((own, model))] * 4,
        x_index,
        core[None],
        *blocks,
        swap(edges),
        third_own,
        third_other,
        taps,
        taps_other,
        flops=1 << 32,
        smem=2,
        limit=18,
        scratch=[
            pltpu.VMEM((half + 16, model), bf16),
            pltpu.VMEM((16, 2 * PAD), f32),
            pltpu.VMEM((half, 2 * PAD), bf16),
            pltpu.VMEM((model, THIRD), bf16),
            pltpu.VMEM((model, THIRD), bf16),
        ],
    )
    result = call(
        final_body,
        shape((own, model)),
        *sent(far, right, left),
        here,
        after_mix,
        row(channel_out_gain),
    )
    return result[None]


def solution(mesh):
    fs = mesh.shape["fs"]
    tp = mesh.shape["tp"]
    split = Mesh(
        mesh.devices.reshape(mesh.shape["rep"], fs // 4, 4, tp // 2, 2),
        ("rep", "z", "y", "x", "c"),
    )
    in_specs = (
        P(("rep", "z", "y"), TP, None),
        P(),
        P(FS, TP),
        P(FS, TP),
        P(FS, TP),
        P(FS, TP),
        P(None, TP),
        P(TP, FS),
        P(),
        P(),
        P(FS, TP),
        P(FS, TP),
        P(None, TP),
        P(None, TP),
        P(TP),
        P(TP),
        P(TP, FS),
        P(),
    )
    out_specs = P(("rep", "z", "y"), TP, None)
    return jax.shard_map(layer, mesh=split, in_specs=in_specs, out_specs=out_specs, check_vma=False)
```

```python
import functools

import jax
import jax.numpy as jnp
import numpy as np
from jax import lax
from jax.experimental import pallas as pl
from jax.experimental.pallas import tpu as pltpu
from jax.sharding import Mesh
from jax.sharding import PartitionSpec as P


DK = 128
DV = 256
TP = ("x", "c")
FS = ("z", "y")
RING = ("rep", "z")
SWAP = ((0, 1), (1, 0))
PAD = 384
PROJECT, FIRST, THIRD = 2 * DK + 2 * DV, 2 * DK + 3 * DV, 3 * PAD
Z_SHIFTS = (4, 3, 2, 1, 0, -1, -2, -3)
Z_ISSUE = (4, -3, 3, -2, 2, -1, 1)
Y_SHIFTS = (0, 1, 2, -1)
Y_ISSUE = (2, 1, -1)
epsilon = 1e-06
rope_base = 10000.0
bf16 = jnp.bfloat16
f32 = jnp.float32

VMEM = pl.BlockSpec(memory_space=pltpu.VMEM)
SMEM = pl.BlockSpec(memory_space=pltpu.SMEM)
HBM = pl.BlockSpec(memory_space=pltpu.HBM)


def call(body, out_shapes, *args, flops=0, smem=0, hbm=0, scratch=(), limit=6):
    specs = [SMEM] * smem + [HBM] * hbm + [VMEM] * (len(args) - smem - hbm)
    single = not isinstance(out_shapes, (list, tuple))
    args = [
        pltpu.with_memory_space_constraint(a, pltpu.HBM) if smem <= k < smem + hbm else a
        for k, a in enumerate(args)
    ]
    return pl.pallas_call(
        body,
        out_shape=out_shapes,
        in_specs=specs,
        out_specs=VMEM if single else [VMEM] * len(out_shapes),
        scratch_shapes=list(scratch),
        compiler_params=pltpu.CompilerParams(vmem_limit_bytes=limit << 20),
        cost_estimate=pl.CostEstimate(
            flops=max(flops, 1 << 24), bytes_accessed=1 << 21, transcendentals=0
        ),
    )(*args)


def shape(dims, kind=bf16):
    return jax.ShapeDtypeStruct(dims, kind)


def permuted(value, axes, shift, size):
    return lax.ppermute(value, axes, [(i, (i + shift) % size) for i in range(size)])


def swap(value):
    return lax.ppermute(value, "c", SWAP)


def exchanged(value):
    return lax.all_to_all(value, "x", 0, 0, tiled=True)


def rms_rows(values, gain):
    return values * lax.rsqrt(jnp.mean(values * values, axis=-1, keepdims=True) + epsilon) * gain


def pack_body(width, *refs):
    sources, out, places, arrived = refs[:8], refs[8], refs[9:17], refs[17]
    copies = [
        pltpu.make_async_copy(source, place, arrived.at[k])
        for k, (source, place) in enumerate(zip(sources, places))
    ]
    for copy in copies:
        copy.start()
    for copy in copies:
        copy.wait()
    at = 0
    for place in places[:5]:
        out[:, at : at + place.shape[1]] = place[...]
        at += place.shape[1]
    gap = jnp.zeros((out.shape[0], PAD - width), bf16)
    for place in places[5:]:
        out[:, at : at + PAD] = jnp.concatenate([place[...], gap], axis=1)
        at += PAD


def taps_body(width, ge_kernel, li_kernel, ge_bias, li_bias, out):
    out[...] = jnp.zeros(out.shape, f32)
    out[0:3, :width] = ge_kernel[...]
    out[3:6, :width] = li_kernel[...]
    out[6:7, :width] = ge_bias[...].reshape(1, width)
    out[7:8, :width] = li_bias[...].reshape(1, width)


def first_norm_body(tokens, gain, out):
    rows = rms_rows(tokens[...].astype(f32), gain[...]).astype(bf16)
    for k in range(out.shape[0]):
        out[k] = rows


def ring_order_body(index, *refs):
    pieces, (one, three) = refs[:8], refs[8:]
    for shift, piece in zip(Z_SHIFTS, pieces):
        at = lax.rem(index[2] - shift + 8, 8)
        one[at] = piece[:, :FIRST]
        three[at] = piece[:, FIRST:]


def line_order_body(index, *refs):
    pieces, out = refs[:4], refs[4]
    for shift, piece in zip(Y_SHIFTS, pieces):
        at = lax.rem(index[1] - shift + 4, 4)
        for z in range(8):
            out[z, at] = piece[z * 32 : z * 32 + 32, :]


def edges_body(far, after, before, own, out):
    rows = [p[k : k + 1, :].astype(f32) for p in (far, after, before, own) for k in (0, 127)]
    out[...] = jnp.concatenate(rows, axis=0).astype(bf16)


def summed(pieces):
    total = pieces[0][...].astype(f32)
    for piece in pieces[1:]:
        total = total + piece[...].astype(f32)
    return total * lax.rsqrt(jnp.mean(total * total, axis=-1, keepdims=True) + epsilon)


def middle_body(far, right, left, here, tokens, out_gain, in_gain, after_mix, channel_in):
    total = summed((here, right, left, far))
    mix = (tokens[...].astype(f32) + total * out_gain[...]).astype(bf16)
    after_mix[...] = mix
    channel_in[...] = rms_rows(mix.astype(f32), in_gain[...]).astype(bf16)


def final_body(far, right, left, here, after_mix, gain, out):
    total = summed((here, right, left, far))
    out[...] = (after_mix[...].astype(f32) + total * gain[...]).astype(bf16)


def log_sigmoid_tile(logit):
    value = jnp.full((8, 128), logit, f32)
    tile = jnp.minimum(value, 0.0) - jnp.log1p(jnp.exp(-jnp.abs(value)))
    return tile[0:1, 0:1]


def attend_body(
    index, logits, own, other, p0, p1, p2, p3, frequency, out_own, out_other, mo, w, qs, ks, vs, gs
):
    y, core = index[1], index[3]
    for shift, piece in zip(Y_SHIFTS, (p0, p1, p2, p3)):
        at = lax.rem(y - shift + 4, 4) * 32
        for z in range(8):
            place = pl.ds(pl.multiple_of(z * 128 + at, 32), 32)
            w[place, :] = piece[z * 32 : z * 32 + 32, :PROJECT]
            mo[place, :] = piece[z * 32 : z * 32 + 32, PROJECT:]
    inside = lax.broadcasted_iota(jnp.int32, (128, DK), 0).astype(f32) * frequency[...]
    cos_in, sin_in = jnp.cos(inside), jnp.sin(inside)
    block = lax.broadcasted_iota(jnp.int32, (8, DK), 0)
    base = (block % 4) * 256 + jnp.where(block < 4, core, 1 - core) * 128
    start = base.astype(f32) * frequency[...]
    cos_at, sin_at = jnp.cos(start), jnp.sin(start)
    sign = jnp.where(lax.broadcasted_iota(jnp.int32, (128, DK), 1) < DK // 2, -1.0, 1.0)
    cos_turn, sin_turn = cos_in * sign, sin_in * sign

    def tables(r):
        c, s = cos_at[r : r + 1, :], sin_at[r : r + 1, :]
        return c * cos_in - s * sin_in, s * cos_turn + c * sin_turn

    step = 256
    for r in range(0, 1024, step):
        rows = own[r : r + step, :] if r < 512 else other[r - 512 : r - 512 + step, :]
        projected = dot(rows, w[...])
        pair = [tables(b) for b in range(r // 128, (r + step) // 128)]
        cos = jnp.concatenate([p[0] for p in pair], axis=0)
        sin = jnp.concatenate([p[1] for p in pair], axis=0)
        q = projected[:, :DK]
        k = projected[:, DK : 2 * DK]
        qs[r : r + step, :] = (q * cos + pltpu.roll(q, DK // 2, 1) * sin).astype(bf16)
        ks[r : r + step, :] = (
            (k * cos + pltpu.roll(k, DK // 2, 1) * sin) * DK ** (-0.5)
        ).astype(bf16)
        vs[r : r + step, :] = projected[:, 2 * DK : 2 * DK + DV].astype(bf16)
        gs[r : r + step, :] = projected[:, 2 * DK + DV :]
    forward = log_sigmoid_tile(logits[0])
    backward = log_sigmoid_tile(logits[1])
    lag = (
        lax.broadcasted_iota(jnp.int32, (128, 128), 0)
        - lax.broadcasted_iota(jnp.int32, (128, 128), 1)
    ).astype(f32)
    ahead, behind = lag * forward, lag * -backward
    side = ((2 * core - 1) * 128).astype(f32)
    for r in range(8):
        decays = []
        for c in range(8):
            gap = float((r % 4 - c % 4) * 256)
            if r < 4 <= c:
                gap = gap + side
            if c < 4 <= r:
                gap = gap - side
            decays.append(jnp.exp(jnp.minimum(ahead + gap * forward, behind - gap * backward)))
        rows = slice(r * 128, r * 128 + 128)
        scores = dot_nt(qs[rows, :], ks[...])
        weighted = (scores * jnp.concatenate(decays, axis=1)).astype(bf16)
        kept = head_norm(dot(weighted, vs[...]))
        gate = gs[rows, :]
        gated = (kept * (gate / (1.0 + jnp.exp(-gate)))).astype(bf16)
        if r < 4:
            out_own[rows, :] = gated
        else:
            out_other[r * 128 - 512 : r * 128 - 384, :] = gated


def output_body(index, mine, theirs, my_weights, their_weights, far, right, left, here, lines):
    for place, ahead in enumerate((2, 1, 3, 0)):
        block = lax.rem(index[0] + ahead, 4)
        rows = pl.ds(pl.multiple_of(block * 128, 128), 128)
        lines[place * 128 : place * 128 + 128, :DV] = mine[rows, :]
        lines[place * 128 : place * 128 + 128, DV:] = theirs[rows, :]
    for d in range(0, 1024, 256):
        columns = slice(d, d + 256)
        total = dot_nt(lines[:, :DV], my_weights[columns, :]) + dot_nt(
            lines[:, DV:], their_weights[columns, :]
        )
        for place, out in enumerate((far, right, left, here)):
            out[:, columns] = total[place * 128 : place * 128 + 128, :].astype(bf16)


def feed_block(main, before, after, taps):
    line = lax.broadcasted_iota(jnp.int32, (128, 1), 0)
    prev = jnp.where(line == 0, before, pltpu.roll(main, 1, 0))
    nxt = jnp.where(line == 127, after, pltpu.roll(main, 127, 0))
    kernel = [
        jnp.concatenate([taps[t : t + 1, :], taps[t + 3 : t + 4, :]], axis=1) for t in range(3)
    ]
    bias = jnp.concatenate([taps[6:7, :], taps[7:8, :]], axis=1)
    conv = kernel[0] * prev + kernel[1] * main + kernel[2] * nxt + bias
    value = conv[:, :PAD]
    bent = value * (0.5 + 0.5 * jnp.tanh(0.7978845608028654 * (value + 0.044715 * value**3)))
    return (bent * conv[:, PAD:]).astype(bf16)


def feed_body(
    index,
    got_far,
    got_next,
    got_prev,
    own,
    edges,
    mine,
    theirs,
    my_taps,
    their_taps,
    far,
    right,
    left,
    here,
    lines,
    outer,
    hidden,
):
    core = index[3]
    blocks = [lax.rem(index[0] + k, 4) for k in (2, 1, 3, 0)]
    for place, piece in enumerate((got_far, got_next, got_prev, own)):
        lines[place * 128 : place * 128 + 128, :] = piece[...]
    lines[512:520, :] = edges[...]
    lines[520:528, :] = jnp.zeros((8, 1024), bf16)
    outer[...] = jnp.zeros(outer.shape, f32)
    for part, (weights, taps) in enumerate(((mine, my_taps), (theirs, their_taps))):
        main = dot(lines[...], weights[:, : 2 * PAD])
        for place, block in enumerate(blocks):
            outer[pl.ds(8 + block, 1), :] = main[512 + 2 * place : 513 + 2 * place, :]
            outer[pl.ds(1 + block, 1), :] = main[513 + 2 * place : 514 + 2 * place, :]
        for place, block in enumerate(blocks):
            inner = slice(place * 128, place * 128 + 128)
            before = outer[pl.ds(block + core, 1), :]
            after = outer[pl.ds(8 + block + core, 1), :]
            hidden[inner, part * PAD : part * PAD + PAD] = feed_block(
                main[inner, :], before, after, taps
            )
    for d in range(0, 1024, 256):
        columns = slice(d, d + 256)
        total = dot_nt(hidden[:, :PAD], mine[columns, 2 * PAD :]) + dot_nt(
            hidden[:, PAD:], theirs[columns, 2 * PAD :]
        )
        for place, out in enumerate((far, right, left, here)):
            out[:, columns] = total[place * 128 : place * 128 + 128, :].astype(bf16)


def head_norm(values):
    centred = values - jnp.mean(values, axis=-1, keepdims=True)
    return centred * lax.rsqrt(jnp.mean(centred * centred, axis=-1, keepdims=True) + epsilon)


def dot(a, b):
    return jnp.dot(a, b, preferred_element_type=f32)


def dot_nt(a, b):
    return lax.dot_general(a, b, (((1,), (1,)), ((), ())), preferred_element_type=f32)


def line_gather(piece):
    got = {0: piece}
    for shift in Y_ISSUE:
        got[shift] = permuted(piece, "y", shift, 4)
    return [got[s].reshape(256, piece.shape[-1]) for s in Y_SHIFTS]


def sent(far, right, left):
    return (permuted(far, "x", 2, 4), permuted(right, "x", 1, 4), permuted(left, "x", -1, 4))


def rope_frequency():
    half = DK // 2
    frequency = 1.0 / rope_base ** (np.arange(half, dtype=np.float32) / half)
    return jnp.asarray(np.tile(frequency.astype(np.float32), 2)[None])


def layer(
    tokens,
    mixer_in_gain,
    query_weight,
    key_weight,
    value_weight,
    gate_weight,
    decay_logits,
    mixer_output,
    mixer_out_gain,
    channel_in_gain,
    gelu_weight,
    linear_weight,
    gelu_kernel,
    linear_kernel,
    gelu_bias,
    linear_bias,
    down_weight,
    channel_out_gain,
):
    place = jnp.stack([lax.axis_index(a).astype(jnp.int32) for a in ("x", "y", "z", "c")])
    place, query_weight = lax.optimization_barrier((place, query_weight))
    token_rows = tokens[0]
    own, model = token_rows.shape
    chips = lax.axis_size("x")
    half = chips * own
    width = gelu_weight.shape[1]

    def row(vector):
        return vector.reshape(1, -1)

    parts = (
        query_weight,
        key_weight,
        value_weight,
        gate_weight,
        mixer_output.T,
        gelu_weight,
        linear_weight,
        down_weight.T,
    )
    packed = call(
        functools.partial(pack_body, width),
        shape((32, FIRST + THIRD)),
        *parts,
        hbm=8,
        scratch=[pltpu.VMEM(part.shape, bf16) for part in parts]
        + [pltpu.SemaphoreType.DMA((8,))],
    )
    got = {0: packed}
    for shift in Z_ISSUE:
        got[shift] = permuted(packed, RING, shift, 16)
    spread = call(
        first_norm_body, shape((chips, own, model)), token_rows, row(mixer_in_gain), limit=60
    )
    normed_own = exchanged(spread).reshape(half, model)
    normed_other = swap(normed_own)
    first_z, third_z = call(
        ring_order_body,
        [shape((8, 32, FIRST)), shape((8, 32, THIRD))],
        place,
        *[got[s] for s in Z_SHIFTS],
        smem=1,
    )
    first_pieces = line_gather(first_z)
    third_pieces = line_gather(third_z)
    taps = call(
        functools.partial(taps_body, width),
        shape((8, PAD), f32),
        gelu_kernel,
        linear_kernel,
        gelu_bias,
        linear_bias,
    )
    taps_other = swap(taps)
    gated_own, gated_other, out_own = call(
        attend_body,
        [shape((half, DV)), shape((half, DV)), shape((model, DV))],
        place,
        decay_logits[:, 0],
        normed_own,
        normed_other,
        *first_pieces,
        rope_frequency(),
        flops=1 << 32,
        smem=2,
        limit=10,
        scratch=[
            pltpu.VMEM((model, PROJECT), bf16),
            pltpu.VMEM((2 * half, DK), bf16),
            pltpu.VMEM((2 * half, DK), bf16),
            pltpu.VMEM((2 * half, DV), bf16),
            pltpu.VMEM((2 * half, DV), f32),
        ],
    )
    gated_partner = swap(gated_other)
    far, right, left, here = call(
        output_body,
        [shape((own, model))] * 4,
        place,
        gated_own,
        gated_partner,
        out_own,
        swap(out_own),
        flops=1 << 30,
        smem=1,
        scratch=[pltpu.VMEM((half, 2 * DV), bf16)],
    )
    after_mix, channel_in = call(
        middle_body,
        [shape((own, model)), shape((own, model))],
        *sent(far, right, left),
        here,
        token_rows,
        row(mixer_out_gain),
        row(channel_in_gain),
    )
    third_own = call(
        line_order_body, shape((8, 4, 32, THIRD)), place, *third_pieces, smem=1
    ).reshape(model, THIRD)
    third_other = swap(third_own)
    got_far, got_prev, got_next = sent(channel_in, channel_in, channel_in)
    blocks = (got_far, got_next, got_prev, channel_in)
    edges = call(edges_body, shape((8, model)), *blocks)
    far, right, left, here = call(
        feed_body,
        [shape((own, model))] * 4,
        place,
        *blocks,
        swap(edges),
        third_own,
        third_other,
        taps,
        taps_other,
        flops=1 << 32,
        smem=1,
        limit=18,
        scratch=[
            pltpu.VMEM((half + 16, model), bf16),
            pltpu.VMEM((16, 2 * PAD), f32),
            pltpu.VMEM((half, 2 * PAD), bf16),
        ],
    )
    result = call(
        final_body,
        shape((own, model)),
        *sent(far, right, left),
        here,
        after_mix,
        row(channel_out_gain),
    )
    return result[None]


def solution(mesh):
    fs = mesh.shape["fs"]
    tp = mesh.shape["tp"]
    split = Mesh(
        mesh.devices.reshape(mesh.shape["rep"], fs // 4, 4, tp // 2, 2),
        ("rep", "z", "y", "x", "c"),
    )
    in_specs = (
        P(("rep", "z", "y"), TP, None),
        P(),
        P(FS, TP),
        P(FS, TP),
        P(FS, TP),
        P(FS, TP),
        P(None, TP),
        P(TP, FS),
        P(),
        P(),
        P(FS, TP),
        P(FS, TP),
        P(None, TP),
        P(None, TP),
        P(TP),
        P(TP),
        P(TP, FS),
        P(),
    )
    out_specs = P(("rep", "z", "y"), TP, None)
    return jax.shard_map(layer, mesh=split, in_specs=in_specs, out_specs=out_specs, check_vma=False)
```

```python
import functools

import jax
import jax.numpy as jnp
import numpy as np
from jax import lax
from jax.experimental import pallas as pl
from jax.experimental.pallas import tpu as pltpu
from jax.sharding import Mesh
from jax.sharding import PartitionSpec as P


DK = 128
DV = 256
TP = ("x", "c")
FS = ("z", "y")
RING = ("rep", "z")
SWAP = ((0, 1), (1, 0))
PAD = 384
PROJECT, FIRST, THIRD = 2 * DK + 2 * DV, 2 * DK + 3 * DV, 3 * PAD
Z_ISSUE = (4, 5, 6, 7, 3, 2, 1)
PARTNERS = (2, 1, 3)
epsilon = 1e-06
rope_base = 10000.0
bf16 = jnp.bfloat16
f32 = jnp.float32

VMEM = pl.BlockSpec(memory_space=pltpu.VMEM)
SMEM = pl.BlockSpec(memory_space=pltpu.SMEM)
HBM = pl.BlockSpec(memory_space=pltpu.HBM)


def call(body, out_shapes, *args, flops=0, smem=0, hbm=0, scratch=(), limit=6):
    specs = [SMEM] * smem + [HBM] * hbm + [VMEM] * (len(args) - smem - hbm)
    single = not isinstance(out_shapes, (list, tuple))
    args = [
        pltpu.with_memory_space_constraint(a, pltpu.HBM) if smem <= k < smem + hbm else a
        for k, a in enumerate(args)
    ]
    return pl.pallas_call(
        body,
        out_shape=out_shapes,
        in_specs=specs,
        out_specs=VMEM if single else [VMEM] * len(out_shapes),
        scratch_shapes=list(scratch),
        compiler_params=pltpu.CompilerParams(vmem_limit_bytes=limit << 20),
        cost_estimate=pl.CostEstimate(
            flops=max(flops, 1 << 24), bytes_accessed=1 << 21, transcendentals=0
        ),
    )(*args)


def shape(dims, kind=bf16):
    return jax.ShapeDtypeStruct(dims, kind)


def line_pairs(k):
    return [(i, i ^ k) for i in range(4)]


def ring_pairs(k):
    pairs = []
    for i in range(16):
        here = i // 8 * 8 + (i % 8 ^ k)
        there = (here + 8) % 16
        gap = min((here - i) % 16, (i - here) % 16)
        pairs.append((i, here if gap <= 4 else there))
    return pairs


def swap(value):
    return lax.ppermute(value, "c", SWAP)


def exchanged(value):
    return lax.all_to_all(value, "x", 0, 0, tiled=True)


def rms_rows(values, gain):
    return values * lax.rsqrt(jnp.mean(values * values, axis=-1, keepdims=True) + epsilon) * gain


def pack_body(width, *refs):
    sources, out, places, arrived = refs[:8], refs[8], refs[9:17], refs[17]
    copies = [
        pltpu.make_async_copy(source, place, arrived.at[k])
        for k, (source, place) in enumerate(zip(sources, places))
    ]
    for copy in copies:
        copy.start()
    for copy in copies:
        copy.wait()
    at = 0
    for place in places[:5]:
        out[:, at : at + place.shape[1]] = place[...]
        at += place.shape[1]
    gap = jnp.zeros((out.shape[0], PAD - width), bf16)
    for place in places[5:]:
        out[:, at : at + PAD] = jnp.concatenate([place[...], gap], axis=1)
        at += PAD


def taps_body(width, ge_kernel, li_kernel, ge_bias, li_bias, out):
    out[...] = jnp.zeros(out.shape, f32)
    out[0:3, :width] = ge_kernel[...]
    out[3:6, :width] = li_kernel[...]
    out[6:7, :width] = ge_bias[...].reshape(1, width)
    out[7:8, :width] = li_bias[...].reshape(1, width)


def first_norm_body(tokens, gain, out):
    rows = rms_rows(tokens[...].astype(f32), gain[...]).astype(bf16)
    for k in range(out.shape[0]):
        out[k] = rows


def ring_order_body(index, *refs):
    pieces, (one, three) = refs[:8], refs[8:]
    for k, piece in enumerate(pieces):
        at = index[2] ^ k
        one[at] = piece[:, :FIRST]
        three[at] = piece[:, FIRST:]


def line_order_body(index, *refs):
    pieces, out = refs[:4], refs[4]
    for k, piece in enumerate(pieces):
        at = index[1] ^ k
        for z in range(8):
            out[z, at] = piece[z * 32 : z * 32 + 32, :]


def edges_body(far, after, before, own, out):
    rows = [p[k : k + 1, :].astype(f32) for p in (far, after, before, own) for k in (0, 127)]
    out[...] = jnp.concatenate(rows, axis=0).astype(bf16)


def summed(pieces):
    total = pieces[0][...].astype(f32)
    for piece in pieces[1:]:
        total = total + piece[...].astype(f32)
    return total * lax.rsqrt(jnp.mean(total * total, axis=-1, keepdims=True) + epsilon)


def middle_body(far, right, left, here, tokens, out_gain, in_gain, after_mix, channel_in):
    total = summed((here, right, left, far))
    mix = (tokens[...].astype(f32) + total * out_gain[...]).astype(bf16)
    after_mix[...] = mix
    channel_in[...] = rms_rows(mix.astype(f32), in_gain[...]).astype(bf16)


def final_body(far, right, left, here, after_mix, gain, out):
    total = summed((here, right, left, far))
    out[...] = (after_mix[...].astype(f32) + total * gain[...]).astype(bf16)


def log_sigmoid_tile(logit):
    value = jnp.full((8, 128), logit, f32)
    tile = jnp.minimum(value, 0.0) - jnp.log1p(jnp.exp(-jnp.abs(value)))
    return tile[0:1, 0:1]


def attend_body(
    index, logits, own, other, p0, p1, p2, p3, frequency, out_own, out_other, mo, w, qs, ks, vs, gs
):
    y, core = index[1], index[3]
    for k, piece in enumerate((p0, p1, p2, p3)):
        at = (y ^ k) * 32
        for z in range(8):
            place = pl.ds(pl.multiple_of(z * 128 + at, 32), 32)
            w[place, :] = piece[z * 32 : z * 32 + 32, :PROJECT]
            mo[place, :] = piece[z * 32 : z * 32 + 32, PROJECT:]
    inside = lax.broadcasted_iota(jnp.int32, (128, DK), 0).astype(f32) * frequency[...]
    cos_in, sin_in = jnp.cos(inside), jnp.sin(inside)
    block = lax.broadcasted_iota(jnp.int32, (8, DK), 0)
    base = (block % 4) * 256 + jnp.where(block < 4, core, 1 - core) * 128
    start = base.astype(f32) * frequency[...]
    cos_at, sin_at = jnp.cos(start), jnp.sin(start)
    sign = jnp.where(lax.broadcasted_iota(jnp.int32, (128, DK), 1) < DK // 2, -1.0, 1.0)
    cos_turn, sin_turn = cos_in * sign, sin_in * sign

    def tables(r):
        c, s = cos_at[r : r + 1, :], sin_at[r : r + 1, :]
        return c * cos_in - s * sin_in, s * cos_turn + c * sin_turn

    step = 256
    for r in range(0, 1024, step):
        rows = own[r : r + step, :] if r < 512 else other[r - 512 : r - 512 + step, :]
        projected = dot(rows, w[...])
        pair = [tables(b) for b in range(r // 128, (r + step) // 128)]
        cos = jnp.concatenate([p[0] for p in pair], axis=0)
        sin = jnp.concatenate([p[1] for p in pair], axis=0)
        q = projected[:, :DK]
        k = projected[:, DK : 2 * DK]
        qs[r : r + step, :] = (q * cos + pltpu.roll(q, DK // 2, 1) * sin).astype(bf16)
        ks[r : r + step, :] = (
            (k * cos + pltpu.roll(k, DK // 2, 1) * sin) * DK ** (-0.5)
        ).astype(bf16)
        vs[r : r + step, :] = projected[:, 2 * DK : 2 * DK + DV].astype(bf16)
        gs[r : r + step, :] = projected[:, 2 * DK + DV :]
    forward = log_sigmoid_tile(logits[0])
    backward = log_sigmoid_tile(logits[1])
    lag = (
        lax.broadcasted_iota(jnp.int32, (128, 128), 0)
        - lax.broadcasted_iota(jnp.int32, (128, 128), 1)
    ).astype(f32)
    ahead, behind = lag * forward, lag * -backward
    side = ((2 * core - 1) * 128).astype(f32)
    for r in range(8):
        decays = []
        for c in range(8):
            gap = float((r % 4 - c % 4) * 256)
            if r < 4 <= c:
                gap = gap + side
            if c < 4 <= r:
                gap = gap - side
            decays.append(jnp.exp(jnp.minimum(ahead + gap * forward, behind - gap * backward)))
        rows = slice(r * 128, r * 128 + 128)
        scores = dot_nt(qs[rows, :], ks[...])
        weighted = (scores * jnp.concatenate(decays, axis=1)).astype(bf16)
        kept = head_norm(dot(weighted, vs[...]))
        gate = gs[rows, :]
        gated = (kept * (gate / (1.0 + jnp.exp(-gate)))).astype(bf16)
        if r < 4:
            out_own[rows, :] = gated
        else:
            out_other[r * 128 - 512 : r * 128 - 384, :] = gated


def output_body(index, mine, theirs, my_weights, their_weights, far, right, left, here, lines):
    for place, k in enumerate((2, 1, 3, 0)):
        block = index[0] ^ k
        rows = pl.ds(pl.multiple_of(block * 128, 128), 128)
        lines[place * 128 : place * 128 + 128, :DV] = mine[rows, :]
        lines[place * 128 : place * 128 + 128, DV:] = theirs[rows, :]
    for d in range(0, 1024, 256):
        columns = slice(d, d + 256)
        total = dot_nt(lines[:, :DV], my_weights[columns, :]) + dot_nt(
            lines[:, DV:], their_weights[columns, :]
        )
        for place, out in enumerate((far, right, left, here)):
            out[:, columns] = total[place * 128 : place * 128 + 128, :].astype(bf16)


def feed_block(main, before, after, taps):
    line = lax.broadcasted_iota(jnp.int32, (128, 1), 0)
    prev = jnp.where(line == 0, before, pltpu.roll(main, 1, 0))
    nxt = jnp.where(line == 127, after, pltpu.roll(main, 127, 0))
    kernel = [
        jnp.concatenate([taps[t : t + 1, :], taps[t + 3 : t + 4, :]], axis=1) for t in range(3)
    ]
    bias = jnp.concatenate([taps[6:7, :], taps[7:8, :]], axis=1)
    conv = kernel[0] * prev + kernel[1] * main + kernel[2] * nxt + bias
    value = conv[:, :PAD]
    bent = value * (0.5 + 0.5 * jnp.tanh(0.7978845608028654 * (value + 0.044715 * value**3)))
    return (bent * conv[:, PAD:]).astype(bf16)


def feed_body(
    index,
    got_far,
    got_next,
    got_prev,
    own,
    edges,
    mine,
    theirs,
    my_taps,
    their_taps,
    far,
    right,
    left,
    here,
    lines,
    outer,
    hidden,
):
    core = index[3]
    blocks = [index[0] ^ k for k in (2, 1, 3, 0)]
    for place, piece in enumerate((got_far, got_next, got_prev, own)):
        lines[place * 128 : place * 128 + 128, :] = piece[...]
    lines[512:520, :] = edges[...]
    lines[520:528, :] = jnp.zeros((8, 1024), bf16)
    outer[...] = jnp.zeros(outer.shape, f32)
    for part, (weights, taps) in enumerate(((mine, my_taps), (theirs, their_taps))):
        main = dot(lines[...], weights[:, : 2 * PAD])
        for place, block in enumerate(blocks):
            outer[pl.ds(8 + block, 1), :] = main[512 + 2 * place : 513 + 2 * place, :]
            outer[pl.ds(1 + block, 1), :] = main[513 + 2 * place : 514 + 2 * place, :]
        for place, block in enumerate(blocks):
            inner = slice(place * 128, place * 128 + 128)
            before = outer[pl.ds(block + core, 1), :]
            after = outer[pl.ds(8 + block + core, 1), :]
            hidden[inner, part * PAD : part * PAD + PAD] = feed_block(
                main[inner, :], before, after, taps
            )
    for d in range(0, 1024, 256):
        columns = slice(d, d + 256)
        total = dot_nt(hidden[:, :PAD], mine[columns, 2 * PAD :]) + dot_nt(
            hidden[:, PAD:], theirs[columns, 2 * PAD :]
        )
        for place, out in enumerate((far, right, left, here)):
            out[:, columns] = total[place * 128 : place * 128 + 128, :].astype(bf16)


def head_norm(values):
    centred = values - jnp.mean(values, axis=-1, keepdims=True)
    return centred * lax.rsqrt(jnp.mean(centred * centred, axis=-1, keepdims=True) + epsilon)


def dot(a, b):
    return jnp.dot(a, b, preferred_element_type=f32)


def dot_nt(a, b):
    return lax.dot_general(a, b, (((1,), (1,)), ((), ())), preferred_element_type=f32)


def line_gather(piece):
    got = {0: piece}
    for k in PARTNERS:
        got[k] = lax.ppermute(piece, "y", line_pairs(k))
    return [got[k].reshape(256, piece.shape[-1]) for k in range(4)]


def sent(blocks):
    return [lax.ppermute(block, "x", line_pairs(k)) for k, block in zip(PARTNERS, blocks)]


def rope_frequency():
    half = DK // 2
    frequency = 1.0 / rope_base ** (np.arange(half, dtype=np.float32) / half)
    return jnp.asarray(np.tile(frequency.astype(np.float32), 2)[None])


def layer(
    tokens,
    mixer_in_gain,
    query_weight,
    key_weight,
    value_weight,
    gate_weight,
    decay_logits,
    mixer_output,
    mixer_out_gain,
    channel_in_gain,
    gelu_weight,
    linear_weight,
    gelu_kernel,
    linear_kernel,
    gelu_bias,
    linear_bias,
    down_weight,
    channel_out_gain,
):
    place = jnp.stack([lax.axis_index(a).astype(jnp.int32) for a in ("x", "y", "z", "c")])
    place, query_weight = lax.optimization_barrier((place, query_weight))
    token_rows = tokens[0]
    own, model = token_rows.shape
    chips = lax.axis_size("x")
    half = chips * own
    width = gelu_weight.shape[1]

    def row(vector):
        return vector.reshape(1, -1)

    parts = (
        query_weight,
        key_weight,
        value_weight,
        gate_weight,
        mixer_output.T,
        gelu_weight,
        linear_weight,
        down_weight.T,
    )
    packed = call(
        functools.partial(pack_body, width),
        shape((32, FIRST + THIRD)),
        *parts,
        hbm=8,
        scratch=[pltpu.VMEM(part.shape, bf16) for part in parts]
        + [pltpu.SemaphoreType.DMA((8,))],
    )
    got = {0: packed}
    for k in Z_ISSUE:
        got[k] = lax.ppermute(packed, RING, ring_pairs(k))
    spread = call(
        first_norm_body, shape((chips, own, model)), token_rows, row(mixer_in_gain), limit=60
    )
    normed_own = exchanged(spread).reshape(half, model)
    normed_other = swap(normed_own)
    first_z, third_z = call(
        ring_order_body,
        [shape((8, 32, FIRST)), shape((8, 32, THIRD))],
        place,
        *[got[k] for k in range(8)],
        smem=1,
    )
    first_pieces = line_gather(first_z)
    third_pieces = line_gather(third_z)
    taps = call(
        functools.partial(taps_body, width),
        shape((8, PAD), f32),
        gelu_kernel,
        linear_kernel,
        gelu_bias,
        linear_bias,
    )
    taps_other = swap(taps)
    gated_own, gated_other, out_own = call(
        attend_body,
        [shape((half, DV)), shape((half, DV)), shape((model, DV))],
        place,
        decay_logits[:, 0],
        normed_own,
        normed_other,
        *first_pieces,
        rope_frequency(),
        flops=1 << 32,
        smem=2,
        limit=10,
        scratch=[
            pltpu.VMEM((model, PROJECT), bf16),
            pltpu.VMEM((2 * half, DK), bf16),
            pltpu.VMEM((2 * half, DK), bf16),
            pltpu.VMEM((2 * half, DV), bf16),
            pltpu.VMEM((2 * half, DV), f32),
        ],
    )
    gated_partner = swap(gated_other)
    far, right, left, here = call(
        output_body,
        [shape((own, model))] * 4,
        place,
        gated_own,
        gated_partner,
        out_own,
        swap(out_own),
        flops=1 << 30,
        smem=1,
        scratch=[pltpu.VMEM((half, 2 * DV), bf16)],
    )
    after_mix, channel_in = call(
        middle_body,
        [shape((own, model)), shape((own, model))],
        *sent((far, right, left)),
        here,
        token_rows,
        row(mixer_out_gain),
        row(channel_in_gain),
    )
    third_own = call(
        line_order_body, shape((8, 4, 32, THIRD)), place, *third_pieces, smem=1
    ).reshape(model, THIRD)
    third_other = swap(third_own)
    blocks = (*sent([channel_in] * 3), channel_in)
    edges = call(edges_body, shape((8, model)), *blocks)
    far, right, left, here = call(
        feed_body,
        [shape((own, model))] * 4,
        place,
        *blocks,
        swap(edges),
        third_own,
        third_other,
        taps,
        taps_other,
        flops=1 << 32,
        smem=1,
        limit=18,
        scratch=[
            pltpu.VMEM((half + 16, model), bf16),
            pltpu.VMEM((16, 2 * PAD), f32),
            pltpu.VMEM((half, 2 * PAD), bf16),
        ],
    )
    result = call(
        final_body,
        shape((own, model)),
        *sent((far, right, left)),
        here,
        after_mix,
        row(channel_out_gain),
    )
    return result[None]


def solution(mesh):
    fs = mesh.shape["fs"]
    tp = mesh.shape["tp"]
    split = Mesh(
        mesh.devices.reshape(mesh.shape["rep"], fs // 4, 4, tp // 2, 2),
        ("rep", "z", "y", "x", "c"),
    )
    in_specs = (
        P(("rep", "z", "y"), TP, None),
        P(),
        P(FS, TP),
        P(FS, TP),
        P(FS, TP),
        P(FS, TP),
        P(None, TP),
        P(TP, FS),
        P(),
        P(),
        P(FS, TP),
        P(FS, TP),
        P(None, TP),
        P(None, TP),
        P(TP),
        P(TP),
        P(TP, FS),
        P(),
    )
    out_specs = P(("rep", "z", "y"), TP, None)
    return jax.shard_map(layer, mesh=split, in_specs=in_specs, out_specs=out_specs, check_vma=False)
```

```python
import functools

import jax
import jax.numpy as jnp
import numpy as np
from jax import lax
from jax.experimental import pallas as pl
from jax.experimental.pallas import tpu as pltpu
from jax.sharding import Mesh
from jax.sharding import PartitionSpec as P


DK = 128
DV = 256
TP = ("x", "c")
FS = ("z", "y")
RING = ("rep", "z")
SWAP = ((0, 1), (1, 0))
PAD = 384
FIRST, SECOND, THIRD = 2 * DK + 2 * DV, DV, 3 * PAD
Z_SHIFTS = (4, 3, 2, 1, 0, -1, -2, -3)
Z_ISSUE = (4, -3, 3, -2, 2, -1, 1)
PARTNERS = (2, 1, 3)
epsilon = 1e-06
rope_base = 10000.0
bf16 = jnp.bfloat16
f32 = jnp.float32

VMEM = pl.BlockSpec(memory_space=pltpu.VMEM)
SMEM = pl.BlockSpec(memory_space=pltpu.SMEM)
HBM = pl.BlockSpec(memory_space=pltpu.HBM)


def call(body, out_shapes, *args, flops=0, smem=0, hbm=0, scratch=(), limit=6):
    specs = [SMEM] * smem + [HBM] * hbm + [VMEM] * (len(args) - smem - hbm)
    single = not isinstance(out_shapes, (list, tuple))
    args = [
        pltpu.with_memory_space_constraint(a, pltpu.HBM) if smem <= k < smem + hbm else a
        for k, a in enumerate(args)
    ]
    return pl.pallas_call(
        body,
        out_shape=out_shapes,
        in_specs=specs,
        out_specs=VMEM if single else [VMEM] * len(out_shapes),
        scratch_shapes=list(scratch),
        compiler_params=pltpu.CompilerParams(vmem_limit_bytes=limit << 20),
        cost_estimate=pl.CostEstimate(
            flops=max(flops, 1 << 24), bytes_accessed=1 << 21, transcendentals=0
        ),
    )(*args)


def shape(dims, kind=bf16):
    return jax.ShapeDtypeStruct(dims, kind)


def line_pairs(k):
    return [(i, i ^ k) for i in range(4)]


def ring_pairs(shift):
    return [(i, (i + shift) % 16) for i in range(16)]


def swap(value):
    return lax.ppermute(value, "c", SWAP)


def exchanged(value):
    return lax.all_to_all(value, "x", 0, 0, tiled=True)


def rms_rows(values, gain):
    return values * lax.rsqrt(jnp.mean(values * values, axis=-1, keepdims=True) + epsilon) * gain


def pack_body(width, *refs):
    sources, out, places, arrived = refs[:8], refs[8], refs[9:17], refs[17]
    copies = [
        pltpu.make_async_copy(source, place, arrived.at[k])
        for k, (source, place) in enumerate(zip(sources, places))
    ]
    for copy in copies:
        copy.start()
    for copy in copies:
        copy.wait()
    at = 0
    for place in places[:5]:
        out[:, at : at + place.shape[1]] = place[...]
        at += place.shape[1]
    gap = jnp.zeros((out.shape[0], PAD - width), bf16)
    for place in places[5:]:
        out[:, at : at + PAD] = jnp.concatenate([place[...], gap], axis=1)
        at += PAD


def taps_body(width, ge_kernel, li_kernel, ge_bias, li_bias, out):
    out[...] = jnp.zeros(out.shape, f32)
    out[0:3, :width] = ge_kernel[...]
    out[3:6, :width] = li_kernel[...]
    out[6:7, :width] = ge_bias[...].reshape(1, width)
    out[7:8, :width] = li_bias[...].reshape(1, width)


def first_norm_body(tokens, gain, out):
    rows = rms_rows(tokens[...].astype(f32), gain[...]).astype(bf16)
    for k in range(out.shape[0]):
        out[k] = rows


def ring_order_body(index, *refs):
    pieces, (one, two, three) = refs[:8], refs[8:]
    for shift, piece in zip(Z_SHIFTS, pieces):
        at = lax.rem(index[2] - shift + 8, 8)
        one[at] = piece[:, :FIRST]
        two[at] = piece[:, FIRST : FIRST + SECOND]
        three[at] = piece[:, FIRST + SECOND :]


def line_order_body(index, *refs):
    pieces, out = refs[:4], refs[4]
    for k, piece in enumerate(pieces):
        at = index[1] ^ k
        for z in range(8):
            out[z, at] = piece[z * 32 : z * 32 + 32, :]


def edges_body(far, after, before, own, out):
    rows = [p[k : k + 1, :].astype(f32) for p in (far, after, before, own) for k in (0, 127)]
    out[...] = jnp.concatenate(rows, axis=0).astype(bf16)


def summed(pieces):
    total = pieces[0][...].astype(f32)
    for piece in pieces[1:]:
        total = total + piece[...].astype(f32)
    return total * lax.rsqrt(jnp.mean(total * total, axis=-1, keepdims=True) + epsilon)


def middle_body(far, right, left, here, tokens, out_gain, in_gain, after_mix, channel_in):
    total = summed((here, right, left, far))
    mix = (tokens[...].astype(f32) + total * out_gain[...]).astype(bf16)
    after_mix[...] = mix
    channel_in[...] = rms_rows(mix.astype(f32), in_gain[...]).astype(bf16)


def final_body(far, right, left, here, after_mix, gain, out):
    total = summed((here, right, left, far))
    out[...] = (after_mix[...].astype(f32) + total * gain[...]).astype(bf16)


def log_sigmoid_tile(logit):
    value = jnp.full((8, 128), logit, f32)
    tile = jnp.minimum(value, 0.0) - jnp.log1p(jnp.exp(-jnp.abs(value)))
    return tile[0:1, 0:1]


def attend_body(
    index, logits, own, other, p0, p1, p2, p3, frequency, out_own, out_other, w, qs, ks, vs, gs
):
    y, core = index[1], index[3]
    for k, piece in enumerate((p0, p1, p2, p3)):
        at = (y ^ k) * 32
        for z in range(8):
            place = pl.ds(pl.multiple_of(z * 128 + at, 32), 32)
            w[place, :] = piece[z * 32 : z * 32 + 32, :]
    inside = lax.broadcasted_iota(jnp.int32, (128, DK), 0).astype(f32) * frequency[...]
    cos_in, sin_in = jnp.cos(inside), jnp.sin(inside)
    block = lax.broadcasted_iota(jnp.int32, (8, DK), 0)
    base = (block % 4) * 256 + jnp.where(block < 4, core, 1 - core) * 128
    start = base.astype(f32) * frequency[...]
    cos_at, sin_at = jnp.cos(start), jnp.sin(start)
    sign = jnp.where(lax.broadcasted_iota(jnp.int32, (128, DK), 1) < DK // 2, -1.0, 1.0)
    cos_turn, sin_turn = cos_in * sign, sin_in * sign

    def tables(r):
        c, s = cos_at[r : r + 1, :], sin_at[r : r + 1, :]
        return c * cos_in - s * sin_in, s * cos_turn + c * sin_turn

    step = 256
    for r in range(0, 1024, step):
        rows = own[r : r + step, :] if r < 512 else other[r - 512 : r - 512 + step, :]
        projected = dot(rows, w[...])
        pair = [tables(b) for b in range(r // 128, (r + step) // 128)]
        cos = jnp.concatenate([p[0] for p in pair], axis=0)
        sin = jnp.concatenate([p[1] for p in pair], axis=0)
        q = projected[:, :DK]
        k = projected[:, DK : 2 * DK]
        qs[r : r + step, :] = (q * cos + pltpu.roll(q, DK // 2, 1) * sin).astype(bf16)
        ks[r : r + step, :] = (
            (k * cos + pltpu.roll(k, DK // 2, 1) * sin) * DK ** (-0.5)
        ).astype(bf16)
        vs[r : r + step, :] = projected[:, 2 * DK : 2 * DK + DV].astype(bf16)
        gs[r : r + step, :] = projected[:, 2 * DK + DV :]
    forward = log_sigmoid_tile(logits[0])
    backward = log_sigmoid_tile(logits[1])
    lag = (
        lax.broadcasted_iota(jnp.int32, (128, 128), 0)
        - lax.broadcasted_iota(jnp.int32, (128, 128), 1)
    ).astype(f32)
    ahead, behind = lag * forward, lag * -backward
    side = ((2 * core - 1) * 128).astype(f32)
    for r in range(8):
        decays = []
        for c in range(8):
            gap = float((r % 4 - c % 4) * 256)
            if r < 4 <= c:
                gap = gap + side
            if c < 4 <= r:
                gap = gap - side
            decays.append(jnp.exp(jnp.minimum(ahead + gap * forward, behind - gap * backward)))
        rows = slice(r * 128, r * 128 + 128)
        scores = dot_nt(qs[rows, :], ks[...])
        weighted = (scores * jnp.concatenate(decays, axis=1)).astype(bf16)
        kept = head_norm(dot(weighted, vs[...]))
        gate = gs[rows, :]
        gated = (kept * (gate / (1.0 + jnp.exp(-gate)))).astype(bf16)
        if r < 4:
            out_own[rows, :] = gated
        else:
            out_other[r * 128 - 512 : r * 128 - 384, :] = gated


def output_body(index, mine, theirs, my_weights, their_weights, far, right, left, here, lines):
    for place, k in enumerate((2, 1, 3, 0)):
        block = index[0] ^ k
        rows = pl.ds(pl.multiple_of(block * 128, 128), 128)
        lines[place * 128 : place * 128 + 128, :DV] = mine[rows, :]
        lines[place * 128 : place * 128 + 128, DV:] = theirs[rows, :]
    for d in range(0, 1024, 256):
        columns = slice(d, d + 256)
        total = dot_nt(lines[:, :DV], my_weights[columns, :]) + dot_nt(
            lines[:, DV:], their_weights[columns, :]
        )
        for place, out in enumerate((far, right, left, here)):
            out[:, columns] = total[place * 128 : place * 128 + 128, :].astype(bf16)


def feed_block(main, before, after, taps):
    line = lax.broadcasted_iota(jnp.int32, (128, 1), 0)
    prev = jnp.where(line == 0, before, pltpu.roll(main, 1, 0))
    nxt = jnp.where(line == 127, after, pltpu.roll(main, 127, 0))
    kernel = [
        jnp.concatenate([taps[t : t + 1, :], taps[t + 3 : t + 4, :]], axis=1) for t in range(3)
    ]
    bias = jnp.concatenate([taps[6:7, :], taps[7:8, :]], axis=1)
    conv = kernel[0] * prev + kernel[1] * main + kernel[2] * nxt + bias
    value = conv[:, :PAD]
    bent = value * (0.5 + 0.5 * jnp.tanh(0.7978845608028654 * (value + 0.044715 * value**3)))
    return (bent * conv[:, PAD:]).astype(bf16)


def feed_body(
    index,
    got_far,
    got_next,
    got_prev,
    own,
    edges,
    mine,
    theirs,
    my_taps,
    their_taps,
    far,
    right,
    left,
    here,
    lines,
    outer,
    hidden,
):
    core = index[3]
    blocks = [index[0] ^ k for k in (2, 1, 3, 0)]
    for place, piece in enumerate((got_far, got_next, got_prev, own)):
        lines[place * 128 : place * 128 + 128, :] = piece[...]
    lines[512:520, :] = edges[...]
    lines[520:528, :] = jnp.zeros((8, 1024), bf16)
    outer[...] = jnp.zeros(outer.shape, f32)
    for part, (weights, taps) in enumerate(((mine, my_taps), (theirs, their_taps))):
        main = dot(lines[...], weights[:, : 2 * PAD])
        for place, block in enumerate(blocks):
            outer[pl.ds(8 + block, 1), :] = main[512 + 2 * place : 513 + 2 * place, :]
            outer[pl.ds(1 + block, 1), :] = main[513 + 2 * place : 514 + 2 * place, :]
        for place, block in enumerate(blocks):
            inner = slice(place * 128, place * 128 + 128)
            before = outer[pl.ds(block + core, 1), :]
            after = outer[pl.ds(8 + block + core, 1), :]
            hidden[inner, part * PAD : part * PAD + PAD] = feed_block(
                main[inner, :], before, after, taps
            )
    for d in range(0, 1024, 256):
        columns = slice(d, d + 256)
        total = dot_nt(hidden[:, :PAD], mine[columns, 2 * PAD :]) + dot_nt(
            hidden[:, PAD:], theirs[columns, 2 * PAD :]
        )
        for place, out in enumerate((far, right, left, here)):
            out[:, columns] = total[place * 128 : place * 128 + 128, :].astype(bf16)


def head_norm(values):
    centred = values - jnp.mean(values, axis=-1, keepdims=True)
    return centred * lax.rsqrt(jnp.mean(centred * centred, axis=-1, keepdims=True) + epsilon)


def dot(a, b):
    return jnp.dot(a, b, preferred_element_type=f32)


def dot_nt(a, b):
    return lax.dot_general(a, b, (((1,), (1,)), ((), ())), preferred_element_type=f32)


def line_gather(piece):
    got = {0: piece}
    for k in PARTNERS:
        got[k] = lax.ppermute(piece, "y", line_pairs(k))
    return [got[k].reshape(256, piece.shape[-1]) for k in range(4)]


def in_line_order(pieces, place):
    columns = pieces[0].shape[1]
    ordered = call(line_order_body, shape((8, 4, 32, columns)), place, *pieces, smem=1)
    return ordered.reshape(1024, columns)


def sent(blocks):
    return [lax.ppermute(block, "x", line_pairs(k)) for k, block in zip(PARTNERS, blocks)]


def rope_frequency():
    half = DK // 2
    frequency = 1.0 / rope_base ** (np.arange(half, dtype=np.float32) / half)
    return jnp.asarray(np.tile(frequency.astype(np.float32), 2)[None])


def layer(
    tokens,
    mixer_in_gain,
    query_weight,
    key_weight,
    value_weight,
    gate_weight,
    decay_logits,
    mixer_output,
    mixer_out_gain,
    channel_in_gain,
    gelu_weight,
    linear_weight,
    gelu_kernel,
    linear_kernel,
    gelu_bias,
    linear_bias,
    down_weight,
    channel_out_gain,
):
    place = jnp.stack([lax.axis_index(a).astype(jnp.int32) for a in ("x", "y", "z", "c")])
    place, query_weight = lax.optimization_barrier((place, query_weight))
    token_rows = tokens[0]
    own, model = token_rows.shape
    chips = lax.axis_size("x")
    half = chips * own
    width = gelu_weight.shape[1]

    def row(vector):
        return vector.reshape(1, -1)

    parts = (
        query_weight,
        key_weight,
        value_weight,
        gate_weight,
        mixer_output.T,
        gelu_weight,
        linear_weight,
        down_weight.T,
    )
    packed = call(
        functools.partial(pack_body, width),
        shape((32, FIRST + SECOND + THIRD)),
        *parts,
        hbm=8,
        scratch=[pltpu.VMEM(part.shape, bf16) for part in parts]
        + [pltpu.SemaphoreType.DMA((8,))],
    )
    got = {0: packed}
    for k in Z_ISSUE:
        got[k] = lax.ppermute(packed, RING, ring_pairs(k))
    spread = call(
        first_norm_body, shape((chips, own, model)), token_rows, row(mixer_in_gain), limit=60
    )
    normed_own = exchanged(spread).reshape(half, model)
    normed_other = swap(normed_own)
    first_z, second_z, third_z = call(
        ring_order_body,
        [shape((8, 32, columns)) for columns in (FIRST, SECOND, THIRD)],
        place,
        *[got[k] for k in Z_SHIFTS],
        smem=1,
    )
    first_pieces = line_gather(first_z)
    second_pieces = line_gather(second_z)
    third_pieces = line_gather(third_z)
    taps = call(
        functools.partial(taps_body, width),
        shape((8, PAD), f32),
        gelu_kernel,
        linear_kernel,
        gelu_bias,
        linear_bias,
    )
    taps_other = swap(taps)
    gated_own, gated_other = call(
        attend_body,
        [shape((half, DV)), shape((half, DV))],
        place,
        decay_logits[:, 0],
        normed_own,
        normed_other,
        *first_pieces,
        rope_frequency(),
        flops=1 << 32,
        smem=2,
        limit=10,
        scratch=[
            pltpu.VMEM((model, FIRST), bf16),
            pltpu.VMEM((2 * half, DK), bf16),
            pltpu.VMEM((2 * half, DK), bf16),
            pltpu.VMEM((2 * half, DV), bf16),
            pltpu.VMEM((2 * half, DV), f32),
        ],
    )
    gated_partner = swap(gated_other)
    out_own = in_line_order(second_pieces, place)
    far, right, left, here = call(
        output_body,
        [shape((own, model))] * 4,
        place,
        gated_own,
        gated_partner,
        out_own,
        swap(out_own),
        flops=1 << 30,
        smem=1,
        scratch=[pltpu.VMEM((half, 2 * DV), bf16)],
    )
    after_mix, channel_in = call(
        middle_body,
        [shape((own, model)), shape((own, model))],
        *sent((far, right, left)),
        here,
        token_rows,
        row(mixer_out_gain),
        row(channel_in_gain),
    )
    third_own = in_line_order(third_pieces, place)
    third_other = swap(third_own)
    blocks = (*sent([channel_in] * 3), channel_in)
    edges = call(edges_body, shape((8, model)), *blocks)
    far, right, left, here = call(
        feed_body,
        [shape((own, model))] * 4,
        place,
        *blocks,
        swap(edges),
        third_own,
        third_other,
        taps,
        taps_other,
        flops=1 << 32,
        smem=1,
        limit=18,
        scratch=[
            pltpu.VMEM((half + 16, model), bf16),
            pltpu.VMEM((16, 2 * PAD), f32),
            pltpu.VMEM((half, 2 * PAD), bf16),
        ],
    )
    result = call(
        final_body,
        shape((own, model)),
        *sent((far, right, left)),
        here,
        after_mix,
        row(channel_out_gain),
    )
    return result[None]


def solution(mesh):
    fs = mesh.shape["fs"]
    tp = mesh.shape["tp"]
    split = Mesh(
        mesh.devices.reshape(mesh.shape["rep"], fs // 4, 4, tp // 2, 2),
        ("rep", "z", "y", "x", "c"),
    )
    in_specs = (
        P(("rep", "z", "y"), TP, None),
        P(),
        P(FS, TP),
        P(FS, TP),
        P(FS, TP),
        P(FS, TP),
        P(None, TP),
        P(TP, FS),
        P(),
        P(),
        P(FS, TP),
        P(FS, TP),
        P(None, TP),
        P(None, TP),
        P(TP),
        P(TP),
        P(TP, FS),
        P(),
    )
    out_specs = P(("rep", "z", "y"), TP, None)
    return jax.shard_map(layer, mesh=split, in_specs=in_specs, out_specs=out_specs, check_vma=False)
```

```python
import functools

import jax
import jax.numpy as jnp
import numpy as np
from jax import lax
from jax.experimental import pallas as pl
from jax.experimental.pallas import tpu as pltpu
from jax.sharding import Mesh
from jax.sharding import PartitionSpec as P


DK = 128
DV = 256
TP = ("x", "c")
FS = ("zh", "zl", "y")
RING = ("rep", "zh", "zl")
SWAP = ((0, 1), (1, 0))
PAD = 384
FIRST, SECOND, THIRD = 2 * DK + 2 * DV, DV, 3 * PAD
Z_PAIRS = (5, 7, 6)
PARTNERS = (2, 1, 3)
epsilon = 1e-06
rope_base = 10000.0
bf16 = jnp.bfloat16
f32 = jnp.float32

VMEM = pl.BlockSpec(memory_space=pltpu.VMEM)
SMEM = pl.BlockSpec(memory_space=pltpu.SMEM)
HBM = pl.BlockSpec(memory_space=pltpu.HBM)


def call(body, out_shapes, *args, flops=0, smem=0, hbm=0, scratch=(), limit=6):
    specs = [SMEM] * smem + [HBM] * hbm + [VMEM] * (len(args) - smem - hbm)
    single = not isinstance(out_shapes, (list, tuple))
    args = [
        pltpu.with_memory_space_constraint(a, pltpu.HBM) if smem <= k < smem + hbm else a
        for k, a in enumerate(args)
    ]
    return pl.pallas_call(
        body,
        out_shape=out_shapes,
        in_specs=specs,
        out_specs=VMEM if single else [VMEM] * len(out_shapes),
        scratch_shapes=list(scratch),
        compiler_params=pltpu.CompilerParams(vmem_limit_bytes=limit << 20),
        cost_estimate=pl.CostEstimate(
            flops=max(flops, 1 << 24), bytes_accessed=1 << 21, transcendentals=0
        ),
    )(*args)


def shape(dims, kind=bf16):
    return jax.ShapeDtypeStruct(dims, kind)


def line_pairs(k):
    return [(i, i ^ k) for i in range(4)]


def ring_shift(shift):
    return [(i, (i + shift) % 16) for i in range(16)]


def ring_pairs(k):
    pairs = []
    for i in range(16):
        here = i // 8 * 8 + (i % 8 ^ k)
        gap = min((here - i) % 16, (i - here) % 16)
        pairs.append((i, here if gap <= 4 else (here + 8) % 16))
    return pairs


def swap(value):
    return lax.ppermute(value, "c", SWAP)


def exchanged(value):
    return lax.all_to_all(value, "x", 0, 0, tiled=True)


def rms_rows(values, gain):
    return values * lax.rsqrt(jnp.mean(values * values, axis=-1, keepdims=True) + epsilon) * gain


def pack_body(width, *refs):
    sources, (out, spread, front, back) = refs[:8], refs[8:12]
    places, arrived = refs[12:20], refs[20]
    copies = [
        pltpu.make_async_copy(source, place, arrived.at[k])
        for k, (source, place) in enumerate(zip(sources, places))
    ]
    for copy in copies:
        copy.start()
    for copy in copies:
        copy.wait()
    at = 0
    for place in places[:5]:
        out[:, at : at + place.shape[1]] = place[...]
        at += place.shape[1]
    gap = jnp.zeros((out.shape[0], PAD - width), bf16)
    for place in places[5:]:
        out[:, at : at + PAD] = jnp.concatenate([place[...], gap], axis=1)
        at += PAD
    front[...] = out[:, : FIRST + SECOND]
    back[...] = out[:, FIRST + SECOND :]
    for k in range(spread.shape[0]):
        spread[k] = out[...]


def taps_body(width, ge_kernel, li_kernel, ge_bias, li_bias, out):
    out[...] = jnp.zeros(out.shape, f32)
    out[0:3, :width] = ge_kernel[...]
    out[3:6, :width] = li_kernel[...]
    out[6:7, :width] = ge_bias[...].reshape(1, width)
    out[7:8, :width] = li_bias[...].reshape(1, width)


def first_norm_body(tokens, gain, out):
    rows = rms_rows(tokens[...].astype(f32), gain[...]).astype(bf16)
    for k in range(out.shape[0]):
        out[k] = rows


def ring_order_body(index, quad, front, back, p5, p7, p6, one, two, three):
    z = index[2]
    pieces = [(quad.at[k], (z & 4) + k) for k in range(4)]
    pieces += [(piece, z ^ k) for k, piece in zip(Z_PAIRS, (p5, p7, p6))]
    for piece, at in pieces:
        one[at] = piece[:, :FIRST]
        two[at] = piece[:, FIRST : FIRST + SECOND]
        three[at] = piece[:, FIRST + SECOND :]
    at = z ^ 4
    one[at] = front[:, :FIRST]
    two[at] = front[:, FIRST:]
    three[at] = back[...]


def line_order_body(index, *refs):
    pieces, out = refs[:4], refs[4]
    for k, piece in enumerate(pieces):
        at = index[1] ^ k
        for z in range(8):
            out[z, at] = piece[z * 32 : z * 32 + 32, :]


def edges_body(far, after, before, own, out):
    rows = [p[k : k + 1, :].astype(f32) for p in (far, after, before, own) for k in (0, 127)]
    out[...] = jnp.concatenate(rows, axis=0).astype(bf16)


def summed(pieces):
    total = pieces[0][...].astype(f32)
    for piece in pieces[1:]:
        total = total + piece[...].astype(f32)
    return total * lax.rsqrt(jnp.mean(total * total, axis=-1, keepdims=True) + epsilon)


def middle_body(far, right, left, here, tokens, out_gain, in_gain, after_mix, channel_in):
    total = summed((here, right, left, far))
    mix = (tokens[...].astype(f32) + total * out_gain[...]).astype(bf16)
    after_mix[...] = mix
    channel_in[...] = rms_rows(mix.astype(f32), in_gain[...]).astype(bf16)


def final_body(far, right, left, here, after_mix, gain, out):
    total = summed((here, right, left, far))
    out[...] = (after_mix[...].astype(f32) + total * gain[...]).astype(bf16)


def log_sigmoid_tile(logit):
    value = jnp.full((8, 128), logit, f32)
    tile = jnp.minimum(value, 0.0) - jnp.log1p(jnp.exp(-jnp.abs(value)))
    return tile[0:1, 0:1]


def attend_body(
    index, logits, own, other, p0, p1, p2, p3, frequency, out_own, out_other, w, qs, ks, vs, gs
):
    y, core = index[1], index[3]
    for k, piece in enumerate((p0, p1, p2, p3)):
        at = (y ^ k) * 32
        for z in range(8):
            place = pl.ds(pl.multiple_of(z * 128 + at, 32), 32)
            w[place, :] = piece[z * 32 : z * 32 + 32, :]
    inside = lax.broadcasted_iota(jnp.int32, (128, DK), 0).astype(f32) * frequency[...]
    cos_in, sin_in = jnp.cos(inside), jnp.sin(inside)
    block = lax.broadcasted_iota(jnp.int32, (8, DK), 0)
    base = (block % 4) * 256 + jnp.where(block < 4, core, 1 - core) * 128
    start = base.astype(f32) * frequency[...]
    cos_at, sin_at = jnp.cos(start), jnp.sin(start)
    sign = jnp.where(lax.broadcasted_iota(jnp.int32, (128, DK), 1) < DK // 2, -1.0, 1.0)
    cos_turn, sin_turn = cos_in * sign, sin_in * sign

    def tables(r):
        c, s = cos_at[r : r + 1, :], sin_at[r : r + 1, :]
        return c * cos_in - s * sin_in, s * cos_turn + c * sin_turn

    step = 256
    for r in range(0, 1024, step):
        rows = own[r : r + step, :] if r < 512 else other[r - 512 : r - 512 + step, :]
        projected = dot(rows, w[...])
        pair = [tables(b) for b in range(r // 128, (r + step) // 128)]
        cos = jnp.concatenate([p[0] for p in pair], axis=0)
        sin = jnp.concatenate([p[1] for p in pair], axis=0)
        q = projected[:, :DK]
        k = projected[:, DK : 2 * DK]
        qs[r : r + step, :] = (q * cos + pltpu.roll(q, DK // 2, 1) * sin).astype(bf16)
        ks[r : r + step, :] = (
            (k * cos + pltpu.roll(k, DK // 2, 1) * sin) * DK ** (-0.5)
        ).astype(bf16)
        vs[r : r + step, :] = projected[:, 2 * DK : 2 * DK + DV].astype(bf16)
        gs[r : r + step, :] = projected[:, 2 * DK + DV :]
    forward = log_sigmoid_tile(logits[0])
    backward = log_sigmoid_tile(logits[1])
    lag = (
        lax.broadcasted_iota(jnp.int32, (128, 128), 0)
        - lax.broadcasted_iota(jnp.int32, (128, 128), 1)
    ).astype(f32)
    ahead, behind = lag * forward, lag * -backward
    side = ((2 * core - 1) * 128).astype(f32)
    for r in range(8):
        decays = []
        for c in range(8):
            gap = float((r % 4 - c % 4) * 256)
            if r < 4 <= c:
                gap = gap + side
            if c < 4 <= r:
                gap = gap - side
            decays.append(jnp.exp(jnp.minimum(ahead + gap * forward, behind - gap * backward)))
        rows = slice(r * 128, r * 128 + 128)
        scores = dot_nt(qs[rows, :], ks[...])
        weighted = (scores * jnp.concatenate(decays, axis=1)).astype(bf16)
        kept = head_norm(dot(weighted, vs[...]))
        gate = gs[rows, :]
        gated = (kept * (gate / (1.0 + jnp.exp(-gate)))).astype(bf16)
        if r < 4:
            out_own[rows, :] = gated
        else:
            out_other[r * 128 - 512 : r * 128 - 384, :] = gated


def output_body(index, mine, theirs, my_weights, their_weights, far, right, left, here, lines):
    for place, k in enumerate((2, 1, 3, 0)):
        block = index[0] ^ k
        rows = pl.ds(pl.multiple_of(block * 128, 128), 128)
        lines[place * 128 : place * 128 + 128, :DV] = mine[rows, :]
        lines[place * 128 : place * 128 + 128, DV:] = theirs[rows, :]
    for d in range(0, 1024, 256):
        columns = slice(d, d + 256)
        total = dot_nt(lines[:, :DV], my_weights[columns, :]) + dot_nt(
            lines[:, DV:], their_weights[columns, :]
        )
        for place, out in enumerate((far, right, left, here)):
            out[:, columns] = total[place * 128 : place * 128 + 128, :].astype(bf16)


def feed_block(main, before, after, taps):
    line = lax.broadcasted_iota(jnp.int32, (128, 1), 0)
    prev = jnp.where(line == 0, before, pltpu.roll(main, 1, 0))
    nxt = jnp.where(line == 127, after, pltpu.roll(main, 127, 0))
    kernel = [
        jnp.concatenate([taps[t : t + 1, :], taps[t + 3 : t + 4, :]], axis=1) for t in range(3)
    ]
    bias = jnp.concatenate([taps[6:7, :], taps[7:8, :]], axis=1)
    conv = kernel[0] * prev + kernel[1] * main + kernel[2] * nxt + bias
    value = conv[:, :PAD]
    bent = value * (0.5 + 0.5 * jnp.tanh(0.7978845608028654 * (value + 0.044715 * value**3)))
    return (bent * conv[:, PAD:]).astype(bf16)


def feed_body(
    index,
    got_far,
    got_next,
    got_prev,
    own,
    edges,
    mine,
    theirs,
    my_taps,
    their_taps,
    far,
    right,
    left,
    here,
    lines,
    outer,
    hidden,
):
    core = index[3]
    blocks = [index[0] ^ k for k in (2, 1, 3, 0)]
    for place, piece in enumerate((got_far, got_next, got_prev, own)):
        lines[place * 128 : place * 128 + 128, :] = piece[...]
    lines[512:520, :] = edges[...]
    lines[520:528, :] = jnp.zeros((8, 1024), bf16)
    outer[...] = jnp.zeros(outer.shape, f32)
    for part, (weights, taps) in enumerate(((mine, my_taps), (theirs, their_taps))):
        main = dot(lines[...], weights[:, : 2 * PAD])
        for place, block in enumerate(blocks):
            outer[pl.ds(8 + block, 1), :] = main[512 + 2 * place : 513 + 2 * place, :]
            outer[pl.ds(1 + block, 1), :] = main[513 + 2 * place : 514 + 2 * place, :]
        for place, block in enumerate(blocks):
            inner = slice(place * 128, place * 128 + 128)
            before = outer[pl.ds(block + core, 1), :]
            after = outer[pl.ds(8 + block + core, 1), :]
            hidden[inner, part * PAD : part * PAD + PAD] = feed_block(
                main[inner, :], before, after, taps
            )
    for d in range(0, 1024, 256):
        columns = slice(d, d + 256)
        total = dot_nt(hidden[:, :PAD], mine[columns, 2 * PAD :]) + dot_nt(
            hidden[:, PAD:], theirs[columns, 2 * PAD :]
        )
        for place, out in enumerate((far, right, left, here)):
            out[:, columns] = total[place * 128 : place * 128 + 128, :].astype(bf16)


def head_norm(values):
    centred = values - jnp.mean(values, axis=-1, keepdims=True)
    return centred * lax.rsqrt(jnp.mean(centred * centred, axis=-1, keepdims=True) + epsilon)


def dot(a, b):
    return jnp.dot(a, b, preferred_element_type=f32)


def dot_nt(a, b):
    return lax.dot_general(a, b, (((1,), (1,)), ((), ())), preferred_element_type=f32)


def line_gather(piece):
    got = {0: piece}
    for k in PARTNERS:
        got[k] = lax.ppermute(piece, "y", line_pairs(k))
    return [got[k].reshape(256, piece.shape[-1]) for k in range(4)]


def in_line_order(pieces, place):
    columns = pieces[0].shape[1]
    ordered = call(line_order_body, shape((8, 4, 32, columns)), place, *pieces, smem=1)
    return ordered.reshape(1024, columns)


def sent(blocks):
    return [lax.ppermute(block, "x", line_pairs(k)) for k, block in zip(PARTNERS, blocks)]


def rope_frequency():
    half = DK // 2
    frequency = 1.0 / rope_base ** (np.arange(half, dtype=np.float32) / half)
    return jnp.asarray(np.tile(frequency.astype(np.float32), 2)[None])


def layer(
    tokens,
    mixer_in_gain,
    query_weight,
    key_weight,
    value_weight,
    gate_weight,
    decay_logits,
    mixer_output,
    mixer_out_gain,
    channel_in_gain,
    gelu_weight,
    linear_weight,
    gelu_kernel,
    linear_kernel,
    gelu_bias,
    linear_bias,
    down_weight,
    channel_out_gain,
):
    place = jnp.stack([lax.axis_index(a).astype(jnp.int32) for a in ("x", "y", ("zh", "zl"), "c")])
    place, query_weight = lax.optimization_barrier((place, query_weight))
    token_rows = tokens[0]
    own, model = token_rows.shape
    chips = lax.axis_size("x")
    half = chips * own
    width = gelu_weight.shape[1]

    def row(vector):
        return vector.reshape(1, -1)

    parts = (
        query_weight,
        key_weight,
        value_weight,
        gate_weight,
        mixer_output.T,
        gelu_weight,
        linear_weight,
        down_weight.T,
    )
    total = FIRST + SECOND + THIRD
    packed, quad_spread, front, back = call(
        functools.partial(pack_body, width),
        [shape((32, total)), shape((4, 32, total)), shape((32, total - THIRD)), shape((32, THIRD))],
        *parts,
        hbm=8,
        scratch=[pltpu.VMEM(part.shape, bf16) for part in parts]
        + [pltpu.SemaphoreType.DMA((8,))],
    )
    quad = lax.all_to_all(quad_spread, "zl", 0, 0, tiled=True)
    front = lax.ppermute(front, RING, ring_shift(4))
    back = lax.ppermute(back, RING, ring_shift(-4))
    ring_pieces = [lax.ppermute(packed, RING, ring_pairs(k)) for k in Z_PAIRS]
    spread = call(
        first_norm_body, shape((chips, own, model)), token_rows, row(mixer_in_gain), limit=60
    )
    normed_own = exchanged(spread).reshape(half, model)
    normed_other = swap(normed_own)
    first_z, second_z, third_z = call(
        ring_order_body,
        [shape((8, 32, columns)) for columns in (FIRST, SECOND, THIRD)],
        place,
        quad,
        front,
        back,
        *ring_pieces,
        smem=1,
    )
    first_pieces = line_gather(first_z)
    second_pieces = line_gather(second_z)
    third_pieces = line_gather(third_z)
    taps = call(
        functools.partial(taps_body, width),
        shape((8, PAD), f32),
        gelu_kernel,
        linear_kernel,
        gelu_bias,
        linear_bias,
    )
    taps_other = swap(taps)
    gated_own, gated_other = call(
        attend_body,
        [shape((half, DV)), shape((half, DV))],
        place,
        decay_logits[:, 0],
        normed_own,
        normed_other,
        *first_pieces,
        rope_frequency(),
        flops=1 << 32,
        smem=2,
        limit=10,
        scratch=[
            pltpu.VMEM((model, FIRST), bf16),
            pltpu.VMEM((2 * half, DK), bf16),
            pltpu.VMEM((2 * half, DK), bf16),
            pltpu.VMEM((2 * half, DV), bf16),
            pltpu.VMEM((2 * half, DV), f32),
        ],
    )
    gated_partner = swap(gated_other)
    out_own = in_line_order(second_pieces, place)
    far, right, left, here = call(
        output_body,
        [shape((own, model))] * 4,
        place,
        gated_own,
        gated_partner,
        out_own,
        swap(out_own),
        flops=1 << 30,
        smem=1,
        scratch=[pltpu.VMEM((half, 2 * DV), bf16)],
    )
    after_mix, channel_in = call(
        middle_body,
        [shape((own, model)), shape((own, model))],
        *sent((far, right, left)),
        here,
        token_rows,
        row(mixer_out_gain),
        row(channel_in_gain),
    )
    third_own = in_line_order(third_pieces, place)
    third_other = swap(third_own)
    blocks = (*sent([channel_in] * 3), channel_in)
    edges = call(edges_body, shape((8, model)), *blocks)
    far, right, left, here = call(
        feed_body,
        [shape((own, model))] * 4,
        place,
        *blocks,
        swap(edges),
        third_own,
        third_other,
        taps,
        taps_other,
        flops=1 << 32,
        smem=1,
        limit=18,
        scratch=[
            pltpu.VMEM((half + 16, model), bf16),
            pltpu.VMEM((16, 2 * PAD), f32),
            pltpu.VMEM((half, 2 * PAD), bf16),
        ],
    )
    result = call(
        final_body,
        shape((own, model)),
        *sent((far, right, left)),
        here,
        after_mix,
        row(channel_out_gain),
    )
    return result[None]


def solution(mesh):
    fs = mesh.shape["fs"]
    tp = mesh.shape["tp"]
    split = Mesh(
        mesh.devices.reshape(mesh.shape["rep"], fs // 16, 4, 4, tp // 2, 2),
        ("rep", "zh", "zl", "y", "x", "c"),
    )
    in_specs = (
        P(("rep", *FS), TP, None),
        P(),
        P(FS, TP),
        P(FS, TP),
        P(FS, TP),
        P(FS, TP),
        P(None, TP),
        P(TP, FS),
        P(),
        P(),
        P(FS, TP),
        P(FS, TP),
        P(None, TP),
        P(None, TP),
        P(TP),
        P(TP),
        P(TP, FS),
        P(),
    )
    out_specs = P(("rep", *FS), TP, None)
    return jax.shard_map(layer, mesh=split, in_specs=in_specs, out_specs=out_specs, check_vma=False)
```

```python
import functools

import jax
import jax.numpy as jnp
import numpy as np
from jax import lax
from jax.experimental import pallas as pl
from jax.experimental.pallas import tpu as pltpu
from jax.sharding import Mesh
from jax.sharding import PartitionSpec as P


DK = 128
DV = 256
TP = ("x", "c")
FS = ("z", "y")
RING = ("rep", "z")
SWAP = ((0, 1), (1, 0))
PAD = 384
FIRST, SECOND, THIRD = 2 * DK + 2 * DV, DV, 3 * PAD
Z_SHIFTS = (4, 3, 2, 1, 0, -1, -2, -3)
Z_ISSUE = (4, -3, 3, -2, 2, -1, 1)
PARTNERS = (2, 1, 3)
epsilon = 1e-06
rope_base = 10000.0
bf16 = jnp.bfloat16
f32 = jnp.float32

VMEM = pl.BlockSpec(memory_space=pltpu.VMEM)
SMEM = pl.BlockSpec(memory_space=pltpu.SMEM)
HBM = pl.BlockSpec(memory_space=pltpu.HBM)


def call(body, out_shapes, *args, flops=0, smem=0, hbm=0, scratch=(), limit=6):
    specs = [SMEM] * smem + [HBM] * hbm + [VMEM] * (len(args) - smem - hbm)
    single = not isinstance(out_shapes, (list, tuple))
    args = [
        pltpu.with_memory_space_constraint(a, pltpu.HBM) if smem <= k < smem + hbm else a
        for k, a in enumerate(args)
    ]
    return pl.pallas_call(
        body,
        out_shape=out_shapes,
        in_specs=specs,
        out_specs=VMEM if single else [VMEM] * len(out_shapes),
        scratch_shapes=list(scratch),
        compiler_params=pltpu.CompilerParams(vmem_limit_bytes=limit << 20),
        cost_estimate=pl.CostEstimate(
            flops=max(flops, 1 << 24), bytes_accessed=1 << 21, transcendentals=0
        ),
    )(*args)


def shape(dims, kind=bf16):
    return jax.ShapeDtypeStruct(dims, kind)


def line_pairs(k):
    return [(i, i ^ k) for i in range(4)]


def ring_pairs(shift):
    return [(i, (i + shift) % 16) for i in range(16)]


def swap(value):
    return lax.ppermute(value, "c", SWAP)


def exchanged(value):
    return lax.all_to_all(value, "x", 0, 0, tiled=True)


def rms_rows(values, gain):
    return values * lax.rsqrt(jnp.mean(values * values, axis=-1, keepdims=True) + epsilon) * gain


def pack_body(width, *refs):
    sources, out, places, arrived = refs[:8], refs[8], refs[9:17], refs[17]
    copies = [
        pltpu.make_async_copy(source, place, arrived.at[k])
        for k, (source, place) in enumerate(zip(sources, places))
    ]
    for copy in copies:
        copy.start()
    for copy in copies:
        copy.wait()
    at = 0
    for place in places[:5]:
        out[:, at : at + place.shape[1]] = place[...]
        at += place.shape[1]
    gap = jnp.zeros((out.shape[0], PAD - width), bf16)
    for place in places[5:]:
        out[:, at : at + PAD] = jnp.concatenate([place[...], gap], axis=1)
        at += PAD


def taps_body(width, ge_kernel, li_kernel, ge_bias, li_bias, out):
    out[...] = jnp.zeros(out.shape, f32)
    out[0:3, :width] = ge_kernel[...]
    out[3:6, :width] = li_kernel[...]
    out[6:7, :width] = ge_bias[...].reshape(1, width)
    out[7:8, :width] = li_bias[...].reshape(1, width)


def first_norm_body(tokens, gain, out):
    rows = rms_rows(tokens[...].astype(f32), gain[...]).astype(bf16)
    for k in range(out.shape[0]):
        out[k] = rows


def ring_order_body(index, *refs):
    pieces, (one, two, three) = refs[:8], refs[8:]
    for shift, piece in zip(Z_SHIFTS, pieces):
        at = lax.rem(index[2] - shift + 8, 8)
        one[at] = piece[:, :FIRST]
        two[at] = piece[:, FIRST : FIRST + SECOND]
        three[at] = piece[:, FIRST + SECOND :]


def line_order_body(index, *refs):
    pieces, out = refs[:4], refs[4]
    for k, piece in enumerate(pieces):
        at = index[1] ^ k
        for z in range(8):
            out[z, at] = piece[z * 32 : z * 32 + 32, :]


def edges_body(far, after, before, own, out):
    rows = [p[k : k + 1, :].astype(f32) for p in (far, after, before, own) for k in (0, 127)]
    out[...] = jnp.concatenate(rows, axis=0).astype(bf16)


def summed(pieces):
    total = pieces[0][...].astype(f32)
    for piece in pieces[1:]:
        total = total + piece[...].astype(f32)
    return total * lax.rsqrt(jnp.mean(total * total, axis=-1, keepdims=True) + epsilon)


def middle_body(far, right, left, here, tokens, out_gain, in_gain, after_mix, channel_in):
    total = summed((here, right, left, far))
    mix = (tokens[...].astype(f32) + total * out_gain[...]).astype(bf16)
    after_mix[...] = mix
    channel_in[...] = rms_rows(mix.astype(f32), in_gain[...]).astype(bf16)


def final_body(far, right, left, here, after_mix, gain, out):
    total = summed((here, right, left, far))
    out[...] = (after_mix[...].astype(f32) + total * gain[...]).astype(bf16)


def log_sigmoid_tile(logit):
    value = jnp.full((8, 128), logit, f32)
    tile = jnp.minimum(value, 0.0) - jnp.log1p(jnp.exp(-jnp.abs(value)))
    return tile[0:1, 0:1]


def attend_body(
    index, logits, own, other, p0, p1, p2, p3, frequency, out_own, out_other, w, qs, ks, vs, gs
):
    y, core = index[1], index[3]
    for k, piece in enumerate((p0, p1, p2, p3)):
        at = (y ^ k) * 32
        for z in range(8):
            place = pl.ds(pl.multiple_of(z * 128 + at, 32), 32)
            w[place, :] = piece[z * 32 : z * 32 + 32, :]
    inside = lax.broadcasted_iota(jnp.int32, (128, DK), 0).astype(f32) * frequency[...]
    cos_in, sin_in = jnp.cos(inside), jnp.sin(inside)
    block = lax.broadcasted_iota(jnp.int32, (8, DK), 0)
    base = (block % 4) * 256 + jnp.where(block < 4, core, 1 - core) * 128
    start = base.astype(f32) * frequency[...]
    cos_at, sin_at = jnp.cos(start), jnp.sin(start)
    sign = jnp.where(lax.broadcasted_iota(jnp.int32, (128, DK), 1) < DK // 2, -1.0, 1.0)
    cos_turn, sin_turn = cos_in * sign, sin_in * sign

    def tables(r):
        c, s = cos_at[r : r + 1, :], sin_at[r : r + 1, :]
        return c * cos_in - s * sin_in, s * cos_turn + c * sin_turn

    step = 256
    for r in range(0, 1024, step):
        rows = own[r : r + step, :] if r < 512 else other[r - 512 : r - 512 + step, :]
        projected = dot(rows, w[...])
        pair = [tables(b) for b in range(r // 128, (r + step) // 128)]
        cos = jnp.concatenate([p[0] for p in pair], axis=0)
        sin = jnp.concatenate([p[1] for p in pair], axis=0)
        q = projected[:, :DK]
        k = projected[:, DK : 2 * DK]
        qs[r : r + step, :] = (q * cos + pltpu.roll(q, DK // 2, 1) * sin).astype(bf16)
        ks[r : r + step, :] = (
            (k * cos + pltpu.roll(k, DK // 2, 1) * sin) * DK ** (-0.5)
        ).astype(bf16)
        vs[r : r + step, :] = projected[:, 2 * DK : 2 * DK + DV].astype(bf16)
        gs[r : r + step, :] = projected[:, 2 * DK + DV :]
    forward = log_sigmoid_tile(logits[0])
    backward = log_sigmoid_tile(logits[1])
    lag = (
        lax.broadcasted_iota(jnp.int32, (128, 128), 0)
        - lax.broadcasted_iota(jnp.int32, (128, 128), 1)
    ).astype(f32)
    ahead, behind = lag * forward, lag * -backward
    side = ((2 * core - 1) * 128).astype(f32)
    for r in range(8):
        decays = []
        for c in range(8):
            gap = float((r % 4 - c % 4) * 256)
            if r < 4 <= c:
                gap = gap + side
            if c < 4 <= r:
                gap = gap - side
            decays.append(jnp.exp(jnp.minimum(ahead + gap * forward, behind - gap * backward)))
        rows = slice(r * 128, r * 128 + 128)
        scores = dot_nt(qs[rows, :], ks[...])
        weighted = (scores * jnp.concatenate(decays, axis=1)).astype(bf16)
        kept = head_norm(dot(weighted, vs[...]))
        gate = gs[rows, :]
        gated = (kept * (gate / (1.0 + jnp.exp(-gate)))).astype(bf16)
        spot = index[0] ^ (r % 4)
        spot = jnp.where(spot == 0, 3, jnp.where(spot == 2, 0, jnp.where(spot == 1, 1, 2)))
        spot = pl.ds(pl.multiple_of(spot * 128, 128), 128)
        if r < 4:
            out_own[spot, :] = gated
        else:
            out_other[spot, :] = gated


def other_body(gated, weights, out):
    for d in range(0, 1024, 256):
        columns = slice(d, d + 256)
        out[:, columns] = dot_nt(gated[...], weights[columns, :]).astype(bf16)


def output_body(index, mine, weights, theirs, far, right, left, here):
    for d in range(0, 1024, 256):
        columns = slice(d, d + 256)
        total = dot_nt(mine[...], weights[columns, :]) + theirs[:, columns].astype(f32)
        far[:, columns] = total[:128, :].astype(bf16)
        right[:, columns] = total[128:256, :].astype(bf16)
        left[:, columns] = total[256:384, :].astype(bf16)
        here[:, columns] = total[384:, :].astype(bf16)


def feed_block(main, before, after, taps):
    line = lax.broadcasted_iota(jnp.int32, (128, 1), 0)
    prev = jnp.where(line == 0, before, pltpu.roll(main, 1, 0))
    nxt = jnp.where(line == 127, after, pltpu.roll(main, 127, 0))
    kernel = [
        jnp.concatenate([taps[t : t + 1, :], taps[t + 3 : t + 4, :]], axis=1) for t in range(3)
    ]
    bias = jnp.concatenate([taps[6:7, :], taps[7:8, :]], axis=1)
    conv = kernel[0] * prev + kernel[1] * main + kernel[2] * nxt + bias
    value = conv[:, :PAD]
    bent = value * (0.5 + 0.5 * jnp.tanh(0.7978845608028654 * (value + 0.044715 * value**3)))
    return (bent * conv[:, PAD:]).astype(bf16)


def feed_body(
    index,
    got_far,
    got_next,
    got_prev,
    own,
    edges,
    mine,
    theirs,
    my_taps,
    their_taps,
    far,
    right,
    left,
    here,
    lines,
    outer,
    hidden,
):
    core = index[3]
    blocks = [index[0] ^ k for k in (2, 1, 3, 0)]
    for place, piece in enumerate((got_far, got_next, got_prev, own)):
        lines[place * 128 : place * 128 + 128, :] = piece[...]
    lines[512:520, :] = edges[...]
    lines[520:528, :] = jnp.zeros((8, 1024), bf16)
    outer[...] = jnp.zeros(outer.shape, f32)
    for part, (weights, taps) in enumerate(((mine, my_taps), (theirs, their_taps))):
        main = dot(lines[...], weights[:, : 2 * PAD])
        for place, block in enumerate(blocks):
            outer[pl.ds(8 + block, 1), :] = main[512 + 2 * place : 513 + 2 * place, :]
            outer[pl.ds(1 + block, 1), :] = main[513 + 2 * place : 514 + 2 * place, :]
        for place, block in enumerate(blocks):
            inner = slice(place * 128, place * 128 + 128)
            before = outer[pl.ds(block + core, 1), :]
            after = outer[pl.ds(8 + block + core, 1), :]
            hidden[inner, part * PAD : part * PAD + PAD] = feed_block(
                main[inner, :], before, after, taps
            )
    for d in range(0, 1024, 256):
        columns = slice(d, d + 256)
        total = dot_nt(hidden[:, :PAD], mine[columns, 2 * PAD :]) + dot_nt(
            hidden[:, PAD:], theirs[columns, 2 * PAD :]
        )
        for place, out in enumerate((far, right, left, here)):
            out[:, columns] = total[place * 128 : place * 128 + 128, :].astype(bf16)


def head_norm(values):
    centred = values - jnp.mean(values, axis=-1, keepdims=True)
    return centred * lax.rsqrt(jnp.mean(centred * centred, axis=-1, keepdims=True) + epsilon)


def dot(a, b):
    return jnp.dot(a, b, preferred_element_type=f32)


def dot_nt(a, b):
    return lax.dot_general(a, b, (((1,), (1,)), ((), ())), preferred_element_type=f32)


def line_gather(piece):
    got = {0: piece}
    for k in PARTNERS:
        got[k] = lax.ppermute(piece, "y", line_pairs(k))
    return [got[k].reshape(256, piece.shape[-1]) for k in range(4)]


def in_line_order(pieces, place):
    columns = pieces[0].shape[1]
    ordered = call(line_order_body, shape((8, 4, 32, columns)), place, *pieces, smem=1)
    return ordered.reshape(1024, columns)


def sent(blocks):
    return [lax.ppermute(block, "x", line_pairs(k)) for k, block in zip(PARTNERS, blocks)]


def rope_frequency():
    half = DK // 2
    frequency = 1.0 / rope_base ** (np.arange(half, dtype=np.float32) / half)
    return jnp.asarray(np.tile(frequency.astype(np.float32), 2)[None])


def layer(
    tokens,
    mixer_in_gain,
    query_weight,
    key_weight,
    value_weight,
    gate_weight,
    decay_logits,
    mixer_output,
    mixer_out_gain,
    channel_in_gain,
    gelu_weight,
    linear_weight,
    gelu_kernel,
    linear_kernel,
    gelu_bias,
    linear_bias,
    down_weight,
    channel_out_gain,
):
    place = jnp.stack([lax.axis_index(a).astype(jnp.int32) for a in ("x", "y", "z", "c")])
    place, query_weight = lax.optimization_barrier((place, query_weight))
    token_rows = tokens[0]
    own, model = token_rows.shape
    chips = lax.axis_size("x")
    half = chips * own
    width = gelu_weight.shape[1]

    def row(vector):
        return vector.reshape(1, -1)

    parts = (
        query_weight,
        key_weight,
        value_weight,
        gate_weight,
        mixer_output.T,
        gelu_weight,
        linear_weight,
        down_weight.T,
    )
    packed = call(
        functools.partial(pack_body, width),
        shape((32, FIRST + SECOND + THIRD)),
        *parts,
        hbm=8,
        scratch=[pltpu.VMEM(part.shape, bf16) for part in parts]
        + [pltpu.SemaphoreType.DMA((8,))],
    )
    got = {0: packed}
    for k in Z_ISSUE:
        got[k] = lax.ppermute(packed, RING, ring_pairs(k))
    spread = call(
        first_norm_body, shape((chips, own, model)), token_rows, row(mixer_in_gain), limit=60
    )
    normed_own = exchanged(spread).reshape(half, model)
    normed_other = swap(normed_own)
    first_z, second_z, third_z = call(
        ring_order_body,
        [shape((8, 32, columns)) for columns in (FIRST, SECOND, THIRD)],
        place,
        *[got[k] for k in Z_SHIFTS],
        smem=1,
    )
    first_pieces = line_gather(first_z)
    second_pieces = line_gather(second_z)
    third_pieces = line_gather(third_z)
    taps = call(
        functools.partial(taps_body, width),
        shape((8, PAD), f32),
        gelu_kernel,
        linear_kernel,
        gelu_bias,
        linear_bias,
    )
    taps_other = swap(taps)
    gated_own, gated_other = call(
        attend_body,
        [shape((half, DV)), shape((half, DV))],
        place,
        decay_logits[:, 0],
        normed_own,
        normed_other,
        *first_pieces,
        rope_frequency(),
        flops=1 << 32,
        smem=2,
        limit=10,
        scratch=[
            pltpu.VMEM((model, FIRST), bf16),
            pltpu.VMEM((2 * half, DK), bf16),
            pltpu.VMEM((2 * half, DK), bf16),
            pltpu.VMEM((2 * half, DV), bf16),
            pltpu.VMEM((2 * half, DV), f32),
        ],
    )
    out_own = in_line_order(second_pieces, place)
    for_partner = call(other_body, shape((half, model)), gated_other, out_own, flops=1 << 29)
    from_partner = swap(for_partner)
    far, right, left, here = call(
        output_body,
        [shape((own, model))] * 4,
        place,
        gated_own,
        out_own,
        from_partner,
        flops=1 << 29,
        smem=1,
    )
    after_mix, channel_in = call(
        middle_body,
        [shape((own, model)), shape((own, model))],
        *sent((far, right, left)),
        here,
        token_rows,
        row(mixer_out_gain),
        row(channel_in_gain),
    )
    third_own = in_line_order(third_pieces, place)
    third_other = swap(third_own)
    blocks = (*sent([channel_in] * 3), channel_in)
    edges = call(edges_body, shape((8, model)), *blocks)
    far, right, left, here = call(
        feed_body,
        [shape((own, model))] * 4,
        place,
        *blocks,
        swap(edges),
        third_own,
        third_other,
        taps,
        taps_other,
        flops=1 << 32,
        smem=1,
        limit=18,
        scratch=[
            pltpu.VMEM((half + 16, model), bf16),
            pltpu.VMEM((16, 2 * PAD), f32),
            pltpu.VMEM((half, 2 * PAD), bf16),
        ],
    )
    result = call(
        final_body,
        shape((own, model)),
        *sent((far, right, left)),
        here,
        after_mix,
        row(channel_out_gain),
    )
    return result[None]


def solution(mesh):
    fs = mesh.shape["fs"]
    tp = mesh.shape["tp"]
    split = Mesh(
        mesh.devices.reshape(mesh.shape["rep"], fs // 4, 4, tp // 2, 2),
        ("rep", "z", "y", "x", "c"),
    )
    in_specs = (
        P(("rep", "z", "y"), TP, None),
        P(),
        P(FS, TP),
        P(FS, TP),
        P(FS, TP),
        P(FS, TP),
        P(None, TP),
        P(TP, FS),
        P(),
        P(),
        P(FS, TP),
        P(FS, TP),
        P(None, TP),
        P(None, TP),
        P(TP),
        P(TP),
        P(TP, FS),
        P(),
    )
    out_specs = P(("rep", "z", "y"), TP, None)
    return jax.shard_map(layer, mesh=split, in_specs=in_specs, out_specs=out_specs, check_vma=False)
```
